256 devices in a mesh: ep: 32 (over z, x), tp: 8 (over y, core).
Axes of the slice: x: 4, y: 4, z: 8, core: 2. Of those that a mesh axis runs over, the one named last changes fastest.
Arguments:
- queries: bfloat16 [32768, 2048], P('ep', 'tp'), may hold values from -6 to 6
- key_vectors: bfloat16 [32768, 2048], P('ep', 'tp'), may hold values from -6 to 6
- value_vectors: bfloat16 [32768, 4096], P('ep', 'tp'), may hold values from -6 to 6
- decay_logit: float32 [32768, 2048], P('ep', 'tp'), may hold values from -11 to 16
- head_gain: float32 [256], replicated, may hold values from 0.1 to 1.9
- routed_rows: bfloat16 [8192, 4096], P('ep'), may hold values from -6 to 6
- pre_gain: float32 [4096], replicated, may hold values from 0.1 to 1.9
- expert_pick: int32 [8192, 2], P('ep'), may hold values from 0 to 31, as said below
- route_weight: float32 [8192, 2], P('ep'), may hold values from 0.2 to 1
- gate_weight: bfloat16 [32, 4096, 2048], P('ep', None, 'tp'), may hold values from -0.09375 to 0.09375
- up_weight: bfloat16 [32, 4096, 2048], P('ep', None, 'tp'), may hold values from -0.09375 to 0.09375
- down_weight: bfloat16 [32, 2048, 4096], P('ep', 'tp'), may hold values from -0.125 to 0.125
- post_gain: float32 [4096], replicated, may hold values from 0.1 to 1.9
Outputs:
- mixed_heads: bfloat16 [32768, 4096], P('ep', 'tp')
- routed_out: bfloat16 [8192, 4096], P(('ep', 'tp'))
The draws below stay inside these ranges and needn't reach their ends.
Inputs may be any that keep to these rules, and one draw needn't show every extreme that they name: `expert_pick`: each row names 2 different experts, both in the same one of 4 equal groups of consecutive expert numbers. In every aligned block of 32 rows no expert is named more than 4 times, and some expert exactly 4 times.
All inputs are finite; a program needn't handle non-finite values.
Results may differ from the reference program's by a relative error of at most 0.015.
Values may be sent and summed in bfloat16 or wider, within the bound.
No kernel may reach another device: no remote copies, remote signals or barrier semaphores. Data moves between devices by JAX's collectives and lax.ppermute only.
A program may use at most 128 MiB of HBM per device.

```python
import math
import jax
import jax.numpy as jnp
from jax import lax

D = 4096
HEADS = 16
DK = 128
DV = 256
FF = 2048
GROUPS = 4
TOP_K = 2
BLK = 64
TOK_A_DEV = 1024
SPAN_LENGTH = 32768
TOK_B = 8192
EXPERTS = 32
PART_ROWS = 32
CAP = 4
N_EP = 32
N_TP = 8


def draw_decay_logit(key, part):
    channel_count = HEADS * DK
    random_subkeys = jax.random.split(jax.random.fold_in(key, 7), 7)
    slow_level = jnp.log(SPAN_LENGTH * 1.18 / 8.0)
    fast_share = 0.5
    jitter = jax.random.uniform(random_subkeys[0], (SPAN_LENGTH, channel_count), jnp.float32, -1.0, 1.0)
    fast_mask = jax.random.uniform(random_subkeys[1], (channel_count,), jnp.float32) < fast_share
    fast_level = jax.random.uniform(random_subkeys[2], (channel_count,), jnp.float32, 0.5, 1.5)
    slow_spread = jax.random.uniform(random_subkeys[3], (channel_count,), jnp.float32, -0.5, 0.5)
    baseline = jnp.where(fast_mask, fast_level, slow_level + slow_spread)
    shards = SPAN_LENGTH // TOK_A_DEV
    shifts = jax.random.uniform(random_subkeys[4], (shards,), jnp.float32, -0.7, 0.7)
    shift_rows = jnp.repeat(shifts, TOK_A_DEV)
    surge_rows = jax.random.randint(random_subkeys[5], (3,), 0, SPAN_LENGTH)
    surge_value = jax.random.uniform(random_subkeys[6], (3, channel_count), jnp.float32, -11.0, -3.5)
    dropped_indicator = (jnp.arange(SPAN_LENGTH)[:, None] == surge_rows[None, :]).astype(jnp.float32)
    spike_segment = jnp.dot(dropped_indicator, surge_value, precision=lax.Precision.HIGHEST)
    spike_exists = jnp.sum(dropped_indicator, axis=1, keepdims=True) > 0.0
    expert_affinity_scores = baseline[None, :] + jitter + shift_rows[:, None]
    expert_affinity_scores = jnp.where(spike_exists, spike_segment, expert_affinity_scores)
    return jnp.clip(expert_affinity_scores, -11.0, 16.0).astype(jnp.float32)


def pick_block(block_key):
    per_group = EXPERTS // GROUPS
    half_cap = CAP // 2
    random_subkeys = jax.random.split(block_key, 6)
    orders = jax.vmap(lambda one_key: jax.random.permutation(one_key, per_group))(jax.random.split(random_subkeys[0], GROUPS))
    orders = orders.astype(jnp.int32)
    inverse = jnp.argsort(orders, axis=1).astype(jnp.int32)
    offsets = jax.random.randint(random_subkeys[1], (GROUPS, 1), 1, per_group)
    opening_round = jnp.take_along_axis(orders, (inverse + 1) % per_group, axis=1)
    second_turn = jnp.take_along_axis(orders, (inverse + offsets) % per_group, axis=1)
    member = jnp.arange(per_group, dtype=jnp.int32)[None, :, None]
    copy_index = jnp.arange(half_cap, dtype=jnp.int32)[None, None, :]
    partner = jnp.where(copy_index % 2 == 0, opening_round[:, :, None], second_turn[:, :, None])
    group_base = (jnp.arange(GROUPS, dtype=jnp.int32) * per_group)[:, None, None]
    leader = jnp.broadcast_to(group_base + member, partner.shape).reshape(-1)
    follower = (group_base + partner).reshape(-1)
    pair_count = leader.shape[0]
    chosen = jax.random.randint(random_subkeys[2], (), 0, EXPERTS)
    forced = ((leader == chosen) | (follower == chosen)).astype(jnp.int32)
    ranks = jax.random.permutation(random_subkeys[3], pair_count).astype(jnp.int32)
    picked = jnp.argsort(-(ranks + forced * pair_count))[:PART_ROWS]
    picked = picked[jax.random.permutation(random_subkeys[4], PART_ROWS)]
    flips = jax.random.randint(random_subkeys[5], (PART_ROWS,), 0, 2)
    first_col = jnp.where(flips == 1, follower[picked], leader[picked])
    second_col = jnp.where(flips == 1, leader[picked], follower[picked])
    return jnp.stack([first_col, second_col], axis=1).astype(jnp.int32)


def draw_expert_pick(key, part):
    blocks = TOK_B // PART_ROWS
    block_keys = jax.random.split(jax.random.fold_in(key, 11), blocks)
    return jax.vmap(pick_block)(block_keys).reshape(TOK_B, TOP_K).astype(jnp.int32)


def block_scale(stream_key, extent, cuts, least, top_value):
    def one(dim, shards_of):
        steps = jax.random.uniform(jax.random.fold_in(jax.random.fold_in(stream_key, 6), dim), (shards_of,), jnp.float32, least / len(cuts), top_value / len(cuts))
        return jnp.repeat(jnp.exp(steps), extent[dim] // shards_of).reshape((-1,) + (1,) * (len(extent) - dim - 1))

    loudness = one(*cuts[0])
    for cut in cuts[1:]:
        loudness = loudness * one(*cut)
    return loudness


def bell_draw(own_key, dims, deviation, reach, pieces=(), kind=jnp.bfloat16):
    factor_of = block_scale(own_key, dims, pieces, -0.22, 0.18) if pieces else 1.0
    drawn = jax.random.normal(own_key, dims, jnp.float32) * deviation * factor_of
    return jnp.minimum(jnp.maximum(drawn, -reach), reach).astype(kind)


def setup_inputs(seed: int = 0) -> dict:
    streams_of = jax.random.split(jax.random.key(seed), 14)
    return {
        "queries": bell_draw(streams_of[0], (SPAN_LENGTH, HEADS * DK), 1.0, 6.0, ((0, 32), (1, 8))),
        "key_vectors": bell_draw(streams_of[1], (SPAN_LENGTH, HEADS * DK), 1.0, 6.0, ((0, 32), (1, 8))),
        "value_vectors": bell_draw(streams_of[2], (SPAN_LENGTH, HEADS * DV), 1.0, 6.0, ((0, 32), (1, 8))),
        "decay_logit": draw_decay_logit(jax.random.fold_in(streams_of[13], 71), 0),
        "head_gain": jnp.clip(1.0 + 0.18 * jax.random.normal(streams_of[4], (DV,), jnp.float32), 0.1, 1.9),
        "routed_rows": bell_draw(streams_of[5], (TOK_B, D), 1.0, 6.0, ((0, 32),)),
        "pre_gain": jnp.clip(1.0 + 0.18 * jax.random.normal(streams_of[6], (D,), jnp.float32), 0.1, 1.9),
        "expert_pick": draw_expert_pick(jax.random.fold_in(streams_of[13], 71), 0),
        "route_weight": jnp.clip(jnp.exp(math.log(1.0) - 1.609438 * jax.random.uniform(streams_of[8], (TOK_B, TOP_K), jnp.float32) ** block_scale(streams_of[8], (TOK_B, TOP_K), ((0, 32),), -0.2, 0.2)), 0.2, 1.0),
        "gate_weight": bell_draw(streams_of[9], (EXPERTS, D, FF), D ** -0.5, 0.09375, ((0, 32), (2, 8))),
        "up_weight": bell_draw(streams_of[10], (EXPERTS, D, FF), D ** -0.5, 0.09375, ((0, 32), (2, 8))),
        "down_weight": bell_draw(streams_of[11], (EXPERTS, FF, D), FF ** -0.5, 0.125, ((0, 32), (1, 8))),
        "post_gain": jnp.clip(1.0 + 0.18 * jax.random.normal(streams_of[12], (D,), jnp.float32), 0.1, 1.9),
    }


def to_half(array):
    return lax.optimization_barrier(array.astype(jnp.bfloat16))

def row_norm(values, gain):
    return values * lax.rsqrt(lax.optimization_barrier(jnp.mean(values * values, axis=-1, keepdims=True)) + 1e-06) * gain

def token_mixer(queries, key_vectors, value_vectors, decay_logit, head_gain):
    blocks = SPAN_LENGTH // BLK
    key_shape = (blocks, BLK, HEADS, DK)
    log_rate = (jax.nn.log_sigmoid(decay_logit) / 16.0).reshape(key_shape)
    query_blocks = queries.reshape(key_shape)
    key_blocks = key_vectors.reshape(key_shape)
    value_blocks = value_vectors.reshape(blocks, BLK, HEADS, DV)
    causal_mask = jnp.tril(jnp.ones((BLK, BLK), dtype=bool))

    def advance(carry_state, inputs):
        query_rows, key_rows, value_rows, rate_rows = inputs
        cumulative = jnp.cumsum(rate_rows, axis=0)
        ending = cumulative[-1]
        query_decay = to_half(query_rows.astype(jnp.float32) * jnp.exp(cumulative))
        key_decay = to_half(key_rows.astype(jnp.float32) * jnp.exp(-cumulative))
        key_to_end = to_half(key_rows.astype(jnp.float32) * jnp.exp(ending[None] - cumulative))
        values_wide = value_rows.astype(jnp.float32)
        scores = jnp.einsum('ihd,jhd->hij', query_decay.astype(jnp.float32), key_decay.astype(jnp.float32))
        weights = to_half(jnp.where(causal_mask[None], scores, 0.0))
        inside = jnp.einsum('hij,jhe->ihe', weights.astype(jnp.float32), values_wide)
        state_half = to_half(carry_state).astype(jnp.float32)
        carried = jnp.einsum('ihd,hde->ihe', query_decay.astype(jnp.float32), state_half)
        update = jnp.einsum('jhd,jhe->hde', key_to_end.astype(jnp.float32), values_wide)
        next_state = carry_state * jnp.exp(ending)[:, :, None] + update
        produced = row_norm(inside + carried, head_gain).astype(jnp.bfloat16)
        return (next_state, produced)
    start_state = jnp.zeros((HEADS, DK, DV), jnp.float32)
    _, outputs = lax.scan(advance, start_state, (query_blocks, key_blocks, value_blocks, log_rate))
    return outputs.reshape(SPAN_LENGTH, HEADS * DV)

def routed_experts(routed_rows, pre_gain, expert_pick, route_weight, gate_weight, up_weight, down_weight, post_gain):
    normed = row_norm(routed_rows.astype(jnp.float32), pre_gain).astype(jnp.bfloat16)
    flat_pick = expert_pick.reshape(-1).astype(jnp.int32)
    flat_weight = route_weight.reshape(-1)
    expert_room = N_EP * N_TP * CAP
    slice_width = FF // N_TP

    def per_expert(summed, expert):
        ordering = jnp.argsort((flat_pick != expert).astype(jnp.int32), stable=True)[:expert_room].astype(jnp.int32)
        is_live = flat_pick[ordering] == expert
        row_index = (ordering // TOP_K).astype(jnp.int32)
        inputs = normed[row_index].astype(jnp.float32)
        gate_act = jnp.dot(inputs, gate_weight[expert].astype(jnp.float32), preferred_element_type=jnp.float32)
        up_act = jnp.dot(inputs, up_weight[expert].astype(jnp.float32), preferred_element_type=jnp.float32)
        hidden = to_half(jax.nn.silu(gate_act) * up_act).astype(jnp.float32)
        running = jnp.zeros((expert_room, D), jnp.float32)
        for portion in range(N_TP):
            lower_edge = portion * slice_width
            partial_value = jnp.dot(hidden[:, lower_edge:lower_edge + slice_width], down_weight[expert, lower_edge:lower_edge + slice_width].astype(jnp.float32), preferred_element_type=jnp.float32)
            running = running + to_half(partial_value).astype(jnp.float32)
        produced = to_half(running).astype(jnp.float32)
        factor = jnp.where(is_live, flat_weight[ordering], jnp.zeros_like(flat_weight[ordering]))
        return (summed.at[row_index].add(factor[:, None] * produced), None)
    summed, _ = lax.scan(per_expert, jnp.zeros((TOK_B, D), jnp.float32), jnp.arange(EXPERTS, dtype=jnp.int32))
    return row_norm(summed, post_gain).astype(jnp.bfloat16)

def reference(queries, key_vectors, value_vectors, decay_logit, head_gain, routed_rows, pre_gain, expert_pick, route_weight, gate_weight, up_weight, down_weight, post_gain):
    mixed_heads = token_mixer(queries, key_vectors, value_vectors, decay_logit, head_gain)
    routed_out = routed_experts(routed_rows, pre_gain, expert_pick, route_weight, gate_weight, up_weight, down_weight, post_gain)
    return (mixed_heads, routed_out)
```

```python
import functools

import jax
import jax.numpy as jnp
from jax import lax
from jax.experimental import pallas as pl
from jax.experimental.pallas import tpu as pltpu
from jax.sharding import Mesh
from jax.sharding import PartitionSpec as P

DK = 128
DV = 256
BLK = 64
CAP = 4
NY = 4
EP = ("z", "x")
F32 = jnp.float32
BF16 = jnp.bfloat16


def ring(size, step):
    return [(i, (i + step) % size) for i in range(size)]


def contract(a, b, dim_a, dim_b):
    return lax.dot_general(
        a, b, (((dim_a,), (dim_b,)), ((), ())), preferred_element_type=F32
    )


def attn_local_kernel(q_ref, k_ref, v_ref, g_ref, o_ref, qc_ref, st_ref, state, decay):
    step = pl.program_id(0)
    heads = state.shape[0]

    @pl.when(step == 0)
    def _():
        state[...] = jnp.zeros_like(state)
        decay[...] = jnp.zeros_like(decay)

    logit = g_ref[...]
    rate = (jnp.minimum(logit, 0.0) - jnp.log1p(jnp.exp(-jnp.abs(logit)))) * (1.0 / 16.0)
    row = lax.broadcasted_iota(jnp.int32, (BLK, BLK), 0)
    col = lax.broadcasted_iota(jnp.int32, (BLK, BLK), 1)
    causal = row >= col
    cumulative = jnp.dot(
        causal.astype(F32), rate, precision=lax.Precision.HIGHEST, preferred_element_type=F32
    )
    ending = cumulative[BLK - 1 : BLK, :]
    q = q_ref[...].astype(F32)
    k = k_ref[...].astype(F32)
    query_decay = (q * jnp.exp(cumulative)).astype(BF16)
    key_decay = (k * jnp.exp(-cumulative)).astype(BF16)
    key_to_end = (k * jnp.exp(ending - cumulative)).astype(BF16)
    before = decay[0:1, :]
    qc_ref[...] = (q * jnp.exp(cumulative + before)).astype(BF16)
    decay[...] = jnp.broadcast_to(before + ending, decay.shape)
    step_decay = jnp.exp(ending)
    for h in range(heads):
        ks = slice(h * DK, (h + 1) * DK)
        vs = slice(h * DV, (h + 1) * DV)
        v = v_ref[:, vs]
        scores = contract(query_decay[:, ks], key_decay[:, ks], 1, 1)
        weights = jnp.where(causal, scores, 0.0).astype(BF16)
        old = state[h]
        inside = contract(weights, v, 1, 0)
        o_ref[:, vs] = inside + contract(query_decay[:, ks], old.astype(BF16), 1, 1)
        state[h] = old * step_decay[:, ks] + contract(v, key_to_end[:, ks], 0, 0)

    @pl.when(step == pl.num_programs(0) - 1)
    def _():
        for h in range(heads):
            total = jnp.exp(decay[0:1, h * DK : (h + 1) * DK])
            st_ref[h, 0:DV, :] = state[h].astype(BF16)
            st_ref[h, DV:, :] = jnp.broadcast_to(total, (16, DK)).astype(BF16)


def attn_local(q, k, v, g):
    rows, keys = q.shape
    values = v.shape[1]
    heads = keys // DK
    return pl.pallas_call(
        attn_local_kernel,
        grid=(rows // BLK,),
        in_specs=[
            pl.BlockSpec((BLK, keys), lambda n: (n, 0)),
            pl.BlockSpec((BLK, keys), lambda n: (n, 0)),
            pl.BlockSpec((BLK, values), lambda n: (n, 0)),
            pl.BlockSpec((BLK, keys), lambda n: (n, 0)),
        ],
        out_specs=[
            pl.BlockSpec((BLK, values), lambda n: (n, 0)),
            pl.BlockSpec((BLK, keys), lambda n: (n, 0)),
            pl.BlockSpec((heads, DV + 16, DK), lambda n: (0, 0, 0)),
        ],
        out_shape=[
            jax.ShapeDtypeStruct((rows, values), F32),
            jax.ShapeDtypeStruct((rows, keys), BF16),
            jax.ShapeDtypeStruct((heads, DV + 16, DK), BF16),
        ],
        scratch_shapes=[
            pltpu.VMEM((heads, DV, DK), F32),
            pltpu.VMEM((8, keys), F32),
        ],
        compiler_params=pltpu.CompilerParams(dimension_semantics=("arbitrary",)),
        cost_estimate=pl.CostEstimate(
            flops=8 * 10**9, transcendentals=10**6, bytes_accessed=6 * 10**6
        ),
        name="attn_local",
    )(q, k, v, g)


def attn_out_kernel(o_ref, qc_ref, in_ref, gain_ref, out_ref):
    gain = gain_ref[...]
    for h in range(in_ref.shape[0]):
        vs = slice(h * DV, (h + 1) * DV)
        carried = contract(qc_ref[:, h * DK : (h + 1) * DK], in_ref[h, 0:DV, :], 1, 1)
        total = o_ref[:, vs] + carried
        mean = jnp.mean(total * total, axis=-1, keepdims=True)
        out_ref[:, vs] = (total * lax.rsqrt(mean + 1e-06) * gain).astype(BF16)


def attn_out(o, qc, incoming, gain):
    rows, values = o.shape
    tile = 256
    return pl.pallas_call(
        attn_out_kernel,
        grid=(rows // tile,),
        in_specs=[
            pl.BlockSpec((tile, values), lambda n: (n, 0)),
            pl.BlockSpec((tile, qc.shape[1]), lambda n: (n, 0)),
            pl.BlockSpec(incoming.shape, lambda n: (0, 0, 0)),
            pl.BlockSpec((1, DV), lambda n: (0, 0)),
        ],
        out_specs=pl.BlockSpec((tile, values), lambda n: (n, 0)),
        out_shape=jax.ShapeDtypeStruct((rows, values), BF16),
        compiler_params=pltpu.CompilerParams(dimension_semantics=("arbitrary",)),
        cost_estimate=pl.CostEstimate(
            flops=3 * 10**9, transcendentals=2048, bytes_accessed=4 * 10**6
        ),
        name="attn_out",
    )(o, qc, incoming, gain.reshape(1, DV))


def incoming_state(local):
    count = lax.axis_size(EP)

    def shifted(x, step):
        return lax.ppermute(x, EP, [(i, i + step) for i in range(count - step)])

    is_state = lax.broadcasted_iota(jnp.int32, local.shape, 1) < DV
    carry = shifted(local, 1).astype(F32)
    step = 1
    while step < count:
        arrived = shifted(carry.astype(BF16), step).astype(F32)
        carry = arrived * carry[:, DV : DV + 1, :] + jnp.where(is_state, carry, 0.0)
        step *= 2
    return carry.astype(BF16)


def dispatch_kernel(idx_ref, rows_ref, gain_ref, pick_ref, out_ref, slot_ref, *, part, experts):
    total = pick_ref.shape[0]
    first = pick_ref[:, 0:1]
    second = pick_ref[:, 1:2]
    lane = lax.broadcasted_iota(jnp.int32, (total, 128), 1)
    hit0 = first == lane
    hit1 = second == lane
    named = jnp.where(hit0 | hit1, 1.0, 0.0).astype(BF16)
    row = lax.broadcasted_iota(jnp.int32, (total, total), 0)
    col = lax.broadcasted_iota(jnp.int32, (total, total), 1)
    earlier = (col < row) & (col // part == row // part)
    before = contract(jnp.where(earlier, 1.0, 0.0).astype(BF16), named, 1, 0)
    rank0 = jnp.sum(jnp.where(hit0, before, 0.0), axis=1, keepdims=True)
    rank1 = jnp.sum(jnp.where(hit1, before, 0.0), axis=1, keepdims=True)
    slot_ref[:, 0:1] = first * CAP + rank0.astype(jnp.int32)
    slot_ref[:, 1:2] = second * CAP + rank1.astype(jnp.int32)
    values = rows_ref[...].astype(F32)
    mean = jnp.mean(values * values, axis=-1, keepdims=True)
    normed = (values * lax.rsqrt(mean + 1e-06) * gain_ref[...]).astype(BF16)
    own = slot_ref[pl.ds(pl.multiple_of(idx_ref[0] * part, part), part), :]
    place = lax.broadcasted_iota(jnp.int32, (part, experts * CAP), 1)
    chosen = (own[:, 0:1] == place) | (own[:, 1:2] == place)
    out_ref[...] = contract(jnp.where(chosen, 1.0, 0.0).astype(BF16), normed, 0, 0).astype(BF16)


def dispatch(index, rows, gain, pick, part, experts):
    total, width = rows.shape
    return pl.pallas_call(
        functools.partial(dispatch_kernel, part=part, experts=experts),
        grid_spec=pltpu.PrefetchScalarGridSpec(
            num_scalar_prefetch=1,
            grid=(1,),
            in_specs=[
                pl.BlockSpec((part, width), lambda n, idx: (idx[0], 0)),
                pl.BlockSpec((1, width), lambda n, idx: (0, 0)),
                pl.BlockSpec((total, 2), lambda n, idx: (0, 0)),
            ],
            out_specs=[
                pl.BlockSpec((experts * CAP, width), lambda n, idx: (0, 0)),
                pl.BlockSpec((total, 2), lambda n, idx: (0, 0)),
            ],
        ),
        out_shape=[
            jax.ShapeDtypeStruct((experts * CAP, width), BF16),
            jax.ShapeDtypeStruct((total, 2), jnp.int32),
        ],
        name="dispatch",
    )(index, rows, gain.reshape(1, width), pick)


def hidden_kernel(*refs, parts):
    xs = refs[:parts]
    weights = refs[parts : parts + 4]
    out_ref = refs[parts + 4]
    acc = refs[parts + 5]
    step = pl.program_id(0)
    x = jnp.concatenate([r[...] for r in xs], axis=0) if parts > 1 else xs[0][...]

    @pl.when(step == 0)
    def _():
        acc[...] = jnp.zeros_like(acc)

    width = weights[0].shape[1]
    for j, w in enumerate(weights):
        acc[:, j * width : (j + 1) * width] += contract(x, w[...], 1, 0)

    @pl.when(step == pl.num_programs(0) - 1)
    def _():
        for j in range(2):
            gate = acc[:, 2 * j * width : (2 * j + 1) * width]
            up = acc[:, (2 * j + 1) * width : (2 * j + 2) * width]
            value = gate / (1.0 + jnp.exp(-gate)) * up
            out_ref[:, j * width : (j + 1) * width] = value.astype(BF16)


def hidden_units(xs, weights, ktile=1024):
    rows = sum(x.shape[0] for x in xs)
    depth, width = weights[0].shape
    return pl.pallas_call(
        functools.partial(hidden_kernel, parts=len(xs)),
        grid=(depth // ktile,),
        in_specs=[pl.BlockSpec((x.shape[0], ktile), lambda n: (0, n)) for x in xs]
        + [pl.BlockSpec((ktile, width), lambda n: (n, 0)) for _ in weights],
        out_specs=pl.BlockSpec((rows, 2 * width), lambda n: (0, 0)),
        out_shape=jax.ShapeDtypeStruct((rows, 2 * width), BF16),
        scratch_shapes=[pltpu.VMEM((rows, 4 * width), F32)],
        compiler_params=pltpu.CompilerParams(dimension_semantics=("arbitrary",)),
        cost_estimate=pl.CostEstimate(
            flops=8 * rows * depth * width,
            transcendentals=2 * rows * width,
            bytes_accessed=8 * depth * width + 2 * rows * depth,
        ),
        name="hidden_units",
    )(*xs, *weights)


def down_kernel(h0, h1, h2a, h2b, h3, *rest):
    weights = rest[:8]
    out_ref = rest[8]
    width = weights[0].shape[0]
    group = h0.shape[1]
    rows = NY * group

    def blocks(pieces, shift):
        return jnp.concatenate([pieces[(i + shift) % NY] for i in range(NY)], axis=0)

    own = [h0[i] for i in range(NY)]
    right = [h1[i] for i in range(NY)]
    left = [h3[i] for i in range(NY)]
    far = [h2a[i] for i in range(2)] + [h2b[i] for i in range(2)]
    acts = (blocks(own, 0), blocks(right, 3), blocks(far, 2), blocks(left, 1))
    total = jnp.zeros((rows, out_ref.shape[1]), F32)
    for m, act in enumerate(acts):
        for c in range(2):
            total += contract(act[:, c * width : (c + 1) * width], weights[2 * m + c][...], 1, 0)
    new = lax.broadcasted_iota(jnp.int32, (rows, rows), 0)
    old = lax.broadcasted_iota(jnp.int32, (rows, rows), 1)
    want = (new // CAP % NY) * group + (new // (CAP * NY)) * CAP + new % CAP
    order = jnp.where(old == want, 1.0, 0.0).astype(BF16)
    out_ref[...] = contract(order, total.astype(BF16), 1, 0).astype(BF16)


def expert_down(hs, weights, tiles=2):
    h0, h1, h2a, h2b, h3 = hs
    blocks, rows, units = h0.shape
    group = rows // tiles
    width = weights[0].shape[1]

    def spec(h):
        return pl.BlockSpec((h.shape[0], group, units), lambda n: (0, n, 0))

    return pl.pallas_call(
        down_kernel,
        grid=(tiles,),
        in_specs=[spec(h) for h in hs]
        + [pl.BlockSpec(w.shape, lambda n: (0, 0)) for w in weights],
        out_specs=pl.BlockSpec((blocks * group, width), lambda n: (n, 0)),
        out_shape=jax.ShapeDtypeStruct((blocks * rows, width), BF16),
        compiler_params=pltpu.CompilerParams(dimension_semantics=("arbitrary",)),
        cost_estimate=pl.CostEstimate(
            flops=2 * blocks * rows * units * NY * width,
            transcendentals=0,
            bytes_accessed=8 * 10**6,
        ),
        name="expert_down",
    )(*hs, *weights)


def combine_kernel(idx_ref, back_ref, slot_ref, weight_ref, o0, o1, o2, o3, *, part):
    y = idx_ref[1]
    core = idx_ref[2]
    slots = back_ref.shape[0]
    place = lax.broadcasted_iota(jnp.int32, (part, slots), 1)
    picks0, picks1, w0, w1 = [], [], [], []
    for i in range(NY):
        block = ((y + i) % NY) * 2 + core
        rows = pl.ds(pl.multiple_of(block * part, part), part)
        slot = slot_ref[rows, :]
        weight = weight_ref[rows, :]
        spot = (slot // CAP) * (CAP * NY) + i * CAP + slot % CAP
        picks0.append(jnp.where(spot[:, 0:1] == place, 1.0, 0.0).astype(BF16))
        picks1.append(jnp.where(spot[:, 1:2] == place, 1.0, 0.0).astype(BF16))
        w0.append(weight[:, 0:1])
        w1.append(weight[:, 1:2])
    back = back_ref[...]
    first = contract(jnp.concatenate(picks0, axis=0), back, 1, 0)
    second = contract(jnp.concatenate(picks1, axis=0), back, 1, 0)
    mixed = first * jnp.concatenate(w0, axis=0) + second * jnp.concatenate(w1, axis=0)
    for i, out in enumerate((o0, o1, o2, o3)):
        out[...] = mixed[i * part : (i + 1) * part].astype(out.dtype)


def combine(index, back, slots, weight, part):
    width = back.shape[1]
    total = slots.shape[0]
    return pl.pallas_call(
        functools.partial(combine_kernel, part=part),
        grid_spec=pltpu.PrefetchScalarGridSpec(
            num_scalar_prefetch=1,
            grid=(1,),
            in_specs=[
                pl.BlockSpec(back.shape, lambda n, idx: (0, 0)),
                pl.BlockSpec((total, 2), lambda n, idx: (0, 0)),
                pl.BlockSpec((total, 2), lambda n, idx: (0, 0)),
            ],
            out_specs=[pl.BlockSpec((part, width), lambda n, idx: (0, 0)) for _ in range(NY)],
        ),
        out_shape=[jax.ShapeDtypeStruct((part, width), BF16) for _ in range(NY)],
        name="combine",
    )(index, back, slots, weight)


def finish_kernel(idx_ref, p0, p1, p2, p3, gain_ref, out_ref):
    y = idx_ref[1]
    width = p0.shape[1]
    pieces = [p[...].astype(F32) for p in (p0, p1, p2, p3)]
    square = sum(jnp.sum(p * p, axis=-1, keepdims=True) for p in pieces)
    scale = lax.rsqrt(square / (width * NY) + 1e-06)
    for i, piece in enumerate(pieces):
        columns = pl.ds(pl.multiple_of(((y + i) % NY) * width, width), width)
        out_ref[:, columns] = (piece * scale * gain_ref[:, columns]).astype(BF16)


def finish(index, pieces, gain):
    part, width = pieces[0].shape
    full = width * NY
    return pl.pallas_call(
        finish_kernel,
        grid_spec=pltpu.PrefetchScalarGridSpec(
            num_scalar_prefetch=1,
            grid=(1,),
            in_specs=[pl.BlockSpec((part, width), lambda n, idx: (0, 0)) for _ in pieces]
            + [pl.BlockSpec((1, full), lambda n, idx: (0, 0))],
            out_specs=pl.BlockSpec((part, full), lambda n, idx: (0, 0)),
        ),
        out_shape=jax.ShapeDtypeStruct((part, full), BF16),
        name="finish",
    )(index, *pieces, gain.reshape(1, full))


def gather_y(own):
    half = own.shape[0] // 2
    right = lax.ppermute(own, "y", ring(NY, -1))
    left = lax.ppermute(own, "y", ring(NY, 1))
    far_a = lax.ppermute(left[:half], "y", ring(NY, 1))
    far_b = lax.ppermute(right[half:], "y", ring(NY, -1))
    return own, right, far_a, far_b, left


def on_device(
    queries,
    key_vectors,
    value_vectors,
    decay_logit,
    head_gain,
    routed_rows,
    pre_gain,
    expert_pick,
    route_weight,
    gate_weight,
    up_weight,
    down_weight,
    post_gain,
):
    y = lax.axis_index("y")
    core = lax.axis_index("c")
    experts = lax.axis_size(EP)
    part = routed_rows.shape[0] // (NY * 2)
    width = routed_rows.shape[1]
    index = jnp.stack([y * 2 + core, y, core]).astype(jnp.int32)
    swap = [(0, 1), (1, 0)]

    outgoing, slots = dispatch(index, routed_rows, pre_gain, expert_pick, part, experts)
    arrived = lax.all_to_all(
        outgoing.reshape(experts, CAP, width), EP, split_axis=0, concat_axis=0, tiled=True
    ).reshape(experts * CAP, width)

    gate, up, down = gate_weight[0], up_weight[0], down_weight[0]
    weights = (gate, up, lax.ppermute(gate, "c", swap), lax.ppermute(up, "c", swap))
    cut = width // NY
    slices = [
        lax.dynamic_slice_in_dim(down, ((y + i) % NY) * cut, cut, axis=1) for i in range(NY)
    ]
    downs = []
    for m in range(NY):
        mine = slices[(-m) % NY]
        if m:
            mine = lax.ppermute(mine, "y", ring(NY, -m))
        downs += [mine, lax.ppermute(mine, "c", swap)]

    local_out, query_carry, local_state = attn_local(
        queries, key_vectors, value_vectors, decay_logit
    )
    incoming = incoming_state(local_state)

    own, right, far_a, far_b, left = gather_y(arrived)
    h_own = hidden_units([own], weights)
    h_sides = hidden_units([right, left], weights)
    h_far = hidden_units([far_a, far_b], weights)
    n = own.shape[0]
    hidden = jnp.stack([h_own, h_sides[:n], h_far, h_sides[n:]])
    back = expert_down(gather_y(hidden), downs)
    returned = lax.all_to_all(
        back.reshape(experts, NY * CAP, cut), EP, split_axis=0, concat_axis=0, tiled=True
    ).reshape(experts * NY * CAP, cut)

    pieces = combine(index, returned, slots, route_weight, part)
    gathered = [pieces[0]]
    for m in range(1, NY):
        gathered.append(lax.ppermute(pieces[(-m) % NY], "y", ring(NY, -m)))
    routed_out = finish(index, gathered, post_gain)

    mixed_heads = attn_out(local_out, query_carry, incoming, head_gain)
    return (mixed_heads, routed_out)


def solution(mesh):
    ep, tp = mesh.shape["ep"], mesh.shape["tp"]
    torus = Mesh(mesh.devices.reshape(ep // 4, 4, NY, tp // NY), ("z", "x", "y", "c"))
    tpa = ("y", "c")
    placed = (
        P(EP, tpa),
        P(EP, tpa),
        P(EP, tpa),
        P(EP, tpa),
        P(),
        P(EP, None),
        P(),
        P(EP, None),
        P(EP, None),
        P(EP, None, tpa),
        P(EP, None, tpa),
        P(EP, tpa, None),
        P(),
    )
    return jax.shard_map(
        on_device,
        mesh=torus,
        in_specs=placed,
        out_specs=(P(EP, tpa), P(("z", "x", "y", "c"), None)),
        check_vma=False,
    )
```

```python
import functools

import jax
import jax.numpy as jnp
from jax import lax
from jax.experimental import pallas as pl
from jax.experimental.pallas import tpu as pltpu
from jax.sharding import Mesh
from jax.sharding import PartitionSpec as P

DK = 128
DV = 256
BLK = 64
VROWS = 16
CAP = 4
NY = 4
EP = ("z", "x")
F32 = jnp.float32
BF16 = jnp.bfloat16


def ring(size, step):
    return [(i, (i + step) % size) for i in range(size)]


def contract(a, b, dim_a, dim_b):
    return lax.dot_general(
        a, b, (((dim_a,), (dim_b,)), ((), ())), preferred_element_type=F32
    )


def attn_local_kernel(q_ref, k_ref, v_ref, g_ref, o_ref, qc_ref, st_ref, state, decay):
    step = pl.program_id(0)
    heads = state.shape[0]

    @pl.when(step == 0)
    def _():
        state[...] = jnp.zeros_like(state)
        decay[...] = jnp.zeros_like(decay)

    logit = g_ref[...]
    rate = (jnp.minimum(logit, 0.0) - jnp.log1p(jnp.exp(-jnp.abs(logit)))) * (1.0 / 16.0)
    row = lax.broadcasted_iota(jnp.int32, (BLK, BLK), 0)
    col = lax.broadcasted_iota(jnp.int32, (BLK, BLK), 1)
    causal = row >= col
    cumulative = jnp.dot(
        causal.astype(F32), rate, precision=lax.Precision.HIGHEST, preferred_element_type=F32
    )
    ending = cumulative[BLK - 1 : BLK, :]
    q = q_ref[...].astype(F32)
    k = k_ref[...].astype(F32)
    query_decay = (q * jnp.exp(cumulative)).astype(BF16)
    key_decay = (k * jnp.exp(-cumulative)).astype(BF16)
    key_to_end = (k * jnp.exp(ending - cumulative)).astype(BF16)
    before = decay[0:1, :]
    qc_ref[...] = (q * jnp.exp(cumulative + before)).astype(BF16)
    decay[...] = jnp.broadcast_to(before + ending, decay.shape)
    step_decay = jnp.exp(ending)
    for h in range(heads):
        ks = slice(h * DK, (h + 1) * DK)
        vs = slice(h * DV, (h + 1) * DV)
        v = v_ref[:, vs]
        scores = contract(query_decay[:, ks], key_decay[:, ks], 1, 1)
        weights = jnp.where(causal, scores, 0.0).astype(BF16)
        old = state[h]
        inside = contract(weights, v, 1, 0)
        o_ref[:, vs] = inside + contract(query_decay[:, ks], old.astype(BF16), 1, 1)
        state[h] = old * step_decay[:, ks] + contract(v, key_to_end[:, ks], 0, 0)

    @pl.when(step == pl.num_programs(0) - 1)
    def _():
        for h in range(heads):
            total = jnp.exp(decay[0:1, h * DK : (h + 1) * DK])
            chunks = DV // VROWS
            own = slice(h * chunks, (h + 1) * chunks)
            st_ref[own, 0:VROWS, :] = state[h].astype(BF16).reshape(chunks, VROWS, DK)
            st_ref[own, VROWS:, :] = jnp.broadcast_to(total, (chunks, 8, DK)).astype(BF16)


def attn_local(q, k, v, g):
    rows, keys = q.shape
    values = v.shape[1]
    heads = keys // DK
    return pl.pallas_call(
        attn_local_kernel,
        grid=(rows // BLK,),
        in_specs=[
            pl.BlockSpec((BLK, keys), lambda n: (n, 0)),
            pl.BlockSpec((BLK, keys), lambda n: (n, 0)),
            pl.BlockSpec((BLK, values), lambda n: (n, 0)),
            pl.BlockSpec((BLK, keys), lambda n: (n, 0)),
        ],
        out_specs=[
            pl.BlockSpec((BLK, values), lambda n: (n, 0)),
            pl.BlockSpec((BLK, keys), lambda n: (n, 0)),
            pl.BlockSpec((heads * DV // VROWS, VROWS + 8, DK), lambda n: (0, 0, 0)),
        ],
        out_shape=[
            jax.ShapeDtypeStruct((rows, values), F32),
            jax.ShapeDtypeStruct((rows, keys), BF16),
            jax.ShapeDtypeStruct((heads * DV // VROWS, VROWS + 8, DK), BF16),
        ],
        scratch_shapes=[
            pltpu.VMEM((heads, DV, DK), F32),
            pltpu.VMEM((8, keys), F32),
        ],
        compiler_params=pltpu.CompilerParams(dimension_semantics=("arbitrary",)),
        cost_estimate=pl.CostEstimate(
            flops=8 * 10**9, transcendentals=10**6, bytes_accessed=6 * 10**6
        ),
        name="attn_local",
    )(q, k, v, g)


def attn_out_kernel(o_ref, qc_ref, in_ref, gain_ref, out_ref):
    gain = gain_ref[...]
    for h in range(in_ref.shape[0]):
        vs = slice(h * DV, (h + 1) * DV)
        carried = contract(qc_ref[:, h * DK : (h + 1) * DK], in_ref[h], 1, 1)
        total = o_ref[:, vs] + carried
        mean = jnp.mean(total * total, axis=-1, keepdims=True)
        out_ref[:, vs] = (total * lax.rsqrt(mean + 1e-06) * gain).astype(BF16)


def attn_out(o, qc, incoming, gain):
    rows, values = o.shape
    tile = 256
    return pl.pallas_call(
        attn_out_kernel,
        grid=(rows // tile,),
        in_specs=[
            pl.BlockSpec((tile, values), lambda n: (n, 0)),
            pl.BlockSpec((tile, qc.shape[1]), lambda n: (n, 0)),
            pl.BlockSpec(incoming.shape, lambda n: (0, 0, 0)),
            pl.BlockSpec((1, DV), lambda n: (0, 0)),
        ],
        out_specs=pl.BlockSpec((tile, values), lambda n: (n, 0)),
        out_shape=jax.ShapeDtypeStruct((rows, values), BF16),
        compiler_params=pltpu.CompilerParams(dimension_semantics=("arbitrary",)),
        cost_estimate=pl.CostEstimate(
            flops=3 * 10**9, transcendentals=2048, bytes_accessed=4 * 10**6
        ),
        name="attn_out",
    )(o, qc, incoming, gain.reshape(1, DV))


def prefix_kernel(in_ref, out_ref):
    carry = jnp.zeros((VROWS, DK), F32)
    for s in range(in_ref.shape[0]):
        out_ref[s] = carry.astype(BF16)
        decay = in_ref[s, VROWS:, :].astype(F32)[0:1, :]
        carry = carry * decay + in_ref[s, 0:VROWS, :].astype(F32)


def exchange(x):
    return lax.all_to_all(x, EP, split_axis=0, concat_axis=0, tiled=True)


def prefix(arrived):
    return pl.pallas_call(
        prefix_kernel,
        out_shape=jax.ShapeDtypeStruct((arrived.shape[0], VROWS, DK), BF16),
        name="prefix",
    )(arrived)


def dispatch_kernel(idx_ref, rows_ref, gain_ref, pick_ref, out_ref, slot_ref, *, part, experts):
    total = pick_ref.shape[0]
    first = pick_ref[:, 0:1]
    second = pick_ref[:, 1:2]
    lane = lax.broadcasted_iota(jnp.int32, (total, 128), 1)
    hit0 = first == lane
    hit1 = second == lane
    named = jnp.where(hit0 | hit1, 1.0, 0.0).astype(BF16)
    row = lax.broadcasted_iota(jnp.int32, (total, total), 0)
    col = lax.broadcasted_iota(jnp.int32, (total, total), 1)
    earlier = (col < row) & (col // part == row // part)
    before = contract(jnp.where(earlier, 1.0, 0.0).astype(BF16), named, 1, 0)
    rank0 = jnp.sum(jnp.where(hit0, before, 0.0), axis=1, keepdims=True)
    rank1 = jnp.sum(jnp.where(hit1, before, 0.0), axis=1, keepdims=True)
    slot_ref[:, 0:1] = first * CAP + rank0.astype(jnp.int32)
    slot_ref[:, 1:2] = second * CAP + rank1.astype(jnp.int32)
    values = rows_ref[...].astype(F32)
    mean = jnp.mean(values * values, axis=-1, keepdims=True)
    normed = (values * lax.rsqrt(mean + 1e-06) * gain_ref[...]).astype(BF16)
    own = slot_ref[pl.ds(pl.multiple_of(idx_ref[0] * part, part), part), :]
    place = lax.broadcasted_iota(jnp.int32, (part, experts * CAP), 1)
    chosen = (own[:, 0:1] == place) | (own[:, 1:2] == place)
    out_ref[...] = contract(jnp.where(chosen, 1.0, 0.0).astype(BF16), normed, 0, 0).astype(BF16)


def dispatch(index, rows, gain, pick, part, experts):
    total, width = rows.shape
    return pl.pallas_call(
        functools.partial(dispatch_kernel, part=part, experts=experts),
        grid_spec=pltpu.PrefetchScalarGridSpec(
            num_scalar_prefetch=1,
            grid=(1,),
            in_specs=[
                pl.BlockSpec((part, width), lambda n, idx: (idx[0], 0)),
                pl.BlockSpec((1, width), lambda n, idx: (0, 0)),
                pl.BlockSpec((total, 2), lambda n, idx: (0, 0)),
            ],
            out_specs=[
                pl.BlockSpec((experts * CAP, width), lambda n, idx: (0, 0)),
                pl.BlockSpec((total, 2), lambda n, idx: (0, 0)),
            ],
        ),
        out_shape=[
            jax.ShapeDtypeStruct((experts * CAP, width), BF16),
            jax.ShapeDtypeStruct((total, 2), jnp.int32),
        ],
        name="dispatch",
    )(index, rows, gain.reshape(1, width), pick)


def hidden_kernel(*refs, parts):
    xs = refs[:parts]
    weights = refs[parts : parts + 4]
    out_ref = refs[parts + 4]
    acc = refs[parts + 5]
    step = pl.program_id(0)
    x = jnp.concatenate([r[...] for r in xs], axis=0) if parts > 1 else xs[0][...]

    @pl.when(step == 0)
    def _():
        acc[...] = jnp.zeros_like(acc)

    width = weights[0].shape[1]
    for j, w in enumerate(weights):
        acc[:, j * width : (j + 1) * width] += contract(x, w[...], 1, 0)

    @pl.when(step == pl.num_programs(0) - 1)
    def _():
        for j in range(2):
            gate = acc[:, 2 * j * width : (2 * j + 1) * width]
            up = acc[:, (2 * j + 1) * width : (2 * j + 2) * width]
            value = gate / (1.0 + jnp.exp(-gate)) * up
            out_ref[:, j * width : (j + 1) * width] = value.astype(BF16)


def hidden_units(xs, weights, ktile=1024):
    rows = sum(x.shape[0] for x in xs)
    depth, width = weights[0].shape
    return pl.pallas_call(
        functools.partial(hidden_kernel, parts=len(xs)),
        grid=(depth // ktile,),
        in_specs=[pl.BlockSpec((x.shape[0], ktile), lambda n: (0, n)) for x in xs]
        + [pl.BlockSpec((ktile, width), lambda n: (n, 0)) for _ in weights],
        out_specs=pl.BlockSpec((rows, 2 * width), lambda n: (0, 0)),
        out_shape=jax.ShapeDtypeStruct((rows, 2 * width), BF16),
        scratch_shapes=[pltpu.VMEM((rows, 4 * width), F32)],
        compiler_params=pltpu.CompilerParams(dimension_semantics=("arbitrary",)),
        cost_estimate=pl.CostEstimate(
            flops=8 * rows * depth * width,
            transcendentals=2 * rows * width,
            bytes_accessed=8 * depth * width + 2 * rows * depth,
        ),
        name="hidden_units",
    )(*xs, *weights)


def down_kernel(h0, h1, h2a, h2b, h3, *rest):
    weights = rest[:8]
    out_ref = rest[8]
    width = weights[0].shape[0]
    group = h0.shape[1]
    rows = NY * group

    def blocks(pieces, shift):
        return jnp.concatenate([pieces[(i + shift) % NY] for i in range(NY)], axis=0)

    own = [h0[i] for i in range(NY)]
    right = [h1[i] for i in range(NY)]
    left = [h3[i] for i in range(NY)]
    far = [h2a[i] for i in range(2)] + [h2b[i] for i in range(2)]
    acts = (blocks(own, 0), blocks(right, 3), blocks(far, 2), blocks(left, 1))
    total = jnp.zeros((rows, out_ref.shape[1]), F32)
    for m, act in enumerate(acts):
        for c in range(2):
            total += contract(act[:, c * width : (c + 1) * width], weights[2 * m + c][...], 1, 0)
    new = lax.broadcasted_iota(jnp.int32, (rows, rows), 0)
    old = lax.broadcasted_iota(jnp.int32, (rows, rows), 1)
    want = (new // CAP % NY) * group + (new // (CAP * NY)) * CAP + new % CAP
    order = jnp.where(old == want, 1.0, 0.0).astype(BF16)
    out_ref[...] = contract(order, total.astype(BF16), 1, 0).astype(BF16)


def expert_down(hs, weights, tiles=2):
    h0, h1, h2a, h2b, h3 = hs
    blocks, rows, units = h0.shape
    group = rows // tiles
    width = weights[0].shape[1]

    def spec(h):
        return pl.BlockSpec((h.shape[0], group, units), lambda n: (0, n, 0))

    return pl.pallas_call(
        down_kernel,
        grid=(tiles,),
        in_specs=[spec(h) for h in hs]
        + [pl.BlockSpec(w.shape, lambda n: (0, 0)) for w in weights],
        out_specs=pl.BlockSpec((blocks * group, width), lambda n: (n, 0)),
        out_shape=jax.ShapeDtypeStruct((blocks * rows, width), BF16),
        compiler_params=pltpu.CompilerParams(dimension_semantics=("arbitrary",)),
        cost_estimate=pl.CostEstimate(
            flops=2 * blocks * rows * units * NY * width,
            transcendentals=0,
            bytes_accessed=8 * 10**6,
        ),
        name="expert_down",
    )(*hs, *weights)


def combine_kernel(idx_ref, back_ref, slot_ref, weight_ref, o0, o1, o2, o3, *, part):
    y = idx_ref[1]
    core = idx_ref[2]
    slots = back_ref.shape[0]
    place = lax.broadcasted_iota(jnp.int32, (part, slots), 1)
    picks0, picks1, w0, w1 = [], [], [], []
    for i in range(NY):
        block = ((y + i) % NY) * 2 + core
        rows = pl.ds(pl.multiple_of(block * part, part), part)
        slot = slot_ref[rows, :]
        weight = weight_ref[rows, :]
        spot = (slot // CAP) * (CAP * NY) + i * CAP + slot % CAP
        picks0.append(jnp.where(spot[:, 0:1] == place, 1.0, 0.0).astype(BF16))
        picks1.append(jnp.where(spot[:, 1:2] == place, 1.0, 0.0).astype(BF16))
        w0.append(weight[:, 0:1])
        w1.append(weight[:, 1:2])
    back = back_ref[...]
    first = contract(jnp.concatenate(picks0, axis=0), back, 1, 0)
    second = contract(jnp.concatenate(picks1, axis=0), back, 1, 0)
    mixed = first * jnp.concatenate(w0, axis=0) + second * jnp.concatenate(w1, axis=0)
    for i, out in enumerate((o0, o1, o2, o3)):
        out[...] = mixed[i * part : (i + 1) * part].astype(out.dtype)


def combine(index, back, slots, weight, part):
    width = back.shape[1]
    total = slots.shape[0]
    return pl.pallas_call(
        functools.partial(combine_kernel, part=part),
        grid_spec=pltpu.PrefetchScalarGridSpec(
            num_scalar_prefetch=1,
            grid=(1,),
            in_specs=[
                pl.BlockSpec(back.shape, lambda n, idx: (0, 0)),
                pl.BlockSpec((total, 2), lambda n, idx: (0, 0)),
                pl.BlockSpec((total, 2), lambda n, idx: (0, 0)),
            ],
            out_specs=[pl.BlockSpec((part, width), lambda n, idx: (0, 0)) for _ in range(NY)],
        ),
        out_shape=[jax.ShapeDtypeStruct((part, width), BF16) for _ in range(NY)],
        name="combine",
    )(index, back, slots, weight)


def finish_kernel(idx_ref, p0, p1, p2, p3, gain_ref, out_ref):
    y = idx_ref[1]
    width = p0.shape[1]
    pieces = [p[...].astype(F32) for p in (p0, p1, p2, p3)]
    square = sum(jnp.sum(p * p, axis=-1, keepdims=True) for p in pieces)
    scale = lax.rsqrt(square / (width * NY) + 1e-06)
    for i, piece in enumerate(pieces):
        columns = pl.ds(pl.multiple_of(((y + i) % NY) * width, width), width)
        out_ref[:, columns] = (piece * scale * gain_ref[:, columns]).astype(BF16)


def finish(index, pieces, gain):
    part, width = pieces[0].shape
    full = width * NY
    return pl.pallas_call(
        finish_kernel,
        grid_spec=pltpu.PrefetchScalarGridSpec(
            num_scalar_prefetch=1,
            grid=(1,),
            in_specs=[pl.BlockSpec((part, width), lambda n, idx: (0, 0)) for _ in pieces]
            + [pl.BlockSpec((1, full), lambda n, idx: (0, 0))],
            out_specs=pl.BlockSpec((part, full), lambda n, idx: (0, 0)),
        ),
        out_shape=jax.ShapeDtypeStruct((part, full), BF16),
        name="finish",
    )(index, *pieces, gain.reshape(1, full))


def gather_y(own):
    half = own.shape[0] // 2
    right = lax.ppermute(own, "y", ring(NY, -1))
    left = lax.ppermute(own, "y", ring(NY, 1))
    far_a = lax.ppermute(left[:half], "y", ring(NY, 1))
    far_b = lax.ppermute(right[half:], "y", ring(NY, -1))
    return own, right, far_a, far_b, left


def on_device(
    queries,
    key_vectors,
    value_vectors,
    decay_logit,
    head_gain,
    routed_rows,
    pre_gain,
    expert_pick,
    route_weight,
    gate_weight,
    up_weight,
    down_weight,
    post_gain,
):
    y = lax.axis_index("y")
    core = lax.axis_index("c")
    experts = lax.axis_size(EP)
    part = routed_rows.shape[0] // (NY * 2)
    width = routed_rows.shape[1]
    index = jnp.stack([y * 2 + core, y, core]).astype(jnp.int32)
    swap = [(0, 1), (1, 0)]

    outgoing, slots = dispatch(index, routed_rows, pre_gain, expert_pick, part, experts)
    arrived = lax.all_to_all(
        outgoing.reshape(experts, CAP, width), EP, split_axis=0, concat_axis=0, tiled=True
    ).reshape(experts * CAP, width)

    gate, up, down = gate_weight[0], up_weight[0], down_weight[0]
    weights = (gate, up, lax.ppermute(gate, "c", swap), lax.ppermute(up, "c", swap))
    cut = width // NY
    slices = [
        lax.dynamic_slice_in_dim(down, ((y + i) % NY) * cut, cut, axis=1) for i in range(NY)
    ]
    downs = []
    for m in range(NY):
        mine = slices[(-m) % NY]
        if m:
            mine = lax.ppermute(mine, "y", ring(NY, -m))
        downs += [mine, lax.ppermute(mine, "c", swap)]

    local_out, query_carry, local_state = attn_local(
        queries, key_vectors, value_vectors, decay_logit
    )
    arrived, downs, weights, local_state = lax.optimization_barrier(
        (arrived, downs, weights, local_state)
    )
    own, right, far_a, far_b, left = gather_y(arrived)
    right, left, chunk_states = lax.optimization_barrier((right, left, exchange(local_state)))
    before = exchange(prefix(chunk_states))
    h_own = hidden_units([own], weights)
    h_sides = hidden_units([right, left], weights)
    h_far = hidden_units([far_a, far_b], weights)
    n = own.shape[0]
    hidden = jnp.stack([h_own, h_sides[:n], h_far, h_sides[n:]])
    hidden, before = lax.optimization_barrier((hidden, before))
    incoming = before.reshape(-1, DV, DK)
    back = expert_down(gather_y(hidden), downs)
    returned = lax.all_to_all(
        back.reshape(experts, NY * CAP, cut), EP, split_axis=0, concat_axis=0, tiled=True
    ).reshape(experts * NY * CAP, cut)

    mixed_heads = attn_out(local_out, query_carry, incoming, head_gain)
    returned, mixed_heads = lax.optimization_barrier((returned, mixed_heads))
    pieces = combine(index, returned, slots, route_weight, part)
    gathered = [pieces[0]]
    for m in range(1, NY):
        gathered.append(lax.ppermute(pieces[(-m) % NY], "y", ring(NY, -m)))
    routed_out = finish(index, gathered, post_gain)
    return (mixed_heads, routed_out)


def solution(mesh):
    ep, tp = mesh.shape["ep"], mesh.shape["tp"]
    torus = Mesh(mesh.devices.reshape(ep // 4, 4, NY, tp // NY), ("z", "x", "y", "c"))
    tpa = ("y", "c")
    placed = (
        P(EP, tpa),
        P(EP, tpa),
        P(EP, tpa),
        P(EP, tpa),
        P(),
        P(EP, None),
        P(),
        P(EP, None),
        P(EP, None),
        P(EP, None, tpa),
        P(EP, None, tpa),
        P(EP, tpa, None),
        P(),
    )
    return jax.shard_map(
        on_device,
        mesh=torus,
        in_specs=placed,
        out_specs=(P(EP, tpa), P(("z", "x", "y", "c"), None)),
        check_vma=False,
    )
```

```python
import functools

import jax
import jax.numpy as jnp
from jax import lax
from jax.experimental import pallas as pl
from jax.experimental.pallas import tpu as pltpu
from jax.sharding import Mesh
from jax.sharding import PartitionSpec as P

DK = 128
DV = 256
BLK = 64
VROWS = 16
CAP = 4
NY = 4
EP = ("z", "x")
F32 = jnp.float32
BF16 = jnp.bfloat16


def ring(size, step):
    return [(i, (i + step) % size) for i in range(size)]


def contract(a, b, dim_a, dim_b):
    return lax.dot_general(
        a, b, (((dim_a,), (dim_b,)), ((), ())), preferred_element_type=F32
    )


def attn_local_kernel(q_ref, k_ref, v_ref, g_ref, o_ref, qc_ref, st_ref, state, decay):
    step = pl.program_id(0)
    heads = state.shape[0]

    @pl.when(step == 0)
    def _():
        state[...] = jnp.zeros_like(state)
        decay[...] = jnp.zeros_like(decay)

    logit = g_ref[...]
    rate = (jnp.minimum(logit, 0.0) - jnp.log1p(jnp.exp(-jnp.abs(logit)))) * (1.0 / 16.0)
    row = lax.broadcasted_iota(jnp.int32, (BLK, BLK), 0)
    col = lax.broadcasted_iota(jnp.int32, (BLK, BLK), 1)
    causal = row >= col
    cumulative = jnp.dot(
        causal.astype(F32), rate, precision=lax.Precision.HIGHEST, preferred_element_type=F32
    )
    ending = cumulative[BLK - 1 : BLK, :]
    q = q_ref[...].astype(F32)
    k = k_ref[...].astype(F32)
    query_decay = (q * jnp.exp(cumulative)).astype(BF16)
    key_decay = (k * jnp.exp(-cumulative)).astype(BF16)
    key_to_end = (k * jnp.exp(ending - cumulative)).astype(BF16)
    before = decay[0:1, :]
    qc_ref[...] = (q * jnp.exp(cumulative + before)).astype(BF16)
    decay[...] = jnp.broadcast_to(before + ending, decay.shape)
    step_decay = jnp.exp(ending)
    for h in range(heads):
        ks = slice(h * DK, (h + 1) * DK)
        vs = slice(h * DV, (h + 1) * DV)
        v = v_ref[:, vs]
        scores = contract(query_decay[:, ks], key_decay[:, ks], 1, 1)
        weights = jnp.where(causal, scores, 0.0).astype(BF16)
        old = state[h]
        inside = contract(weights, v, 1, 0)
        o_ref[:, vs] = inside + contract(query_decay[:, ks], old.astype(BF16), 1, 1)
        state[h] = old * step_decay[:, ks] + contract(v, key_to_end[:, ks], 0, 0)

    @pl.when(step == pl.num_programs(0) - 1)
    def _():
        for h in range(heads):
            total = jnp.exp(decay[0:1, h * DK : (h + 1) * DK])
            chunks = DV // VROWS
            own = slice(h * chunks, (h + 1) * chunks)
            st_ref[own, 0:VROWS, :] = state[h].astype(BF16).reshape(chunks, VROWS, DK)
            st_ref[own, VROWS:, :] = jnp.broadcast_to(total, (chunks, 8, DK)).astype(BF16)


def attn_local(q, k, v, g):
    rows, keys = q.shape
    values = v.shape[1]
    heads = keys // DK
    return pl.pallas_call(
        attn_local_kernel,
        grid=(rows // BLK,),
        in_specs=[
            pl.BlockSpec((BLK, keys), lambda n: (n, 0)),
            pl.BlockSpec((BLK, keys), lambda n: (n, 0)),
            pl.BlockSpec((BLK, values), lambda n: (n, 0)),
            pl.BlockSpec((BLK, keys), lambda n: (n, 0)),
        ],
        out_specs=[
            pl.BlockSpec((BLK, values), lambda n: (n, 0)),
            pl.BlockSpec((BLK, keys), lambda n: (n, 0)),
            pl.BlockSpec((heads * DV // VROWS, VROWS + 8, DK), lambda n: (0, 0, 0)),
        ],
        out_shape=[
            jax.ShapeDtypeStruct((rows, values), F32),
            jax.ShapeDtypeStruct((rows, keys), BF16),
            jax.ShapeDtypeStruct((heads * DV // VROWS, VROWS + 8, DK), BF16),
        ],
        scratch_shapes=[
            pltpu.VMEM((heads, DV, DK), F32),
            pltpu.VMEM((8, keys), F32),
        ],
        compiler_params=pltpu.CompilerParams(dimension_semantics=("arbitrary",)),
        cost_estimate=pl.CostEstimate(
            flops=8 * 10**9, transcendentals=10**6, bytes_accessed=6 * 10**6
        ),
        name="attn_local",
    )(q, k, v, g)


def attn_out_kernel(o_ref, qc_ref, in_ref, gain_ref, out_ref):
    gain = gain_ref[...]
    for h in range(in_ref.shape[0] // DV):
        vs = slice(h * DV, (h + 1) * DV)
        carried = contract(qc_ref[:, h * DK : (h + 1) * DK], in_ref[h * DV : (h + 1) * DV, :], 1, 1)
        total = o_ref[:, vs] + carried
        mean = jnp.mean(total * total, axis=-1, keepdims=True)
        out_ref[:, vs] = (total * lax.rsqrt(mean + 1e-06) * gain).astype(BF16)


def attn_out(o, qc, returned, gain, column):
    rows, values = o.shape
    tile = 256
    return pl.pallas_call(
        attn_out_kernel,
        grid=(rows // tile,),
        in_specs=[
            pl.BlockSpec((tile, values), lambda n: (n, 0)),
            pl.BlockSpec((tile, qc.shape[1]), lambda n: (n, 0)),
            pl.BlockSpec((returned.shape[0], DK), lambda n: (0, column)),
            pl.BlockSpec((1, DV), lambda n: (0, 0)),
        ],
        out_specs=pl.BlockSpec((tile, values), lambda n: (n, 0)),
        out_shape=jax.ShapeDtypeStruct((rows, values), BF16),
        compiler_params=pltpu.CompilerParams(dimension_semantics=("arbitrary",)),
        cost_estimate=pl.CostEstimate(
            flops=3 * 10**9, transcendentals=2048, bytes_accessed=4 * 10**6
        ),
        name="attn_out",
    )(o, qc, returned, gain.reshape(1, DV))


def prefix_kernel(in_ref, out_ref):
    carry = jnp.zeros((VROWS, DK), F32)
    for s in range(in_ref.shape[0]):
        out_ref[s] = carry.astype(BF16)
        decay = in_ref[s, VROWS:, :].astype(F32)[0:1, :]
        carry = carry * decay + in_ref[s, 0:VROWS, :].astype(F32)


def exchange(x):
    return lax.all_to_all(x, EP, split_axis=0, concat_axis=0, tiled=True)


def prefix(arrived):
    return pl.pallas_call(
        prefix_kernel,
        out_shape=jax.ShapeDtypeStruct((arrived.shape[0], VROWS, DK), BF16),
        name="prefix",
    )(arrived)


def own_columns(slots, first_rows, part):
    rows = slots.shape[1]
    wide = jnp.concatenate([slots] * 4, axis=0).astype(F32).astype(BF16)
    count = part * len(first_rows)
    row = lax.broadcasted_iota(jnp.int32, (rows, count), 0)
    col = lax.broadcasted_iota(jnp.int32, (rows, count), 1)
    source = col % part
    for i, first in enumerate(first_rows):
        source += jnp.where(col // part == i, first, 0)
    pick = jnp.where(row == source, 1.0, 0.0).astype(BF16)
    return contract(wide, pick, 1, 0)[0:2].astype(jnp.int32)


def dispatch_kernel(idx_ref, rows_ref, gain_ref, pick_ref, out_ref, slot_ref, *, part, experts):
    total = pick_ref.shape[1]
    pick = pick_ref[...]
    first = pick[0:1]
    second = pick[1:2]
    expert = lax.broadcasted_iota(jnp.int32, (experts, total), 0)
    hit0 = first == expert
    hit1 = second == expert
    named = jnp.where(hit0 | hit1, 1.0, 0.0).astype(BF16)
    row = lax.broadcasted_iota(jnp.int32, (total, total), 0)
    col = lax.broadcasted_iota(jnp.int32, (total, total), 1)
    earlier = (row < col) & (col // part == row // part)
    before = contract(named, jnp.where(earlier, 1.0, 0.0).astype(BF16), 1, 0)
    rank0 = jnp.sum(jnp.where(hit0, before, 0.0), axis=0, keepdims=True)
    rank1 = jnp.sum(jnp.where(hit1, before, 0.0), axis=0, keepdims=True)
    slots = pick * CAP + jnp.concatenate([rank0, rank1], axis=0).astype(jnp.int32)
    slot_ref[...] = slots
    values = rows_ref[...].astype(F32)
    mean = jnp.mean(values * values, axis=-1, keepdims=True)
    normed = (values * lax.rsqrt(mean + 1e-06) * gain_ref[...]).astype(BF16)
    own = own_columns(slots, [idx_ref[0] * part], part)
    place = lax.broadcasted_iota(jnp.int32, (out_ref.shape[0], part), 0)
    target = (place // (2 * CAP)) * CAP + place % CAP
    chosen = (own[0:1] == target) | (own[1:2] == target)
    half = out_ref.shape[1]
    total_out = None
    for h in range(2):
        mine = chosen & (place // CAP % 2 == h)
        piece = contract(
            jnp.where(mine, 1.0, 0.0).astype(BF16), normed[:, h * half : (h + 1) * half], 1, 0
        )
        total_out = piece if total_out is None else total_out + piece
    out_ref[...] = total_out.astype(BF16)


def dispatch(index, rows, gain, pick, part, experts):
    total, width = rows.shape
    return pl.pallas_call(
        functools.partial(dispatch_kernel, part=part, experts=experts),
        grid_spec=pltpu.PrefetchScalarGridSpec(
            num_scalar_prefetch=1,
            grid=(1,),
            in_specs=[
                pl.BlockSpec((part, width), lambda n, idx: (idx[0], 0)),
                pl.BlockSpec((1, width), lambda n, idx: (0, 0)),
                pl.BlockSpec((2, total), lambda n, idx: (0, 0)),
            ],
            out_specs=[
                pl.BlockSpec((experts * CAP * 2, width // 2), lambda n, idx: (0, 0)),
                pl.BlockSpec((2, total), lambda n, idx: (0, 0)),
            ],
        ),
        out_shape=[
            jax.ShapeDtypeStruct((experts * CAP * 2, width // 2), BF16),
            jax.ShapeDtypeStruct((2, total), jnp.int32),
        ],
        name="dispatch",
    )(index, rows, gain.reshape(1, width), pick.T)


def hidden_kernel(*refs, parts):
    xs = refs[:parts]
    weights = refs[parts : parts + 8]
    out_ref = refs[parts + 8]
    acc = refs[parts + 9]
    step = pl.program_id(0)
    rows = xs[0].shape[0]
    new = lax.broadcasted_iota(jnp.int32, (rows // 2, rows), 0)
    old = lax.broadcasted_iota(jnp.int32, (rows // 2, rows), 1)
    spread = (new // CAP) * (2 * CAP) + new % CAP
    x = []
    for h in range(2):
        order = jnp.where(old == spread + h * CAP, 1.0, 0.0).astype(BF16)
        x.append(
            jnp.concatenate([contract(order, r[...], 1, 0).astype(BF16) for r in xs], axis=0)
        )

    @pl.when(step == 0)
    def _():
        acc[...] = jnp.zeros_like(acc)

    width = weights[0].shape[1]
    for j in range(4):
        acc[:, j * width : (j + 1) * width] += contract(x[0], weights[2 * j][...], 1, 0) + contract(
            x[1], weights[2 * j + 1][...], 1, 0
        )

    @pl.when(step == pl.num_programs(0) - 1)
    def _():
        for j in range(2):
            gate = acc[:, 2 * j * width : (2 * j + 1) * width]
            up = acc[:, (2 * j + 1) * width : (2 * j + 2) * width]
            value = gate / (1.0 + jnp.exp(-gate)) * up
            out_ref[:, j * width : (j + 1) * width] = value.astype(BF16)


def hidden_units(xs, weights, ktile=512):
    rows = sum(x.shape[0] for x in xs) // 2
    depth, width = weights[0].shape
    steps = depth // 2 // ktile
    specs, doubled = [], []
    for w in weights:
        doubled += [w, w]
        specs += [
            pl.BlockSpec((ktile, width), lambda n: (n, 0)),
            pl.BlockSpec((ktile, width), lambda n: (n + steps, 0)),
        ]
    return pl.pallas_call(
        functools.partial(hidden_kernel, parts=len(xs)),
        grid=(steps,),
        in_specs=[pl.BlockSpec((x.shape[0], ktile), lambda n: (0, n)) for x in xs] + specs,
        out_specs=pl.BlockSpec((rows, 2 * width), lambda n: (0, 0)),
        out_shape=jax.ShapeDtypeStruct((rows, 2 * width), BF16),
        scratch_shapes=[pltpu.VMEM((rows, 4 * width), F32)],
        compiler_params=pltpu.CompilerParams(dimension_semantics=("arbitrary",)),
        cost_estimate=pl.CostEstimate(
            flops=8 * rows * depth * width,
            transcendentals=2 * rows * width,
            bytes_accessed=8 * depth * width + 2 * rows * depth,
        ),
        name="hidden_units",
    )(*xs, *doubled)


def down_kernel(n0, f0, n1, f1, n2, f2, n3, f3, *rest):
    weights = rest[:8]
    state_ref = rest[8]
    out_ref = rest[9]
    width = weights[0].shape[0]
    group = f0.shape[0]
    rows = NY * group
    depth = weights[0].shape[1]

    def blocks(near, far, shift):
        ordered = (near[0], near[1], far[...], near[2])
        return jnp.concatenate([ordered[(i + shift) % NY] for i in range(NY)], axis=0)

    acts = (blocks(n0, f0, 0), blocks(n1, f1, 3), blocks(n2, f2, 2), blocks(n3, f3, 1))
    total = jnp.zeros((rows, depth), F32)
    for m, act in enumerate(acts):
        for c in range(2):
            total += contract(act[:, c * width : (c + 1) * width], weights[2 * m + c][...], 1, 0)
    new = lax.broadcasted_iota(jnp.int32, (rows, rows), 0)
    old = lax.broadcasted_iota(jnp.int32, (rows, rows), 1)
    want = (new // CAP % NY) * group + (new // (CAP * NY)) * CAP + new % CAP
    order = jnp.where(old == want, 1.0, 0.0).astype(BF16)
    out_ref[:, 0:depth] = contract(order, total.astype(BF16), 1, 0).astype(BF16)
    out_ref[:, depth:] = state_ref[...]


def expert_down(hs, weights, states, tiles=2):
    rows, units = hs[1].shape
    group = rows // tiles
    width = weights[0].shape[1]
    out_rows = NY * rows

    def spec(h):
        if h.ndim == 2:
            return pl.BlockSpec((group, units), lambda n: (n, 0))
        return pl.BlockSpec((h.shape[0], group, units), lambda n: (0, n, 0))

    return pl.pallas_call(
        down_kernel,
        grid=(tiles,),
        in_specs=[spec(h) for h in hs]
        + [pl.BlockSpec(w.shape, lambda n: (0, 0)) for w in weights]
        + [pl.BlockSpec((out_rows // tiles, DK), lambda n: (n, 0))],
        out_specs=pl.BlockSpec((out_rows // tiles, width + DK), lambda n: (n, 0)),
        out_shape=jax.ShapeDtypeStruct((out_rows, width + DK), BF16),
        compiler_params=pltpu.CompilerParams(dimension_semantics=("arbitrary",)),
        cost_estimate=pl.CostEstimate(
            flops=2 * out_rows * units * NY * width,
            transcendentals=0,
            bytes_accessed=8 * 10**6,
        ),
        name="expert_down",
    )(*hs, *weights, states)


def combine_kernel(idx_ref, back_ref, slot_ref, weight_ref, o0, o1, o2, o3, *, part):
    y = idx_ref[0] // 2
    core = idx_ref[0] % 2
    firsts = [(((y + i) % NY) * 2 + core) * part for i in range(NY)]
    own = own_columns(slot_ref[...], firsts, part)
    block = lax.broadcasted_iota(jnp.int32, own.shape, 1) // part
    spot = (own // CAP) * (CAP * NY) + block * CAP + own % CAP
    place = lax.broadcasted_iota(jnp.int32, (back_ref.shape[0], NY * part), 0)
    weight = jnp.concatenate(
        [weight_ref[pl.ds(pl.multiple_of(first, part), part), :] for first in firsts], axis=0
    )
    back = back_ref[...]
    mixed = None
    for j in range(2):
        chosen = jnp.where(place == spot[j : j + 1], 1.0, 0.0).astype(BF16)
        term = contract(chosen, back, 0, 0) * weight[:, j : j + 1]
        mixed = term if mixed is None else mixed + term
    for i, out in enumerate((o0, o1, o2, o3)):
        out[...] = mixed[i * part : (i + 1) * part].astype(out.dtype)


def combine(index, back, slots, weight, part, width):
    total = weight.shape[0]
    return pl.pallas_call(
        functools.partial(combine_kernel, part=part),
        grid_spec=pltpu.PrefetchScalarGridSpec(
            num_scalar_prefetch=1,
            grid=(1,),
            in_specs=[
                pl.BlockSpec((back.shape[0], width), lambda n, idx: (0, 0)),
                pl.BlockSpec((2, total), lambda n, idx: (0, 0)),
                pl.BlockSpec((total, 2), lambda n, idx: (0, 0)),
            ],
            out_specs=[pl.BlockSpec((part, width), lambda n, idx: (0, 0)) for _ in range(NY)],
        ),
        out_shape=[jax.ShapeDtypeStruct((part, width), BF16) for _ in range(NY)],
        name="combine",
    )(index, back, slots, weight)


def finish_kernel(idx_ref, p0, p1, p2, p3, gain_ref, out_ref):
    y = idx_ref[0] // 2
    width = p0.shape[1]
    pieces = [p[...].astype(F32) for p in (p0, p1, p2, p3)]
    square = sum(jnp.sum(p * p, axis=-1, keepdims=True) for p in pieces)
    scale = lax.rsqrt(square / (width * NY) + 1e-06)
    for i, piece in enumerate(pieces):
        columns = pl.ds(pl.multiple_of(((y + i) % NY) * width, width), width)
        out_ref[:, columns] = (piece * scale * gain_ref[:, columns]).astype(BF16)


def finish(index, pieces, gain):
    part, width = pieces[0].shape
    full = width * NY
    return pl.pallas_call(
        finish_kernel,
        grid_spec=pltpu.PrefetchScalarGridSpec(
            num_scalar_prefetch=1,
            grid=(1,),
            in_specs=[pl.BlockSpec((part, width), lambda n, idx: (0, 0)) for _ in pieces]
            + [pl.BlockSpec((1, full), lambda n, idx: (0, 0))],
            out_specs=pl.BlockSpec((part, full), lambda n, idx: (0, 0)),
        ),
        out_shape=jax.ShapeDtypeStruct((part, full), BF16),
        name="finish",
    )(index, *pieces, gain.reshape(1, full))


def from_right(x):
    return lax.ppermute(x, "y", ring(NY, -1))


def from_left(x):
    return lax.ppermute(x, "y", ring(NY, 1))


def on_device(
    queries,
    key_vectors,
    value_vectors,
    decay_logit,
    head_gain,
    routed_rows,
    pre_gain,
    expert_pick,
    route_weight,
    gate_weight,
    up_weight,
    down_weight,
    post_gain,
):
    y = lax.axis_index("y")
    core = lax.axis_index("c")
    experts = lax.axis_size(EP)
    part = routed_rows.shape[0] // (NY * 2)
    width = routed_rows.shape[1]
    index = (y * 2 + core).astype(jnp.int32).reshape(1)
    swap = [(0, 1), (1, 0)]

    outgoing, slots = dispatch(index, routed_rows, pre_gain, expert_pick, part, experts)
    arrived = exchange(outgoing.reshape(experts, 2 * CAP, width // 2))

    gate, up, down = gate_weight[0], up_weight[0], down_weight[0]
    weights = (gate, up, lax.ppermute(gate, "c", swap), lax.ppermute(up, "c", swap))
    cut = width // NY
    slices = [
        lax.dynamic_slice_in_dim(down, lax.rem(y + i, NY) * cut, cut, axis=1) for i in range(NY)
    ]
    mine = [slices[0]] + [
        lax.ppermute(slices[-m % NY], "y", ring(NY, -m)) for m in range(1, NY)
    ]
    local_out, query_carry, local_state = attn_local(
        queries, key_vectors, value_vectors, decay_logit
    )
    mine, local_state = lax.optimization_barrier((mine, local_state))
    arrived, local_state, mine = lax.optimization_barrier((arrived, local_state, mine))
    downs = []
    for piece in mine:
        downs += [piece, lax.ppermute(piece, "c", swap)]

    half = experts // 2
    top = arrived[:half].reshape(-1, width // 2)
    bottom = arrived[half:].reshape(-1, width // 2)
    right_top, right_bottom = from_right(top), from_right(bottom)
    left_top, left_bottom = from_left(top), from_left(bottom)
    far_top, far_bottom = from_left(left_top), from_right(right_bottom)

    chunk_states = exchange(local_state)
    before = prefix(chunk_states)
    sides, before = lax.optimization_barrier(
        ((right_top, right_bottom, left_top, left_bottom), before)
    )
    near = hidden_units([top, bottom, *sides], weights).reshape(3, -1, 2 * gate.shape[1])
    far = hidden_units([far_top, far_bottom], weights)
    near_left, near_right = from_left(near), from_right(near)
    far_left, far_right = from_left(far), from_right(far)
    acts = (
        near,
        far,
        near_right,
        far_right,
        from_left(near_left),
        from_right(far_right),
        near_left,
        far_left,
    )
    back = expert_down(acts, downs, before.reshape(-1, DK))
    returned = exchange(back.reshape(experts, NY * CAP, cut + DK)).reshape(-1, cut + DK)

    pieces = combine(index, returned, slots, route_weight, part, cut)
    gathered = [pieces[0]] + [
        lax.ppermute(pieces[-m % NY], "y", ring(NY, -m)) for m in range(1, NY)
    ]
    routed_out = finish(index, gathered, post_gain)
    mixed_heads = attn_out(local_out, query_carry, returned, head_gain, cut // DK)
    return (mixed_heads, routed_out)


def solution(mesh):
    ep, tp = mesh.shape["ep"], mesh.shape["tp"]
    torus = Mesh(mesh.devices.reshape(ep // 4, 4, NY, tp // NY), ("z", "x", "y", "c"))
    tpa = ("y", "c")
    placed = (
        P(EP, tpa),
        P(EP, tpa),
        P(EP, tpa),
        P(EP, tpa),
        P(),
        P(EP, None),
        P(),
        P(EP, None),
        P(EP, None),
        P(EP, None, tpa),
        P(EP, None, tpa),
        P(EP, tpa, None),
        P(),
    )
    return jax.shard_map(
        on_device,
        mesh=torus,
        in_specs=placed,
        out_specs=(P(EP, tpa), P(("z", "x", "y", "c"), None)),
        check_vma=False,
    )
```

```python
import functools

import jax
import jax.numpy as jnp
from jax import lax
from jax.experimental import pallas as pl
from jax.experimental.pallas import tpu as pltpu
from jax.sharding import Mesh
from jax.sharding import PartitionSpec as P


DK = 128
DV = 256
BLK = 64
VROWS = 16
CAP = 4
NY = 4
EP = ("z", "x")
F32 = jnp.float32
BF16 = jnp.bfloat16


def ring(size, step):
    return [(i, (i + step) % size) for i in range(size)]


def contract(a, b, dim_a, dim_b):
    return lax.dot_general(
        a, b, (((dim_a,), (dim_b,)), ((), ())), preferred_element_type=F32
    )


def attn_local_kernel(q_ref, k_ref, v_ref, g_ref, o_ref, qc_ref, st_ref, state, decay):
    step = pl.program_id(0)
    heads = state.shape[0]

    @pl.when(step == 0)
    def _():
        state[...] = jnp.zeros_like(state)
        decay[...] = jnp.zeros_like(decay)

    row = lax.broadcasted_iota(jnp.int32, (BLK, BLK), 0)
    col = lax.broadcasted_iota(jnp.int32, (BLK, BLK), 1)
    causal = row >= col
    before = decay[0:1, :]
    old = [state[h] for h in range(heads)]
    for b in range(q_ref.shape[0] // BLK):
        rows = slice(b * BLK, (b + 1) * BLK)
        logit = g_ref[rows, :]
        rate = (jnp.minimum(logit, 0.0) - jnp.log1p(jnp.exp(-jnp.abs(logit)))) * (1.0 / 16.0)
        cumulative = jnp.dot(
            causal.astype(F32), rate, precision=lax.Precision.HIGHEST, preferred_element_type=F32
        )
        ending = cumulative[BLK - 1 : BLK, :]
        q = q_ref[rows, :].astype(F32)
        k = k_ref[rows, :].astype(F32)
        query_decay = (q * jnp.exp(cumulative)).astype(BF16)
        key_decay = (k * jnp.exp(-cumulative)).astype(BF16)
        key_to_end = (k * jnp.exp(ending - cumulative)).astype(BF16)
        qc_ref[rows, :] = (q * jnp.exp(cumulative + before)).astype(BF16)
        before = before + ending
        step_decay = jnp.exp(ending)
        for h in range(heads):
            ks = slice(h * DK, (h + 1) * DK)
            vs = slice(h * DV, (h + 1) * DV)
            v = v_ref[rows, vs]
            scores = contract(query_decay[:, ks], key_decay[:, ks], 1, 1)
            weights = jnp.where(causal, scores, 0.0).astype(BF16)
            inside = contract(weights, v, 1, 0)
            o_ref[rows, vs] = inside + contract(query_decay[:, ks], old[h].astype(BF16), 1, 1)
            old[h] = old[h] * step_decay[:, ks] + contract(v, key_to_end[:, ks], 0, 0)
    decay[...] = jnp.broadcast_to(before, decay.shape)
    for h in range(heads):
        state[h] = old[h]

    @pl.when(step == pl.num_programs(0) - 1)
    def _():
        for h in range(heads):
            total = jnp.exp(decay[0:1, h * DK : (h + 1) * DK])
            chunks = DV // VROWS
            own = slice(h * chunks, (h + 1) * chunks)
            st_ref[own, 0:VROWS, :] = state[h].astype(BF16).reshape(chunks, VROWS, DK)
            st_ref[own, VROWS:, :] = jnp.broadcast_to(total, (chunks, 8, DK)).astype(BF16)


def attn_local(q, k, v, g):
    rows, keys = q.shape
    values = v.shape[1]
    heads = keys // DK
    tile = 4 * BLK
    return pl.pallas_call(
        attn_local_kernel,
        grid=(rows // tile,),
        in_specs=[
            pl.BlockSpec((tile, keys), lambda n: (n, 0)),
            pl.BlockSpec((tile, keys), lambda n: (n, 0)),
            pl.BlockSpec((tile, values), lambda n: (n, 0)),
            pl.BlockSpec((tile, keys), lambda n: (n, 0)),
        ],
        out_specs=[
            pl.BlockSpec((tile, values), lambda n: (n, 0)),
            pl.BlockSpec((tile, keys), lambda n: (n, 0)),
            pl.BlockSpec((heads * DV // VROWS, VROWS + 8, DK), lambda n: (0, 0, 0)),
        ],
        out_shape=[
            jax.ShapeDtypeStruct((rows, values), F32),
            jax.ShapeDtypeStruct((rows, keys), BF16),
            jax.ShapeDtypeStruct((heads * DV // VROWS, VROWS + 8, DK), BF16),
        ],
        scratch_shapes=[
            pltpu.VMEM((heads, DV, DK), F32),
            pltpu.VMEM((8, keys), F32),
        ],
        compiler_params=pltpu.CompilerParams(dimension_semantics=("arbitrary",)),
        cost_estimate=pl.CostEstimate(
            flops=8 * 10**9, transcendentals=10**6, bytes_accessed=6 * 10**6
        ),
        name="attn_local",
    )(q, k, v, g)


def attn_out_kernel(o_ref, qc_ref, in_ref, gain_ref, out_ref):
    gain = gain_ref[...]
    for h in range(in_ref.shape[0] // DV):
        vs = slice(h * DV, (h + 1) * DV)
        carried = contract(qc_ref[:, h * DK : (h + 1) * DK], in_ref[h * DV : (h + 1) * DV, :], 1, 1)
        total = o_ref[:, vs] + carried
        mean = jnp.mean(total * total, axis=-1, keepdims=True)
        out_ref[:, vs] = (total * lax.rsqrt(mean + 1e-06) * gain).astype(BF16)


def attn_out(o, qc, returned, gain, column):
    rows, values = o.shape
    tile = 256
    return pl.pallas_call(
        attn_out_kernel,
        grid=(rows // tile,),
        in_specs=[
            pl.BlockSpec((tile, values), lambda n: (n, 0)),
            pl.BlockSpec((tile, qc.shape[1]), lambda n: (n, 0)),
            pl.BlockSpec((returned.shape[0], DK), lambda n: (0, column)),
            pl.BlockSpec((1, DV), lambda n: (0, 0)),
        ],
        out_specs=pl.BlockSpec((tile, values), lambda n: (n, 0)),
        out_shape=jax.ShapeDtypeStruct((rows, values), BF16),
        compiler_params=pltpu.CompilerParams(dimension_semantics=("arbitrary",)),
        cost_estimate=pl.CostEstimate(
            flops=3 * 10**9, transcendentals=2048, bytes_accessed=4 * 10**6
        ),
        name="attn_out",
    )(o, qc, returned, gain.reshape(1, DV))


def prefix_kernel(in_ref, out_ref):
    carry = jnp.zeros((VROWS, DK), F32)
    for s in range(in_ref.shape[0]):
        out_ref[s] = carry.astype(BF16)
        decay = in_ref[s, VROWS:, :].astype(F32)[0:1, :]
        carry = carry * decay + in_ref[s, 0:VROWS, :].astype(F32)


def exchange(x):
    return lax.all_to_all(x, EP, split_axis=0, concat_axis=0, tiled=True)


def prefix(arrived):
    return pl.pallas_call(
        prefix_kernel,
        out_shape=jax.ShapeDtypeStruct((arrived.shape[0], VROWS, DK), BF16),
        name="prefix",
    )(arrived)


def own_columns(slots, first_rows, part):
    rows = slots.shape[1]
    wide = jnp.concatenate([slots] * 4, axis=0).astype(F32).astype(BF16)
    count = part * len(first_rows)
    row = lax.broadcasted_iota(jnp.int32, (rows, count), 0)
    col = lax.broadcasted_iota(jnp.int32, (rows, count), 1)
    source = col % part
    for i, first in enumerate(first_rows):
        source += jnp.where(col // part == i, first, 0)
    pick = jnp.where(row == source, 1.0, 0.0).astype(BF16)
    return contract(wide, pick, 1, 0)[0:2].astype(jnp.int32)


def dispatch_kernel(idx_ref, rows_ref, gain_ref, pick_ref, out_ref, slot_ref, *, part, experts):
    total = pick_ref.shape[1]
    pick = pick_ref[...]
    first = pick[0:1]
    second = pick[1:2]
    expert = lax.broadcasted_iota(jnp.int32, (experts, total), 0)
    hit0 = first == expert
    hit1 = second == expert
    named = jnp.where(hit0 | hit1, 1.0, 0.0).astype(BF16)
    row = lax.broadcasted_iota(jnp.int32, (total, total), 0)
    col = lax.broadcasted_iota(jnp.int32, (total, total), 1)
    earlier = (row < col) & (col // part == row // part)
    before = contract(named, jnp.where(earlier, 1.0, 0.0).astype(BF16), 1, 0)
    rank0 = jnp.sum(jnp.where(hit0, before, 0.0), axis=0, keepdims=True)
    rank1 = jnp.sum(jnp.where(hit1, before, 0.0), axis=0, keepdims=True)
    slots = pick * CAP + jnp.concatenate([rank0, rank1], axis=0).astype(jnp.int32)
    slot_ref[...] = slots
    values = rows_ref[...].astype(F32)
    mean = jnp.mean(values * values, axis=-1, keepdims=True)
    normed = (values * lax.rsqrt(mean + 1e-06) * gain_ref[...]).astype(BF16)
    own = own_columns(slots, [idx_ref[0] * part], part)
    place = lax.broadcasted_iota(jnp.int32, (out_ref.shape[0], part), 0)
    target = (place // (2 * CAP)) * CAP + place % CAP
    chosen = (own[0:1] == target) | (own[1:2] == target)
    half = out_ref.shape[1]
    total_out = None
    for h in range(2):
        mine = chosen & (place // CAP % 2 == h)
        piece = contract(
            jnp.where(mine, 1.0, 0.0).astype(BF16), normed[:, h * half : (h + 1) * half], 1, 0
        )
        total_out = piece if total_out is None else total_out + piece
    out_ref[...] = total_out.astype(BF16)


def dispatch(index, rows, gain, pick, part, experts):
    total, width = rows.shape
    return pl.pallas_call(
        functools.partial(dispatch_kernel, part=part, experts=experts),
        grid_spec=pltpu.PrefetchScalarGridSpec(
            num_scalar_prefetch=1,
            grid=(1,),
            in_specs=[
                pl.BlockSpec((part, width), lambda n, idx: (idx[0], 0)),
                pl.BlockSpec((1, width), lambda n, idx: (0, 0)),
                pl.BlockSpec((2, total), lambda n, idx: (0, 0)),
            ],
            out_specs=[
                pl.BlockSpec((experts * CAP * 2, width // 2), lambda n, idx: (0, 0)),
                pl.BlockSpec((2, total), lambda n, idx: (0, 0)),
            ],
        ),
        out_shape=[
            jax.ShapeDtypeStruct((experts * CAP * 2, width // 2), BF16),
            jax.ShapeDtypeStruct((2, total), jnp.int32),
        ],
        name="dispatch",
    )(index, rows, gain.reshape(1, width), pick.T)


def hidden_kernel(*refs, parts):
    xs = refs[:parts]
    weights = refs[parts : parts + 8]
    out_ref = refs[parts + 8]
    acc = refs[parts + 9]
    step = pl.program_id(0)
    rows = xs[0].shape[0]
    new = lax.broadcasted_iota(jnp.int32, (rows // 2, rows), 0)
    old = lax.broadcasted_iota(jnp.int32, (rows // 2, rows), 1)
    spread = (new // CAP) * (2 * CAP) + new % CAP
    x = []
    for h in range(2):
        order = jnp.where(old == spread + h * CAP, 1.0, 0.0).astype(BF16)
        x.append(
            jnp.concatenate([contract(order, r[...], 1, 0).astype(BF16) for r in xs], axis=0)
        )

    @pl.when(step == 0)
    def _():
        acc[...] = jnp.zeros_like(acc)

    width = weights[0].shape[1]
    for j in range(4):
        acc[:, j * width : (j + 1) * width] += contract(x[0], weights[2 * j][...], 1, 0) + contract(
            x[1], weights[2 * j + 1][...], 1, 0
        )

    @pl.when(step == pl.num_programs(0) - 1)
    def _():
        for j in range(2):
            gate = acc[:, 2 * j * width : (2 * j + 1) * width]
            up = acc[:, (2 * j + 1) * width : (2 * j + 2) * width]
            value = gate / (1.0 + jnp.exp(-gate)) * up
            out_ref[:, j * width : (j + 1) * width] = value.astype(BF16)


def hidden_units(xs, weights, ktile=512):
    rows = sum(x.shape[0] for x in xs) // 2
    depth, width = weights[0].shape
    steps = depth // 2 // ktile
    specs, doubled = [], []
    for w in weights:
        doubled += [w, w]
        specs += [
            pl.BlockSpec((ktile, width), lambda n: (n, 0)),
            pl.BlockSpec((ktile, width), lambda n: (n + steps, 0)),
        ]
    return pl.pallas_call(
        functools.partial(hidden_kernel, parts=len(xs)),
        grid=(steps,),
        in_specs=[pl.BlockSpec((x.shape[0], ktile), lambda n: (0, n)) for x in xs] + specs,
        out_specs=pl.BlockSpec((rows, 2 * width), lambda n: (0, 0)),
        out_shape=jax.ShapeDtypeStruct((rows, 2 * width), BF16),
        scratch_shapes=[pltpu.VMEM((rows, 4 * width), F32)],
        compiler_params=pltpu.CompilerParams(dimension_semantics=("arbitrary",)),
        cost_estimate=pl.CostEstimate(
            flops=8 * rows * depth * width,
            transcendentals=2 * rows * width,
            bytes_accessed=8 * depth * width + 2 * rows * depth,
        ),
        name="hidden_units",
    )(*xs, *doubled)


def in_blocks(near, far, shift):
    ordered = (near[0], near[1], far[...], near[2])
    return jnp.concatenate([ordered[(i - shift) % NY] for i in range(NY)], axis=0)


def down_sides_kernel(n0, f0, n1, f1, n3, f3, *rest):
    weights = rest[:6]
    out_ref = rest[6]
    width = weights[0].shape[0]
    total = None
    for m, act in enumerate((in_blocks(n0, f0, 0), in_blocks(n1, f1, 1), in_blocks(n3, f3, 3))):
        for c in range(2):
            term = contract(act[:, c * width : (c + 1) * width], weights[2 * m + c][...], 1, 0)
            total = term if total is None else total + term
    out_ref[...] = total


def down_far_kernel(n2, f2, *rest):
    weights = rest[:4]
    partial_ref, state_ref, out_ref = rest[4:7]
    width, depth = weights[0].shape
    group = f2.shape[0]
    rows = NY * group
    total = partial_ref[...]
    act = in_blocks(n2, f2, 2)
    for c in range(4):
        total += contract(act[:, c * width : (c + 1) * width], weights[c][...], 1, 0)
    new = lax.broadcasted_iota(jnp.int32, (rows, rows), 0)
    old = lax.broadcasted_iota(jnp.int32, (rows, rows), 1)
    want = (new // CAP % NY) * group + (new // (CAP * NY)) * CAP + new % CAP
    order = jnp.where(old == want, 1.0, 0.0).astype(BF16)
    out_ref[:, 0:depth] = contract(order, total.astype(BF16), 1, 0).astype(BF16)
    out_ref[:, depth:] = state_ref[...]


def expert_down(body, hs, weights, extra, columns, dtype, tiles=2):
    rows, units = hs[1].shape
    group = rows // tiles
    out_rows = NY * rows

    def spec(h):
        if h.ndim == 2:
            return pl.BlockSpec((group, units), lambda n: (n, 0))
        return pl.BlockSpec((h.shape[0], group, units), lambda n: (0, n, 0))

    return pl.pallas_call(
        body,
        grid=(tiles,),
        in_specs=[spec(h) for h in hs]
        + [pl.BlockSpec(w.shape, lambda n: (0, 0)) for w in weights]
        + [pl.BlockSpec((out_rows // tiles, x.shape[1]), lambda n: (n, 0)) for x in extra],
        out_specs=pl.BlockSpec((out_rows // tiles, columns), lambda n: (n, 0)),
        out_shape=jax.ShapeDtypeStruct((out_rows, columns), dtype),
        compiler_params=pltpu.CompilerParams(dimension_semantics=("arbitrary",)),
        cost_estimate=pl.CostEstimate(
            flops=2 * out_rows * columns * sum(w.shape[0] for w in weights),
            transcendentals=0,
            bytes_accessed=8 * 10**6,
        ),
    )(*hs, *weights, *extra)


def combine_kernel(idx_ref, back_ref, slot_ref, weight_ref, o0, o1, o2, o3, *, part):
    y = idx_ref[0] // 2
    core = idx_ref[0] % 2
    firsts = [(((y + i) % NY) * 2 + core) * part for i in range(NY)]
    own = own_columns(slot_ref[...], firsts, part)
    block = lax.broadcasted_iota(jnp.int32, own.shape, 1) // part
    spot = (own // CAP) * (CAP * NY) + block * CAP + own % CAP
    place = lax.broadcasted_iota(jnp.int32, (back_ref.shape[0], NY * part), 0)
    weight = jnp.concatenate(
        [weight_ref[pl.ds(pl.multiple_of(first, part), part), :] for first in firsts], axis=0
    )
    back = back_ref[...]
    mixed = None
    for j in range(2):
        chosen = jnp.where(place == spot[j : j + 1], 1.0, 0.0).astype(BF16)
        term = contract(chosen, back, 0, 0) * weight[:, j : j + 1]
        mixed = term if mixed is None else mixed + term
    for i, out in enumerate((o0, o1, o2, o3)):
        out[...] = mixed[i * part : (i + 1) * part].astype(out.dtype)


def combine(index, back, slots, weight, part, width):
    total = weight.shape[0]
    return pl.pallas_call(
        functools.partial(combine_kernel, part=part),
        grid_spec=pltpu.PrefetchScalarGridSpec(
            num_scalar_prefetch=1,
            grid=(1,),
            in_specs=[
                pl.BlockSpec((back.shape[0], width), lambda n, idx: (0, 0)),
                pl.BlockSpec((2, total), lambda n, idx: (0, 0)),
                pl.BlockSpec((total, 2), lambda n, idx: (0, 0)),
            ],
            out_specs=[pl.BlockSpec((part, width), lambda n, idx: (0, 0)) for _ in range(NY)],
        ),
        out_shape=[jax.ShapeDtypeStruct((part, width), BF16) for _ in range(NY)],
        name="combine",
    )(index, back, slots, weight)


def finish_kernel(idx_ref, p0, p1, p2, p3, gain_ref, out_ref):
    y = idx_ref[0] // 2
    width = p0.shape[1]
    pieces = [p[...].astype(F32) for p in (p0, p1, p2, p3)]
    square = sum(jnp.sum(p * p, axis=-1, keepdims=True) for p in pieces)
    scale = lax.rsqrt(square / (width * NY) + 1e-06)
    for i, piece in enumerate(pieces):
        columns = pl.ds(pl.multiple_of(((y + i) % NY) * width, width), width)
        out_ref[:, columns] = (piece * scale * gain_ref[:, columns]).astype(BF16)


def finish(index, pieces, gain):
    part, width = pieces[0].shape
    full = width * NY
    return pl.pallas_call(
        finish_kernel,
        grid_spec=pltpu.PrefetchScalarGridSpec(
            num_scalar_prefetch=1,
            grid=(1,),
            in_specs=[pl.BlockSpec((part, width), lambda n, idx: (0, 0)) for _ in pieces]
            + [pl.BlockSpec((1, full), lambda n, idx: (0, 0))],
            out_specs=pl.BlockSpec((part, full), lambda n, idx: (0, 0)),
        ),
        out_shape=jax.ShapeDtypeStruct((part, full), BF16),
        name="finish",
    )(index, *pieces, gain.reshape(1, full))


def from_right(x):
    return lax.ppermute(x, "y", ring(NY, -1))


def from_left(x):
    return lax.ppermute(x, "y", ring(NY, 1))


def on_device(
    queries,
    key_vectors,
    value_vectors,
    decay_logit,
    head_gain,
    routed_rows,
    pre_gain,
    expert_pick,
    route_weight,
    gate_weight,
    up_weight,
    down_weight,
    post_gain,
):
    y = lax.axis_index("y")
    core = lax.axis_index("c")
    experts = lax.axis_size(EP)
    part = routed_rows.shape[0] // (NY * 2)
    width = routed_rows.shape[1]
    index = (y * 2 + core).astype(jnp.int32).reshape(1)
    swap = [(0, 1), (1, 0)]

    outgoing, slots = dispatch(index, routed_rows, pre_gain, expert_pick, part, experts)
    arrived = exchange(outgoing.reshape(experts, 2 * CAP, width // 2))

    gate, up, down = gate_weight[0], up_weight[0], down_weight[0]
    weights = (gate, up, lax.ppermute(gate, "c", swap), lax.ppermute(up, "c", swap))
    cut = width // NY
    slices = [
        lax.dynamic_slice_in_dim(down, lax.rem(y + i, NY) * cut, cut, axis=1) for i in range(NY)
    ]
    middle = down.shape[0] // 2
    mine = [
        slices[0],
        from_right(slices[3]),
        from_left(slices[1]),
        from_left(slices[2][:middle]),
        from_right(slices[2][middle:]),
    ]
    local_out, query_carry, local_state = attn_local(
        queries, key_vectors, value_vectors, decay_logit
    )
    mine, _ = lax.optimization_barrier((mine, local_state))
    mine[3], mine[4] = from_left(mine[3]), from_right(mine[4])
    arrived, local_state = lax.optimization_barrier((arrived, local_state))
    d0, d1, d3, d2a, d2b = [(piece, lax.ppermute(piece, "c", swap)) for piece in mine]

    half = experts // 2
    top = arrived[:half].reshape(-1, width // 2)
    bottom = arrived[half:].reshape(-1, width // 2)
    right_top, right_bottom = from_right(top), from_right(bottom)
    left_top, left_bottom = from_left(top), from_left(bottom)
    far_top, far_bottom = from_left(left_top), from_right(right_bottom)

    chunk_states = exchange(local_state)
    before = prefix(chunk_states)
    sides, before = lax.optimization_barrier(
        ((right_top, right_bottom, left_top, left_bottom), before)
    )
    near = hidden_units([top, bottom, *sides], weights).reshape(3, -1, 2 * gate.shape[1])
    far = hidden_units([far_top, far_bottom], weights)
    near_left, near_right = from_left(near), from_right(near)
    far_left, far_right = from_left(far), from_right(far)
    near_passed, far = lax.optimization_barrier((near_left, far))
    near_far, far_far = from_left(near_passed), from_right(far_right)
    partial = expert_down(
        down_sides_kernel,
        (near, far, near_right, far_right, near_left, far_left),
        (*d0, *d1, *d3),
        (),
        cut,
        F32,
    )
    back = expert_down(
        down_far_kernel,
        (near_far, far_far),
        (d2a[0], d2b[0], d2a[1], d2b[1]),
        (partial, before.reshape(-1, DK)),
        cut + DK,
        BF16,
    )
    returned = exchange(back.reshape(experts, NY * CAP, cut + DK)).reshape(-1, cut + DK)

    pieces = combine(index, returned, slots, route_weight, part, cut)
    gathered = [pieces[0]] + [
        lax.ppermute(pieces[-m % NY], "y", ring(NY, -m)) for m in range(1, NY)
    ]
    routed_out = finish(index, gathered, post_gain)
    mixed_heads = attn_out(local_out, query_carry, returned, head_gain, cut // DK)
    return (mixed_heads, routed_out)


def solution(mesh):
    ep, tp = mesh.shape["ep"], mesh.shape["tp"]
    torus = Mesh(mesh.devices.reshape(ep // 4, 4, NY, tp // NY), ("z", "x", "y", "c"))
    tpa = ("y", "c")
    placed = (
        P(EP, tpa),
        P(EP, tpa),
        P(EP, tpa),
        P(EP, tpa),
        P(),
        P(EP, None),
        P(),
        P(EP, None),
        P(EP, None),
        P(EP, None, tpa),
        P(EP, None, tpa),
        P(EP, tpa, None),
        P(),
    )
    return jax.shard_map(
        on_device,
        mesh=torus,
        in_specs=placed,
        out_specs=(P(EP, tpa), P(("z", "x", "y", "c"), None)),
        check_vma=False,
    )
```

```python
import functools

import jax
import jax.numpy as jnp
from jax import lax
from jax.experimental import pallas as pl
from jax.experimental.pallas import tpu as pltpu
from jax.sharding import Mesh
from jax.sharding import PartitionSpec as P


DK = 128
DV = 256
BLK = 64
VROWS = 16
CAP = 4
NY = 4
EP = ("z", "x")
F32 = jnp.float32
BF16 = jnp.bfloat16


def ring(size, step):
    return [(i, (i + step) % size) for i in range(size)]


def contract(a, b, dim_a, dim_b):
    return lax.dot_general(
        a, b, (((dim_a,), (dim_b,)), ((), ())), preferred_element_type=F32
    )


def attn_local_kernel(q_ref, k_ref, v_ref, g_ref, o_ref, qc_ref, st_ref, state, decay):
    step = pl.program_id(0)
    heads = state.shape[0]

    @pl.when(step == 0)
    def _():
        state[...] = jnp.zeros_like(state)
        decay[...] = jnp.zeros_like(decay)

    row = lax.broadcasted_iota(jnp.int32, (BLK, BLK), 0)
    col = lax.broadcasted_iota(jnp.int32, (BLK, BLK), 1)
    causal = row >= col
    before = decay[0:1, :]
    old = [state[h] for h in range(heads)]
    for b in range(q_ref.shape[0] // BLK):
        rows = slice(b * BLK, (b + 1) * BLK)
        logit = g_ref[rows, :]
        rate = (jnp.minimum(logit, 0.0) - jnp.log1p(jnp.exp(-jnp.abs(logit)))) * (1.0 / 16.0)
        cumulative = jnp.dot(
            causal.astype(F32), rate, precision=lax.Precision.HIGHEST, preferred_element_type=F32
        )
        ending = cumulative[BLK - 1 : BLK, :]
        q = q_ref[rows, :].astype(F32)
        k = k_ref[rows, :].astype(F32)
        query_decay = (q * jnp.exp(cumulative)).astype(BF16)
        key_decay = (k * jnp.exp(-cumulative)).astype(BF16)
        key_to_end = (k * jnp.exp(ending - cumulative)).astype(BF16)
        qc_ref[rows, :] = (q * jnp.exp(cumulative + before)).astype(BF16)
        before = before + ending
        step_decay = jnp.exp(ending)
        for h in range(heads):
            ks = slice(h * DK, (h + 1) * DK)
            vs = slice(h * DV, (h + 1) * DV)
            v = v_ref[rows, vs]
            scores = contract(query_decay[:, ks], key_decay[:, ks], 1, 1)
            weights = jnp.where(causal, scores, 0.0).astype(BF16)
            inside = contract(weights, v, 1, 0)
            o_ref[rows, vs] = inside + contract(query_decay[:, ks], old[h].astype(BF16), 1, 1)
            old[h] = old[h] * step_decay[:, ks] + contract(v, key_to_end[:, ks], 0, 0)
    decay[...] = jnp.broadcast_to(before, decay.shape)
    for h in range(heads):
        state[h] = old[h]

    @pl.when(step == pl.num_programs(0) - 1)
    def _():
        for h in range(heads):
            total = jnp.exp(decay[0:1, h * DK : (h + 1) * DK])
            chunks = DV // VROWS
            own = slice(h * chunks, (h + 1) * chunks)
            st_ref[own, 0:VROWS, :] = state[h].astype(BF16).reshape(chunks, VROWS, DK)
            st_ref[own, VROWS:, :] = jnp.broadcast_to(total, (chunks, 8, DK)).astype(BF16)


def attn_local(q, k, v, g):
    rows, keys = q.shape
    values = v.shape[1]
    heads = keys // DK
    tile = 4 * BLK
    return pl.pallas_call(
        attn_local_kernel,
        grid=(rows // tile,),
        in_specs=[
            pl.BlockSpec((tile, keys), lambda n: (n, 0)),
            pl.BlockSpec((tile, keys), lambda n: (n, 0)),
            pl.BlockSpec((tile, values), lambda n: (n, 0)),
            pl.BlockSpec((tile, keys), lambda n: (n, 0)),
        ],
        out_specs=[
            pl.BlockSpec((tile, values), lambda n: (n, 0)),
            pl.BlockSpec((tile, keys), lambda n: (n, 0)),
            pl.BlockSpec((heads * DV // VROWS, VROWS + 8, DK), lambda n: (0, 0, 0)),
        ],
        out_shape=[
            jax.ShapeDtypeStruct((rows, values), F32),
            jax.ShapeDtypeStruct((rows, keys), BF16),
            jax.ShapeDtypeStruct((heads * DV // VROWS, VROWS + 8, DK), BF16),
        ],
        scratch_shapes=[
            pltpu.VMEM((heads, DV, DK), F32),
            pltpu.VMEM((8, keys), F32),
        ],
        compiler_params=pltpu.CompilerParams(dimension_semantics=("arbitrary",)),
        cost_estimate=pl.CostEstimate(
            flops=8 * 10**9, transcendentals=10**6, bytes_accessed=6 * 10**6
        ),
        name="attn_local",
    )(q, k, v, g)


def attn_out_kernel(o_ref, qc_ref, in_ref, gain_ref, out_ref):
    gain = gain_ref[...]
    for h in range(in_ref.shape[0] // DV):
        vs = slice(h * DV, (h + 1) * DV)
        carried = contract(qc_ref[:, h * DK : (h + 1) * DK], in_ref[h * DV : (h + 1) * DV, :], 1, 1)
        total = o_ref[:, vs] + carried
        mean = jnp.mean(total * total, axis=-1, keepdims=True)
        out_ref[:, vs] = (total * lax.rsqrt(mean + 1e-06) * gain).astype(BF16)


def attn_out(o, qc, incoming, gain):
    rows, values = o.shape
    tile = 256
    return pl.pallas_call(
        attn_out_kernel,
        grid=(rows // tile,),
        in_specs=[
            pl.BlockSpec((tile, values), lambda n: (n, 0)),
            pl.BlockSpec((tile, qc.shape[1]), lambda n: (n, 0)),
            pl.BlockSpec(incoming.shape, lambda n: (0, 0)),
            pl.BlockSpec((1, DV), lambda n: (0, 0)),
        ],
        out_specs=pl.BlockSpec((tile, values), lambda n: (n, 0)),
        out_shape=jax.ShapeDtypeStruct((rows, values), BF16),
        compiler_params=pltpu.CompilerParams(dimension_semantics=("arbitrary",)),
        cost_estimate=pl.CostEstimate(
            flops=3 * 10**9, transcendentals=2048, bytes_accessed=4 * 10**6
        ),
        name="attn_out",
    )(o, qc, incoming, gain.reshape(1, DV))


def prefix_kernel(in_ref, out_ref):
    carry = jnp.zeros((VROWS, DK), F32)
    for s in range(in_ref.shape[0]):
        out_ref[s] = carry.astype(BF16)
        decay = in_ref[s, VROWS:, :].astype(F32)[0:1, :]
        carry = carry * decay + in_ref[s, 0:VROWS, :].astype(F32)


def exchange(x):
    return lax.all_to_all(x, EP, split_axis=0, concat_axis=0, tiled=True)


def prefix(arrived):
    return pl.pallas_call(
        prefix_kernel,
        out_shape=jax.ShapeDtypeStruct((arrived.shape[0], VROWS, DK), BF16),
        name="prefix",
    )(arrived)


def own_columns(slots, first_rows, part):
    rows = slots.shape[1]
    wide = jnp.concatenate([slots] * 4, axis=0).astype(F32).astype(BF16)
    count = part * len(first_rows)
    row = lax.broadcasted_iota(jnp.int32, (rows, count), 0)
    col = lax.broadcasted_iota(jnp.int32, (rows, count), 1)
    source = col % part
    for i, first in enumerate(first_rows):
        source += jnp.where(col // part == i, first, 0)
    pick = jnp.where(row == source, 1.0, 0.0).astype(BF16)
    return contract(wide, pick, 1, 0)[0:2].astype(jnp.int32)


def dispatch_kernel(idx_ref, rows_ref, gain_ref, pick_ref, out_ref, slot_ref, *, part, experts):
    total = pick_ref.shape[1]
    pick = pick_ref[...]
    first = pick[0:1]
    second = pick[1:2]
    expert = lax.broadcasted_iota(jnp.int32, (experts, total), 0)
    hit0 = first == expert
    hit1 = second == expert
    named = jnp.where(hit0 | hit1, 1.0, 0.0).astype(BF16)
    row = lax.broadcasted_iota(jnp.int32, (total, total), 0)
    col = lax.broadcasted_iota(jnp.int32, (total, total), 1)
    earlier = (row < col) & (col // part == row // part)
    before = contract(named, jnp.where(earlier, 1.0, 0.0).astype(BF16), 1, 0)
    rank0 = jnp.sum(jnp.where(hit0, before, 0.0), axis=0, keepdims=True)
    rank1 = jnp.sum(jnp.where(hit1, before, 0.0), axis=0, keepdims=True)
    slots = pick * CAP + jnp.concatenate([rank0, rank1], axis=0).astype(jnp.int32)
    slot_ref[...] = slots
    values = rows_ref[...].astype(F32)
    mean = jnp.mean(values * values, axis=-1, keepdims=True)
    normed = (values * lax.rsqrt(mean + 1e-06) * gain_ref[...]).astype(BF16)
    own = own_columns(slots, [idx_ref[0] * part], part)
    place = lax.broadcasted_iota(jnp.int32, (out_ref.shape[0], part), 0)
    target = (place // (2 * CAP)) * CAP + place % CAP
    chosen = (own[0:1] == target) | (own[1:2] == target)
    half = out_ref.shape[1]
    total_out = None
    for h in range(2):
        mine = chosen & (place // CAP % 2 == h)
        piece = contract(
            jnp.where(mine, 1.0, 0.0).astype(BF16), normed[:, h * half : (h + 1) * half], 1, 0
        )
        total_out = piece if total_out is None else total_out + piece
    out_ref[...] = total_out.astype(BF16)


def dispatch(index, rows, gain, pick, part, experts):
    total, width = rows.shape
    return pl.pallas_call(
        functools.partial(dispatch_kernel, part=part, experts=experts),
        grid_spec=pltpu.PrefetchScalarGridSpec(
            num_scalar_prefetch=1,
            grid=(1,),
            in_specs=[
                pl.BlockSpec((part, width), lambda n, idx: (idx[0], 0)),
                pl.BlockSpec((1, width), lambda n, idx: (0, 0)),
                pl.BlockSpec((2, total), lambda n, idx: (0, 0)),
            ],
            out_specs=[
                pl.BlockSpec((experts * CAP * 2, width // 2), lambda n, idx: (0, 0)),
                pl.BlockSpec((2, total), lambda n, idx: (0, 0)),
            ],
        ),
        out_shape=[
            jax.ShapeDtypeStruct((experts * CAP * 2, width // 2), BF16),
            jax.ShapeDtypeStruct((2, total), jnp.int32),
        ],
        name="dispatch",
    )(index, rows, gain.reshape(1, width), pick.T)


def hidden_kernel(*refs, parts):
    xs = refs[:parts]
    weights = refs[parts : parts + 8]
    out_ref = refs[parts + 8]
    acc = refs[parts + 9]
    step = pl.program_id(0)
    rows = xs[0].shape[0]
    new = lax.broadcasted_iota(jnp.int32, (rows // 2, rows), 0)
    old = lax.broadcasted_iota(jnp.int32, (rows // 2, rows), 1)
    spread = (new // CAP) * (2 * CAP) + new % CAP
    x = []
    for h in range(2):
        order = jnp.where(old == spread + h * CAP, 1.0, 0.0).astype(BF16)
        x.append(
            jnp.concatenate([contract(order, r[...], 1, 0).astype(BF16) for r in xs], axis=0)
        )

    @pl.when(step == 0)
    def _():
        acc[...] = jnp.zeros_like(acc)

    width = weights[0].shape[1]
    for j in range(4):
        acc[:, j * width : (j + 1) * width] += contract(x[0], weights[2 * j][...], 1, 0) + contract(
            x[1], weights[2 * j + 1][...], 1, 0
        )

    @pl.when(step == pl.num_programs(0) - 1)
    def _():
        for j in range(2):
            gate = acc[:, 2 * j * width : (2 * j + 1) * width]
            up = acc[:, (2 * j + 1) * width : (2 * j + 2) * width]
            value = gate / (1.0 + jnp.exp(-gate)) * up
            out_ref[:, j * width : (j + 1) * width] = value.astype(BF16)


def hidden_units(xs, weights, ktile=512):
    rows = sum(x.shape[0] for x in xs) // 2
    depth, width = weights[0].shape
    steps = depth // 2 // ktile
    specs, doubled = [], []
    for w in weights:
        doubled += [w, w]
        specs += [
            pl.BlockSpec((ktile, width), lambda n: (n, 0)),
            pl.BlockSpec((ktile, width), lambda n: (n + steps, 0)),
        ]
    return pl.pallas_call(
        functools.partial(hidden_kernel, parts=len(xs)),
        grid=(steps,),
        in_specs=[pl.BlockSpec((x.shape[0], ktile), lambda n: (0, n)) for x in xs] + specs,
        out_specs=pl.BlockSpec((rows, 2 * width), lambda n: (0, 0)),
        out_shape=jax.ShapeDtypeStruct((rows, 2 * width), BF16),
        scratch_shapes=[pltpu.VMEM((rows, 4 * width), F32)],
        compiler_params=pltpu.CompilerParams(dimension_semantics=("arbitrary",)),
        cost_estimate=pl.CostEstimate(
            flops=8 * rows * depth * width,
            transcendentals=2 * rows * width,
            bytes_accessed=8 * depth * width + 2 * rows * depth,
        ),
        name="hidden_units",
    )(*xs, *doubled)


def in_blocks(near, far, shift):
    ordered = (near[0], near[1], far[...], near[2])
    return jnp.concatenate([ordered[(i - shift) % NY] for i in range(NY)], axis=0)


def down_kernel(n0, f0, n1, f1, n2, f2, n3, f3, *rest):
    weights = rest[:10]
    out_ref = rest[10]
    rows, _ = out_ref.shape
    group = rows // NY
    total = None
    used = 0
    for m, pair in enumerate(((n0, f0), (n1, f1), (n2, f2), (n3, f3))):
        act = in_blocks(*pair, m)
        start = 0
        while start < act.shape[1]:
            weight = weights[used]
            stop = start + weight.shape[0]
            term = contract(act[:, start:stop], weight[...], 1, 0)
            total = term if total is None else total + term
            start = stop
            used += 1
    new = lax.broadcasted_iota(jnp.int32, (rows, rows), 0)
    old = lax.broadcasted_iota(jnp.int32, (rows, rows), 1)
    want = (new // CAP % NY) * group + (new // (CAP * NY)) * CAP + new % CAP
    order = jnp.where(old == want, 1.0, 0.0).astype(BF16)
    out_ref[...] = contract(order, total.astype(BF16), 1, 0).astype(BF16)


def expert_down(hs, weights, tiles=2):
    rows, units = hs[1].shape
    group = rows // tiles
    out_rows = NY * rows
    columns = weights[0].shape[1]

    def spec(h):
        if h.ndim == 2:
            return pl.BlockSpec((group, units), lambda n: (n, 0))
        return pl.BlockSpec((h.shape[0], group, units), lambda n: (0, n, 0))

    return pl.pallas_call(
        down_kernel,
        grid=(tiles,),
        in_specs=[spec(h) for h in hs]
        + [pl.BlockSpec(w.shape, lambda n: (0, 0)) for w in weights],
        out_specs=pl.BlockSpec((out_rows // tiles, columns), lambda n: (n, 0)),
        out_shape=jax.ShapeDtypeStruct((out_rows, columns), BF16),
        compiler_params=pltpu.CompilerParams(dimension_semantics=("arbitrary",)),
        cost_estimate=pl.CostEstimate(
            flops=2 * out_rows * columns * sum(w.shape[0] for w in weights),
            transcendentals=0,
            bytes_accessed=8 * 10**6,
        ),
        name="expert_down",
    )(*hs, *weights)


def combine_kernel(idx_ref, back_ref, slot_ref, weight_ref, o0, o1, o2, o3, *, part):
    y = idx_ref[0] // 2
    core = idx_ref[0] % 2
    firsts = [(((y + i) % NY) * 2 + core) * part for i in range(NY)]
    own = own_columns(slot_ref[...], firsts, part)
    block = lax.broadcasted_iota(jnp.int32, own.shape, 1) // part
    spot = (own // CAP) * (CAP * NY) + block * CAP + own % CAP
    place = lax.broadcasted_iota(jnp.int32, (back_ref.shape[0], NY * part), 0)
    weight = jnp.concatenate(
        [weight_ref[pl.ds(pl.multiple_of(first, part), part), :] for first in firsts], axis=0
    )
    back = back_ref[...]
    mixed = None
    for j in range(2):
        chosen = jnp.where(place == spot[j : j + 1], 1.0, 0.0).astype(BF16)
        term = contract(chosen, back, 0, 0) * weight[:, j : j + 1]
        mixed = term if mixed is None else mixed + term
    for i, out in enumerate((o0, o1, o2, o3)):
        out[...] = mixed[i * part : (i + 1) * part].astype(out.dtype)


def combine(index, back, slots, weight, part, tiles=4):
    total = weight.shape[0]
    width = back.shape[1]
    tile = width // tiles
    return pl.pallas_call(
        functools.partial(combine_kernel, part=part),
        grid_spec=pltpu.PrefetchScalarGridSpec(
            num_scalar_prefetch=1,
            grid=(tiles,),
            in_specs=[
                pl.BlockSpec((back.shape[0], tile), lambda n, idx: (0, n)),
                pl.BlockSpec((2, total), lambda n, idx: (0, 0)),
                pl.BlockSpec((total, 2), lambda n, idx: (0, 0)),
            ],
            out_specs=[pl.BlockSpec((part, tile), lambda n, idx: (0, n)) for _ in range(NY)],
        ),
        out_shape=[jax.ShapeDtypeStruct((part, width), BF16) for _ in range(NY)],
        name="combine",
    )(index, back, slots, weight)


def finish_kernel(idx_ref, p0, p1, p2, p3, gain_ref, out_ref):
    y = idx_ref[0] // 2
    width = p0.shape[1]
    pieces = [p[...].astype(F32) for p in (p0, p1, p2, p3)]
    square = sum(jnp.sum(p * p, axis=-1, keepdims=True) for p in pieces)
    scale = lax.rsqrt(square / (width * NY) + 1e-06)
    for i, piece in enumerate(pieces):
        columns = pl.ds(pl.multiple_of(((y + i) % NY) * width, width), width)
        out_ref[:, columns] = (piece * scale * gain_ref[:, columns]).astype(BF16)


def finish(index, pieces, gain):
    part, width = pieces[0].shape
    full = width * NY
    return pl.pallas_call(
        finish_kernel,
        grid_spec=pltpu.PrefetchScalarGridSpec(
            num_scalar_prefetch=1,
            grid=(1,),
            in_specs=[pl.BlockSpec((part, width), lambda n, idx: (0, 0)) for _ in pieces]
            + [pl.BlockSpec((1, full), lambda n, idx: (0, 0))],
            out_specs=pl.BlockSpec((part, full), lambda n, idx: (0, 0)),
        ),
        out_shape=jax.ShapeDtypeStruct((part, full), BF16),
        name="finish",
    )(index, *pieces, gain.reshape(1, full))


def from_right(x):
    return lax.ppermute(x, "y", ring(NY, -1))


def from_left(x):
    return lax.ppermute(x, "y", ring(NY, 1))


def on_device(
    queries,
    key_vectors,
    value_vectors,
    decay_logit,
    head_gain,
    routed_rows,
    pre_gain,
    expert_pick,
    route_weight,
    gate_weight,
    up_weight,
    down_weight,
    post_gain,
):
    y = lax.axis_index("y")
    core = lax.axis_index("c")
    experts = lax.axis_size(EP)
    part = routed_rows.shape[0] // (NY * 2)
    width = routed_rows.shape[1]
    index = (y * 2 + core).astype(jnp.int32).reshape(1)
    swap = [(0, 1), (1, 0)]

    outgoing, slots = dispatch(index, routed_rows, pre_gain, expert_pick, part, experts)
    arrived = exchange(outgoing.reshape(experts, 2 * CAP, width // 2))

    gate, up, down = gate_weight[0], up_weight[0], down_weight[0]
    weights = (gate, up, lax.ppermute(gate, "c", swap), lax.ppermute(up, "c", swap))
    cut = width // NY
    slices = [
        lax.dynamic_slice_in_dim(down, lax.rem(y + i, NY) * cut, cut, axis=1) for i in range(NY)
    ]
    middle = down.shape[0] // 2
    mine = [
        slices[0],
        from_right(slices[3]),
        from_left(slices[1]),
        from_left(slices[2][:middle]),
        from_right(slices[2][middle:]),
    ]
    local_out, query_carry, local_state = attn_local(
        queries, key_vectors, value_vectors, decay_logit
    )
    mine, _ = lax.optimization_barrier((mine, local_state))
    mine[3], mine[4] = from_left(mine[3]), from_right(mine[4])
    arrived, local_state, mine = lax.optimization_barrier((arrived, local_state, mine))
    d0, d1, d3, d2a, d2b = [(piece, lax.ppermute(piece, "c", swap)) for piece in mine]

    half = experts // 2
    top = arrived[:half].reshape(-1, width // 2)
    bottom = arrived[half:].reshape(-1, width // 2)
    right_top, right_bottom = from_right(top), from_right(bottom)
    left_top, left_bottom = from_left(top), from_left(bottom)
    far_top, far_bottom = from_left(left_top), from_right(right_bottom)

    chunk_states = exchange(local_state)
    before = prefix(chunk_states)
    sides, before = lax.optimization_barrier(
        ((right_top, right_bottom, left_top, left_bottom), before)
    )
    near = hidden_units([top, bottom, *sides], weights).reshape(3, -1, 2 * gate.shape[1])
    far = hidden_units([far_top, far_bottom], weights)
    near_left, near_right = from_left(near), from_right(near)
    far_left, far_right = from_left(far), from_right(far)
    near_passed, far = lax.optimization_barrier((near_left, far))
    near_far = from_left(near_passed)
    far_far = from_right(far_right)
    incoming = exchange(before)
    back = expert_down(
        (near, far, near_right, far_right, near_far, far_far, near_left, far_left),
        (*d0, *d1, d2a[0], d2b[0], d2a[1], d2b[1], *d3),
    )
    returned = exchange(back.reshape(experts, NY * CAP, cut)).reshape(-1, cut)
    mixed_heads = attn_out(local_out, query_carry, incoming.reshape(-1, DK), head_gain)
    returned, mixed_heads = lax.optimization_barrier((returned, mixed_heads))

    pieces = combine(index, returned, slots, route_weight, part)
    gathered = [pieces[0]] + [
        lax.ppermute(pieces[-m % NY], "y", ring(NY, -m)) for m in range(1, NY)
    ]
    routed_out = finish(index, gathered, post_gain)
    return (mixed_heads, routed_out)


def solution(mesh):
    ep, tp = mesh.shape["ep"], mesh.shape["tp"]
    torus = Mesh(mesh.devices.reshape(ep // 4, 4, NY, tp // NY), ("z", "x", "y", "c"))
    tpa = ("y", "c")
    placed = (
        P(EP, tpa),
        P(EP, tpa),
        P(EP, tpa),
        P(EP, tpa),
        P(),
        P(EP, None),
        P(),
        P(EP, None),
        P(EP, None),
        P(EP, None, tpa),
        P(EP, None, tpa),
        P(EP, tpa, None),
        P(),
    )
    return jax.shard_map(
        on_device,
        mesh=torus,
        in_specs=placed,
        out_specs=(P(EP, tpa), P(("z", "x", "y", "c"), None)),
        check_vma=False,
    )
```

```python
import functools

import jax
import jax.numpy as jnp
from jax import lax
from jax.experimental import pallas as pl
from jax.experimental.pallas import tpu as pltpu
from jax.sharding import Mesh
from jax.sharding import PartitionSpec as P


DK = 128
DV = 256
BLK = 64
VROWS = 16
CAP = 4
NY = 4
EP = ("z", "x")
F32 = jnp.float32
BF16 = jnp.bfloat16


def ring(size, step):
    return [(i, (i + step) % size) for i in range(size)]


def contract(a, b, dim_a, dim_b):
    return lax.dot_general(
        a, b, (((dim_a,), (dim_b,)), ((), ())), preferred_element_type=F32
    )


def attn_local_kernel(q_ref, k_ref, v_ref, g_ref, o_ref, qc_ref, st_ref, state, decay):
    step = pl.program_id(0)
    heads = state.shape[0]

    @pl.when(step == 0)
    def _():
        state[...] = jnp.zeros_like(state)
        decay[...] = jnp.zeros_like(decay)

    row = lax.broadcasted_iota(jnp.int32, (BLK, BLK), 0)
    col = lax.broadcasted_iota(jnp.int32, (BLK, BLK), 1)
    causal = row >= col
    before = decay[0:1, :]
    old = [state[h] for h in range(heads)]
    for b in range(q_ref.shape[0] // BLK):
        rows = slice(b * BLK, (b + 1) * BLK)
        logit = g_ref[rows, :]
        rate = (jnp.minimum(logit, 0.0) - jnp.log1p(jnp.exp(-jnp.abs(logit)))) * (1.0 / 16.0)
        cumulative = jnp.dot(
            causal.astype(F32), rate, precision=lax.Precision.HIGHEST, preferred_element_type=F32
        )
        ending = cumulative[BLK - 1 : BLK, :]
        q = q_ref[rows, :].astype(F32)
        k = k_ref[rows, :].astype(F32)
        query_decay = (q * jnp.exp(cumulative)).astype(BF16)
        key_decay = (k * jnp.exp(-cumulative)).astype(BF16)
        key_to_end = (k * jnp.exp(ending - cumulative)).astype(BF16)
        qc_ref[rows, :] = (q * jnp.exp(cumulative + before)).astype(BF16)
        before = before + ending
        step_decay = jnp.exp(ending)
        for h in range(heads):
            ks = slice(h * DK, (h + 1) * DK)
            vs = slice(h * DV, (h + 1) * DV)
            v = v_ref[rows, vs]
            scores = contract(query_decay[:, ks], key_decay[:, ks], 1, 1)
            weights = jnp.where(causal, scores, 0.0).astype(BF16)
            inside = contract(weights, v, 1, 0)
            o_ref[rows, vs] = inside + contract(query_decay[:, ks], old[h].astype(BF16), 1, 1)
            old[h] = old[h] * step_decay[:, ks] + contract(v, key_to_end[:, ks], 0, 0)
    decay[...] = jnp.broadcast_to(before, decay.shape)
    for h in range(heads):
        state[h] = old[h]

    @pl.when(step == pl.num_programs(0) - 1)
    def _():
        for h in range(heads):
            total = jnp.exp(decay[0:1, h * DK : (h + 1) * DK])
            chunks = DV // VROWS
            own = slice(h * chunks, (h + 1) * chunks)
            st_ref[own, 0:VROWS, :] = state[h].astype(BF16).reshape(chunks, VROWS, DK)
            st_ref[own, VROWS:, :] = jnp.broadcast_to(total, (chunks, 8, DK)).astype(BF16)


def attn_local(q, k, v, g):
    rows, keys = q.shape
    values = v.shape[1]
    heads = keys // DK
    tile = 4 * BLK
    return pl.pallas_call(
        attn_local_kernel,
        grid=(rows // tile,),
        in_specs=[
            pl.BlockSpec((tile, keys), lambda n: (n, 0)),
            pl.BlockSpec((tile, keys), lambda n: (n, 0)),
            pl.BlockSpec((tile, values), lambda n: (n, 0)),
            pl.BlockSpec((tile, keys), lambda n: (n, 0)),
        ],
        out_specs=[
            pl.BlockSpec((tile, values), lambda n: (n, 0)),
            pl.BlockSpec((tile, keys), lambda n: (n, 0)),
            pl.BlockSpec((heads * DV // VROWS, VROWS + 8, DK), lambda n: (0, 0, 0)),
        ],
        out_shape=[
            jax.ShapeDtypeStruct((rows, values), F32),
            jax.ShapeDtypeStruct((rows, keys), BF16),
            jax.ShapeDtypeStruct((heads * DV // VROWS, VROWS + 8, DK), BF16),
        ],
        scratch_shapes=[
            pltpu.VMEM((heads, DV, DK), F32),
            pltpu.VMEM((8, keys), F32),
        ],
        compiler_params=pltpu.CompilerParams(dimension_semantics=("arbitrary",)),
        cost_estimate=pl.CostEstimate(
            flops=8 * 10**9, transcendentals=10**6, bytes_accessed=6 * 10**6
        ),
        name="attn_local",
    )(q, k, v, g)


def attn_out_kernel(o_ref, qc_ref, in_ref, gain_ref, out_ref):
    gain = gain_ref[...]
    for h in range(in_ref.shape[0] // DV):
        vs = slice(h * DV, (h + 1) * DV)
        carried = contract(qc_ref[:, h * DK : (h + 1) * DK], in_ref[h * DV : (h + 1) * DV, :], 1, 1)
        total = o_ref[:, vs] + carried
        mean = jnp.mean(total * total, axis=-1, keepdims=True)
        out_ref[:, vs] = (total * lax.rsqrt(mean + 1e-06) * gain).astype(BF16)


def attn_out(o, qc, returned, gain, column):
    rows, values = o.shape
    tile = 256
    return pl.pallas_call(
        attn_out_kernel,
        grid=(rows // tile,),
        in_specs=[
            pl.BlockSpec((tile, values), lambda n: (n, 0)),
            pl.BlockSpec((tile, qc.shape[1]), lambda n: (n, 0)),
            pl.BlockSpec((returned.shape[0], DK), lambda n: (0, column)),
            pl.BlockSpec((1, DV), lambda n: (0, 0)),
        ],
        out_specs=pl.BlockSpec((tile, values), lambda n: (n, 0)),
        out_shape=jax.ShapeDtypeStruct((rows, values), BF16),
        compiler_params=pltpu.CompilerParams(dimension_semantics=("arbitrary",)),
        cost_estimate=pl.CostEstimate(
            flops=3 * 10**9, transcendentals=2048, bytes_accessed=4 * 10**6
        ),
        name="attn_out",
    )(o, qc, returned, gain.reshape(1, DV))


def prefix_kernel(in_ref, out_ref):
    carry = jnp.zeros((VROWS, DK), F32)
    for s in range(in_ref.shape[0]):
        out_ref[s] = carry.astype(BF16)
        decay = in_ref[s, VROWS:, :].astype(F32)[0:1, :]
        carry = carry * decay + in_ref[s, 0:VROWS, :].astype(F32)


def exchange(x):
    return lax.all_to_all(x, EP, split_axis=0, concat_axis=0, tiled=True)


def prefix(arrived):
    return pl.pallas_call(
        prefix_kernel,
        out_shape=jax.ShapeDtypeStruct((arrived.shape[0], VROWS, DK), BF16),
        name="prefix",
    )(arrived)


def own_columns(slots, first_rows, part):
    rows = slots.shape[1]
    wide = jnp.concatenate([slots] * 4, axis=0).astype(F32).astype(BF16)
    count = part * len(first_rows)
    row = lax.broadcasted_iota(jnp.int32, (rows, count), 0)
    col = lax.broadcasted_iota(jnp.int32, (rows, count), 1)
    source = col % part
    for i, first in enumerate(first_rows):
        source += jnp.where(col // part == i, first, 0)
    pick = jnp.where(row == source, 1.0, 0.0).astype(BF16)
    return contract(wide, pick, 1, 0)[0:2].astype(jnp.int32)


def dispatch_kernel(
    idx_ref, rows_ref, gain_ref, pick_ref, down_ref, out_ref, slot_ref, *rest, part, experts
):
    cuts, sems = rest[:NY], rest[NY]
    cut = cuts[0].shape[1]
    copies = []
    for i, dst in enumerate(cuts):
        column = pl.multiple_of(((idx_ref[0] // 2 + i) % NY) * cut, cut)
        copies.append(
            pltpu.make_async_copy(down_ref.at[:, pl.ds(column, cut)], dst, sems.at[i])
        )
        copies[-1].start()
    total = pick_ref.shape[1]
    pick = pick_ref[...]
    first = pick[0:1]
    second = pick[1:2]
    expert = lax.broadcasted_iota(jnp.int32, (experts, total), 0)
    hit0 = first == expert
    hit1 = second == expert
    named = jnp.where(hit0 | hit1, 1.0, 0.0).astype(BF16)
    row = lax.broadcasted_iota(jnp.int32, (total, total), 0)
    col = lax.broadcasted_iota(jnp.int32, (total, total), 1)
    earlier = (row < col) & (col // part == row // part)
    before = contract(named, jnp.where(earlier, 1.0, 0.0).astype(BF16), 1, 0)
    rank0 = jnp.sum(jnp.where(hit0, before, 0.0), axis=0, keepdims=True)
    rank1 = jnp.sum(jnp.where(hit1, before, 0.0), axis=0, keepdims=True)
    slots = pick * CAP + jnp.concatenate([rank0, rank1], axis=0).astype(jnp.int32)
    slot_ref[...] = slots
    values = rows_ref[...].astype(F32)
    mean = jnp.mean(values * values, axis=-1, keepdims=True)
    normed = (values * lax.rsqrt(mean + 1e-06) * gain_ref[...]).astype(BF16)
    own = own_columns(slots, [idx_ref[0] * part], part)
    place = lax.broadcasted_iota(jnp.int32, (out_ref.shape[0], part), 0)
    target = (place // (2 * CAP)) * CAP + place % CAP
    chosen = (own[0:1] == target) | (own[1:2] == target)
    half = out_ref.shape[1]
    total_out = None
    for h in range(2):
        mine = chosen & (place // CAP % 2 == h)
        piece = contract(
            jnp.where(mine, 1.0, 0.0).astype(BF16), normed[:, h * half : (h + 1) * half], 1, 0
        )
        total_out = piece if total_out is None else total_out + piece
    out_ref[...] = total_out.astype(BF16)
    for copy in copies:
        copy.wait()


def dispatch(index, rows, gain, pick, down, part, experts):
    total, width = rows.shape
    return pl.pallas_call(
        functools.partial(dispatch_kernel, part=part, experts=experts),
        grid_spec=pltpu.PrefetchScalarGridSpec(
            num_scalar_prefetch=1,
            grid=(1,),
            in_specs=[
                pl.BlockSpec((part, width), lambda n, idx: (idx[0], 0)),
                pl.BlockSpec((1, width), lambda n, idx: (0, 0)),
                pl.BlockSpec((2, total), lambda n, idx: (0, 0)),
                pl.BlockSpec(memory_space=pl.ANY),
            ],
            out_specs=[
                pl.BlockSpec((experts * CAP * 2, width // 2), lambda n, idx: (0, 0)),
                pl.BlockSpec((2, total), lambda n, idx: (0, 0)),
            ]
            + [pl.BlockSpec(memory_space=pl.ANY)] * NY,
            scratch_shapes=[pltpu.SemaphoreType.DMA((NY,))],
        ),
        out_shape=[
            jax.ShapeDtypeStruct((experts * CAP * 2, width // 2), BF16),
            jax.ShapeDtypeStruct((2, total), jnp.int32),
        ]
        + [jax.ShapeDtypeStruct((down.shape[0], down.shape[1] // NY), BF16)] * NY,
        name="dispatch",
    )(index, rows, gain.reshape(1, width), pick.T, down)


def hidden_kernel(*refs, parts):
    xs = refs[:parts]
    weights = refs[parts : parts + 8]
    out_ref = refs[parts + 8]
    acc = refs[parts + 9]
    step = pl.program_id(0)
    rows = xs[0].shape[0]
    new = lax.broadcasted_iota(jnp.int32, (rows // 2, rows), 0)
    old = lax.broadcasted_iota(jnp.int32, (rows // 2, rows), 1)
    spread = (new // CAP) * (2 * CAP) + new % CAP
    x = []
    for h in range(2):
        order = jnp.where(old == spread + h * CAP, 1.0, 0.0).astype(BF16)
        x.append(
            jnp.concatenate([contract(order, r[...], 1, 0).astype(BF16) for r in xs], axis=0)
        )

    @pl.when(step == 0)
    def _():
        acc[...] = jnp.zeros_like(acc)

    width = weights[0].shape[1]
    for j in range(4):
        acc[:, j * width : (j + 1) * width] += contract(x[0], weights[2 * j][...], 1, 0) + contract(
            x[1], weights[2 * j + 1][...], 1, 0
        )

    @pl.when(step == pl.num_programs(0) - 1)
    def _():
        for j in range(2):
            gate = acc[:, 2 * j * width : (2 * j + 1) * width]
            up = acc[:, (2 * j + 1) * width : (2 * j + 2) * width]
            value = gate / (1.0 + jnp.exp(-gate)) * up
            out_ref[:, j * width : (j + 1) * width] = value.astype(BF16)


def hidden_units(xs, weights, ktile=512):
    rows = sum(x.shape[0] for x in xs) // 2
    depth, width = weights[0].shape
    steps = depth // 2 // ktile
    specs, doubled = [], []
    for w in weights:
        doubled += [w, w]
        specs += [
            pl.BlockSpec((ktile, width), lambda n: (n, 0)),
            pl.BlockSpec((ktile, width), lambda n: (n + steps, 0)),
        ]
    return pl.pallas_call(
        functools.partial(hidden_kernel, parts=len(xs)),
        grid=(steps,),
        in_specs=[pl.BlockSpec((x.shape[0], ktile), lambda n: (0, n)) for x in xs] + specs,
        out_specs=pl.BlockSpec((rows, 2 * width), lambda n: (0, 0)),
        out_shape=jax.ShapeDtypeStruct((rows, 2 * width), BF16),
        scratch_shapes=[pltpu.VMEM((rows, 4 * width), F32)],
        compiler_params=pltpu.CompilerParams(dimension_semantics=("arbitrary",)),
        cost_estimate=pl.CostEstimate(
            flops=8 * rows * depth * width,
            transcendentals=2 * rows * width,
            bytes_accessed=8 * depth * width + 2 * rows * depth,
        ),
        name="hidden_units",
    )(*xs, *doubled)


def in_blocks(near, far, shift):
    ordered = (near[0], near[1], far[...], near[2])
    return jnp.concatenate([ordered[(i - shift) % NY] for i in range(NY)], axis=0)


def down_kernel(n0, f0, n1, f1, n2a, n2b, f2, n3, f3, *rest):
    weights = rest[:8]
    state_ref, out_ref = rest[8:10]
    width, depth = weights[0].shape
    rows = out_ref.shape[0]
    group = rows // NY
    pairs = ((n0, f0), (n1, f1), ((n2a[0], n2a[1], n2b[0]), f2), (n3, f3))
    total = None
    for m, pair in enumerate(pairs):
        act = in_blocks(*pair, m)
        for c in range(2):
            term = contract(act[:, c * width : (c + 1) * width], weights[2 * m + c][...], 1, 0)
            total = term if total is None else total + term
    new = lax.broadcasted_iota(jnp.int32, (rows, rows), 0)
    old = lax.broadcasted_iota(jnp.int32, (rows, rows), 1)
    want = (new // CAP % NY) * group + (new // (CAP * NY)) * CAP + new % CAP
    order = jnp.where(old == want, 1.0, 0.0).astype(BF16)
    out_ref[:, 0:depth] = contract(order, total.astype(BF16), 1, 0).astype(BF16)
    out_ref[:, depth:] = state_ref[...]


def expert_down(hs, weights, states, tiles=2):
    rows, units = hs[1].shape
    group = rows // tiles
    out_rows = NY * rows
    columns = weights[0].shape[1] + states.shape[1]

    def spec(h):
        if h.ndim == 2:
            return pl.BlockSpec((group, units), lambda n: (n, 0))
        return pl.BlockSpec((h.shape[0], group, units), lambda n: (0, n, 0))

    return pl.pallas_call(
        down_kernel,
        grid=(tiles,),
        in_specs=[spec(h) for h in hs]
        + [pl.BlockSpec(w.shape, lambda n: (0, 0)) for w in weights]
        + [pl.BlockSpec((out_rows // tiles, states.shape[1]), lambda n: (n, 0))],
        out_specs=pl.BlockSpec((out_rows // tiles, columns), lambda n: (n, 0)),
        out_shape=jax.ShapeDtypeStruct((out_rows, columns), BF16),
        compiler_params=pltpu.CompilerParams(dimension_semantics=("arbitrary",)),
        cost_estimate=pl.CostEstimate(
            flops=2 * out_rows * columns * sum(w.shape[0] for w in weights),
            transcendentals=0,
            bytes_accessed=8 * 10**6,
        ),
        name="expert_down",
    )(*hs, *weights, states)


def combine_kernel(idx_ref, back_ref, slot_ref, weight_ref, o0, o1, o2, o3, *, part):
    y = idx_ref[0] // 2
    core = idx_ref[0] % 2
    firsts = [(((y + i) % NY) * 2 + core) * part for i in range(NY)]
    own = own_columns(slot_ref[...], firsts, part)
    block = lax.broadcasted_iota(jnp.int32, own.shape, 1) // part
    spot = (own // CAP) * (CAP * NY) + block * CAP + own % CAP
    place = lax.broadcasted_iota(jnp.int32, (back_ref.shape[0], NY * part), 0)
    weight = jnp.concatenate(
        [weight_ref[pl.ds(pl.multiple_of(first, part), part), :] for first in firsts], axis=0
    )
    back = back_ref[...]
    mixed = None
    for j in range(2):
        chosen = jnp.where(place == spot[j : j + 1], 1.0, 0.0).astype(BF16)
        term = contract(chosen, back, 0, 0) * weight[:, j : j + 1]
        mixed = term if mixed is None else mixed + term
    for i, out in enumerate((o0, o1, o2, o3)):
        out[...] = mixed[i * part : (i + 1) * part].astype(out.dtype)


def combine(index, back, slots, weight, part, width):
    total = weight.shape[0]
    return pl.pallas_call(
        functools.partial(combine_kernel, part=part),
        grid_spec=pltpu.PrefetchScalarGridSpec(
            num_scalar_prefetch=1,
            grid=(1,),
            in_specs=[
                pl.BlockSpec((back.shape[0], width), lambda n, idx: (0, 0)),
                pl.BlockSpec((2, total), lambda n, idx: (0, 0)),
                pl.BlockSpec((total, 2), lambda n, idx: (0, 0)),
            ],
            out_specs=[pl.BlockSpec((part, width), lambda n, idx: (0, 0)) for _ in range(NY)],
        ),
        out_shape=[jax.ShapeDtypeStruct((part, width), BF16) for _ in range(NY)],
        name="combine",
    )(index, back, slots, weight)


def finish_kernel(idx_ref, p0, p1, p2, p3, gain_ref, out_ref):
    y = idx_ref[0] // 2
    width = p0.shape[1]
    pieces = [p[...].astype(F32) for p in (p0, p1, p2, p3)]
    square = sum(jnp.sum(p * p, axis=-1, keepdims=True) for p in pieces)
    scale = lax.rsqrt(square / (width * NY) + 1e-06)
    for i, piece in enumerate(pieces):
        columns = pl.ds(pl.multiple_of(((y + i) % NY) * width, width), width)
        out_ref[:, columns] = (piece * scale * gain_ref[:, columns]).astype(BF16)


def finish(index, pieces, gain):
    part, width = pieces[0].shape
    full = width * NY
    return pl.pallas_call(
        finish_kernel,
        grid_spec=pltpu.PrefetchScalarGridSpec(
            num_scalar_prefetch=1,
            grid=(1,),
            in_specs=[pl.BlockSpec((part, width), lambda n, idx: (0, 0)) for _ in pieces]
            + [pl.BlockSpec((1, full), lambda n, idx: (0, 0))],
            out_specs=pl.BlockSpec((part, full), lambda n, idx: (0, 0)),
        ),
        out_shape=jax.ShapeDtypeStruct((part, full), BF16),
        name="finish",
    )(index, *pieces, gain.reshape(1, full))


def from_right(x):
    return lax.ppermute(x, "y", ring(NY, -1))


def from_left(x):
    return lax.ppermute(x, "y", ring(NY, 1))


def on_device(
    queries,
    key_vectors,
    value_vectors,
    decay_logit,
    head_gain,
    routed_rows,
    pre_gain,
    expert_pick,
    route_weight,
    gate_weight,
    up_weight,
    down_weight,
    post_gain,
):
    y = lax.axis_index("y")
    core = lax.axis_index("c")
    experts = lax.axis_size(EP)
    part = routed_rows.shape[0] // (NY * 2)
    width = routed_rows.shape[1]
    index = (y * 2 + core).astype(jnp.int32).reshape(1)
    swap = [(0, 1), (1, 0)]

    gate, up, down = gate_weight[0], up_weight[0], down_weight[0]
    outgoing, slots, *slices = dispatch(
        index, routed_rows, pre_gain, expert_pick, down, part, experts
    )
    arrived = exchange(outgoing.reshape(experts, 2 * CAP, width // 2))

    weights = (gate, up, lax.ppermute(gate, "c", swap), lax.ppermute(up, "c", swap))
    cut = width // NY
    mine = [slices[0]] + [lax.ppermute(slices[-m % NY], "y", ring(NY, -m)) for m in range(1, NY)]
    local_out, query_carry, local_state = attn_local(
        queries, key_vectors, value_vectors, decay_logit
    )
    mine, _ = lax.optimization_barrier((mine, local_state))
    arrived, local_state = lax.optimization_barrier((arrived, local_state))
    downs = []
    for piece in mine:
        downs += [piece, lax.ppermute(piece, "c", swap)]

    half = experts // 2
    top = arrived[:half].reshape(-1, width // 2)
    bottom = arrived[half:].reshape(-1, width // 2)
    right_top, right_bottom = from_right(top), from_right(bottom)
    left_top, left_bottom = from_left(top), from_left(bottom)
    far_top, far_bottom = from_left(left_top), from_right(right_bottom)

    chunk_states = exchange(local_state)
    before = prefix(chunk_states)
    sides, before = lax.optimization_barrier(
        ((right_top, right_bottom, left_top, left_bottom), before)
    )
    near = hidden_units([top, bottom, *sides], weights).reshape(3, -1, 2 * gate.shape[1])
    far = hidden_units([far_top, far_bottom], weights)
    near_left, near_right = from_left(near), from_right(near)
    far_left, far_right = from_left(far), from_right(far)
    far_far = lax.ppermute(far, "y", ring(NY, 2))
    near_left, near_right, far = lax.optimization_barrier((near_left, near_right, far))
    near_far = (from_left(near_left[:2]), from_right(near_right[2:]))
    back = expert_down(
        (near, far, near_right, far_right, *near_far, far_far, near_left, far_left),
        downs,
        before.reshape(-1, DK),
    )
    returned = exchange(back.reshape(experts, NY * CAP, cut + DK)).reshape(-1, cut + DK)

    pieces = combine(index, returned, slots, route_weight, part, cut)
    gathered = [pieces[0]] + [
        lax.ppermute(pieces[-m % NY], "y", ring(NY, -m)) for m in range(1, NY)
    ]
    routed_out = finish(index, gathered, post_gain)
    mixed_heads = attn_out(local_out, query_carry, returned, head_gain, cut // DK)
    return (mixed_heads, routed_out)


def solution(mesh):
    ep, tp = mesh.shape["ep"], mesh.shape["tp"]
    torus = Mesh(mesh.devices.reshape(ep // 4, 4, NY, tp // NY), ("z", "x", "y", "c"))
    tpa = ("y", "c")
    placed = (
        P(EP, tpa),
        P(EP, tpa),
        P(EP, tpa),
        P(EP, tpa),
        P(),
        P(EP, None),
        P(),
        P(EP, None),
        P(EP, None),
        P(EP, None, tpa),
        P(EP, None, tpa),
        P(EP, tpa, None),
        P(),
    )
    return jax.shard_map(
        on_device,
        mesh=torus,
        in_specs=placed,
        out_specs=(P(EP, tpa), P(("z", "x", "y", "c"), None)),
        check_vma=False,
    )
```

```python
import functools

import jax
import jax.numpy as jnp
from jax import lax
from jax.experimental import pallas as pl
from jax.experimental.pallas import tpu as pltpu
from jax.sharding import Mesh
from jax.sharding import PartitionSpec as P


DK = 128
DV = 256
BLK = 64
VROWS = 16
CAP = 4
NY = 4
EP = ("z", "x")
F32 = jnp.float32
BF16 = jnp.bfloat16


def ring(size, step):
    return [(i, (i + step) % size) for i in range(size)]


def contract(a, b, dim_a, dim_b):
    return lax.dot_general(
        a, b, (((dim_a,), (dim_b,)), ((), ())), preferred_element_type=F32
    )


def attn_local_kernel(q_ref, k_ref, v_ref, g_ref, o_ref, qc_ref, st_ref, state, decay):
    step = pl.program_id(0)
    heads = state.shape[0]

    @pl.when(step == 0)
    def _():
        state[...] = jnp.zeros_like(state)
        decay[...] = jnp.zeros_like(decay)

    row = lax.broadcasted_iota(jnp.int32, (BLK, BLK), 0)
    col = lax.broadcasted_iota(jnp.int32, (BLK, BLK), 1)
    causal = row >= col
    before = decay[0:1, :]
    old = [state[h] for h in range(heads)]
    for b in range(q_ref.shape[0] // BLK):
        rows = slice(b * BLK, (b + 1) * BLK)
        logit = g_ref[rows, :]
        rate = (jnp.minimum(logit, 0.0) - jnp.log1p(jnp.exp(-jnp.abs(logit)))) * (1.0 / 16.0)
        cumulative = jnp.dot(
            causal.astype(F32), rate, precision=lax.Precision.HIGHEST, preferred_element_type=F32
        )
        ending = cumulative[BLK - 1 : BLK, :]
        q = q_ref[rows, :].astype(F32)
        k = k_ref[rows, :].astype(F32)
        query_decay = (q * jnp.exp(cumulative)).astype(BF16)
        key_decay = (k * jnp.exp(-cumulative)).astype(BF16)
        key_to_end = (k * jnp.exp(ending - cumulative)).astype(BF16)
        qc_ref[rows, :] = (q * jnp.exp(cumulative + before)).astype(BF16)
        before = before + ending
        step_decay = jnp.exp(ending)
        for h in range(heads):
            ks = slice(h * DK, (h + 1) * DK)
            vs = slice(h * DV, (h + 1) * DV)
            v = v_ref[rows, vs]
            scores = contract(query_decay[:, ks], key_decay[:, ks], 1, 1)
            weights = jnp.where(causal, scores, 0.0).astype(BF16)
            inside = contract(weights, v, 1, 0)
            o_ref[rows, vs] = inside + contract(query_decay[:, ks], old[h].astype(BF16), 1, 1)
            old[h] = old[h] * step_decay[:, ks] + contract(v, key_to_end[:, ks], 0, 0)
    decay[...] = jnp.broadcast_to(before, decay.shape)
    for h in range(heads):
        state[h] = old[h]

    @pl.when(step == pl.num_programs(0) - 1)
    def _():
        for h in range(heads):
            total = jnp.exp(decay[0:1, h * DK : (h + 1) * DK])
            chunks = DV // VROWS
            own = slice(h * chunks, (h + 1) * chunks)
            st_ref[own, 0:VROWS, :] = state[h].astype(BF16).reshape(chunks, VROWS, DK)
            st_ref[own, VROWS:, :] = jnp.broadcast_to(total, (chunks, 8, DK)).astype(BF16)


def attn_local(q, k, v, g):
    rows, keys = q.shape
    values = v.shape[1]
    heads = keys // DK
    tile = 4 * BLK
    return pl.pallas_call(
        attn_local_kernel,
        grid=(rows // tile,),
        in_specs=[
            pl.BlockSpec((tile, keys), lambda n: (n, 0)),
            pl.BlockSpec((tile, keys), lambda n: (n, 0)),
            pl.BlockSpec((tile, values), lambda n: (n, 0)),
            pl.BlockSpec((tile, keys), lambda n: (n, 0)),
        ],
        out_specs=[
            pl.BlockSpec((tile, values), lambda n: (n, 0)),
            pl.BlockSpec((tile, keys), lambda n: (n, 0)),
            pl.BlockSpec((heads * DV // VROWS, VROWS + 8, DK), lambda n: (0, 0, 0)),
        ],
        out_shape=[
            jax.ShapeDtypeStruct((rows, values), F32),
            jax.ShapeDtypeStruct((rows, keys), BF16),
            jax.ShapeDtypeStruct((heads * DV // VROWS, VROWS + 8, DK), BF16),
        ],
        scratch_shapes=[
            pltpu.VMEM((heads, DV, DK), F32),
            pltpu.VMEM((8, keys), F32),
        ],
        compiler_params=pltpu.CompilerParams(dimension_semantics=("arbitrary",)),
        cost_estimate=pl.CostEstimate(
            flops=8 * 10**9, transcendentals=10**6, bytes_accessed=6 * 10**6
        ),
        name="attn_local",
    )(q, k, v, g)


def attn_out_kernel(o_ref, qc_ref, in_ref, gain_ref, out_ref):
    gain = gain_ref[...]
    for h in range(in_ref.shape[0] // DV):
        vs = slice(h * DV, (h + 1) * DV)
        carried = contract(qc_ref[:, h * DK : (h + 1) * DK], in_ref[h * DV : (h + 1) * DV, :], 1, 1)
        total = o_ref[:, vs] + carried
        mean = jnp.mean(total * total, axis=-1, keepdims=True)
        out_ref[:, vs] = (total * lax.rsqrt(mean + 1e-06) * gain).astype(BF16)


def attn_out(o, qc, returned, gain, column):
    rows, values = o.shape
    tile = 256
    return pl.pallas_call(
        attn_out_kernel,
        grid=(rows // tile,),
        in_specs=[
            pl.BlockSpec((tile, values), lambda n: (n, 0)),
            pl.BlockSpec((tile, qc.shape[1]), lambda n: (n, 0)),
            pl.BlockSpec((returned.shape[0], DK), lambda n: (0, column)),
            pl.BlockSpec((1, DV), lambda n: (0, 0)),
        ],
        out_specs=pl.BlockSpec((tile, values), lambda n: (n, 0)),
        out_shape=jax.ShapeDtypeStruct((rows, values), BF16),
        compiler_params=pltpu.CompilerParams(dimension_semantics=("arbitrary",)),
        cost_estimate=pl.CostEstimate(
            flops=3 * 10**9, transcendentals=2048, bytes_accessed=4 * 10**6
        ),
        name="attn_out",
    )(o, qc, returned, gain.reshape(1, DV))


def prefix_kernel(in_ref, out_ref):
    carry = jnp.zeros((VROWS, DK), F32)
    for s in range(in_ref.shape[0]):
        out_ref[s] = carry.astype(BF16)
        decay = in_ref[s, VROWS:, :].astype(F32)[0:1, :]
        carry = carry * decay + in_ref[s, 0:VROWS, :].astype(F32)


def exchange(x):
    return lax.all_to_all(x, EP, split_axis=0, concat_axis=0, tiled=True)


def prefix(arrived):
    return pl.pallas_call(
        prefix_kernel,
        out_shape=jax.ShapeDtypeStruct((arrived.shape[0], VROWS, DK), BF16),
        name="prefix",
    )(arrived)


def own_columns(slots, first_rows, part):
    rows = slots.shape[1]
    wide = jnp.concatenate([slots] * 4, axis=0).astype(F32).astype(BF16)
    count = part * len(first_rows)
    row = lax.broadcasted_iota(jnp.int32, (rows, count), 0)
    col = lax.broadcasted_iota(jnp.int32, (rows, count), 1)
    source = col % part
    for i, first in enumerate(first_rows):
        source += jnp.where(col // part == i, first, 0)
    pick = jnp.where(row == source, 1.0, 0.0).astype(BF16)
    return contract(wide, pick, 1, 0)[0:2].astype(jnp.int32)


def dispatch_kernel(idx_ref, rows_ref, gain_ref, pick_ref, out_ref, slot_ref, *, part, experts):
    total = pick_ref.shape[1]
    pick = pick_ref[...]
    first = pick[0:1]
    second = pick[1:2]
    expert = lax.broadcasted_iota(jnp.int32, (experts, total), 0)
    hit0 = first == expert
    hit1 = second == expert
    named = jnp.where(hit0 | hit1, 1.0, 0.0).astype(BF16)
    row = lax.broadcasted_iota(jnp.int32, (total, total), 0)
    col = lax.broadcasted_iota(jnp.int32, (total, total), 1)
    earlier = (row < col) & (col // part == row // part)
    before = contract(named, jnp.where(earlier, 1.0, 0.0).astype(BF16), 1, 0)
    rank0 = jnp.sum(jnp.where(hit0, before, 0.0), axis=0, keepdims=True)
    rank1 = jnp.sum(jnp.where(hit1, before, 0.0), axis=0, keepdims=True)
    slots = pick * CAP + jnp.concatenate([rank0, rank1], axis=0).astype(jnp.int32)
    slot_ref[...] = slots
    values = rows_ref[...].astype(F32)
    mean = jnp.mean(values * values, axis=-1, keepdims=True)
    normed = (values * lax.rsqrt(mean + 1e-06) * gain_ref[...]).astype(BF16)
    own = own_columns(slots, [idx_ref[0] * part], part)
    place = lax.broadcasted_iota(jnp.int32, (out_ref.shape[0], part), 0)
    target = (place // (2 * CAP)) * CAP + place % CAP
    chosen = (own[0:1] == target) | (own[1:2] == target)
    half = out_ref.shape[1]
    total_out = None
    for h in range(2):
        mine = chosen & (place // CAP % 2 == h)
        piece = contract(
            jnp.where(mine, 1.0, 0.0).astype(BF16), normed[:, h * half : (h + 1) * half], 1, 0
        )
        total_out = piece if total_out is None else total_out + piece
    out_ref[...] = total_out.astype(BF16)


def dispatch(index, rows, gain, pick, part, experts):
    total, width = rows.shape
    return pl.pallas_call(
        functools.partial(dispatch_kernel, part=part, experts=experts),
        grid_spec=pltpu.PrefetchScalarGridSpec(
            num_scalar_prefetch=1,
            grid=(1,),
            in_specs=[
                pl.BlockSpec((part, width), lambda n, idx: (idx[0], 0)),
                pl.BlockSpec((1, width), lambda n, idx: (0, 0)),
                pl.BlockSpec((2, total), lambda n, idx: (0, 0)),
            ],
            out_specs=[
                pl.BlockSpec((experts * CAP * 2, width // 2), lambda n, idx: (0, 0)),
                pl.BlockSpec((2, total), lambda n, idx: (0, 0)),
            ],
        ),
        out_shape=[
            jax.ShapeDtypeStruct((experts * CAP * 2, width // 2), BF16),
            jax.ShapeDtypeStruct((2, total), jnp.int32),
        ],
        name="dispatch",
    )(index, rows, gain.reshape(1, width), pick.T)


def hidden_kernel(*refs, parts):
    xs = refs[:parts]
    weights = refs[parts : parts + 8]
    out_ref = refs[parts + 8]
    acc = refs[parts + 9]
    step = pl.program_id(0)
    rows = xs[0].shape[0]
    new = lax.broadcasted_iota(jnp.int32, (rows // 2, rows), 0)
    old = lax.broadcasted_iota(jnp.int32, (rows // 2, rows), 1)
    spread = (new // CAP) * (2 * CAP) + new % CAP
    x = []
    for h in range(2):
        order = jnp.where(old == spread + h * CAP, 1.0, 0.0).astype(BF16)
        x.append(
            jnp.concatenate([contract(order, r[...], 1, 0).astype(BF16) for r in xs], axis=0)
        )

    @pl.when(step == 0)
    def _():
        acc[...] = jnp.zeros_like(acc)

    width = weights[0].shape[1]
    for j in range(4):
        acc[:, j * width : (j + 1) * width] += contract(x[0], weights[2 * j][...], 1, 0) + contract(
            x[1], weights[2 * j + 1][...], 1, 0
        )

    @pl.when(step == pl.num_programs(0) - 1)
    def _():
        for j in range(2):
            gate = acc[:, 2 * j * width : (2 * j + 1) * width]
            up = acc[:, (2 * j + 1) * width : (2 * j + 2) * width]
            value = gate / (1.0 + jnp.exp(-gate)) * up
            out_ref[:, j * width : (j + 1) * width] = value.astype(BF16)


def hidden_units(xs, weights, ktile=512):
    rows = sum(x.shape[0] for x in xs) // 2
    depth, width = weights[0].shape
    steps = depth // 2 // ktile
    specs, doubled = [], []
    for w in weights:
        doubled += [w, w]
        specs += [
            pl.BlockSpec((ktile, width), lambda n: (n, 0)),
            pl.BlockSpec((ktile, width), lambda n: (n + steps, 0)),
        ]
    return pl.pallas_call(
        functools.partial(hidden_kernel, parts=len(xs)),
        grid=(steps,),
        in_specs=[pl.BlockSpec((x.shape[0], ktile), lambda n: (0, n)) for x in xs] + specs,
        out_specs=pl.BlockSpec((rows, 2 * width), lambda n: (0, 0)),
        out_shape=jax.ShapeDtypeStruct((rows, 2 * width), BF16),
        scratch_shapes=[pltpu.VMEM((rows, 4 * width), F32)],
        compiler_params=pltpu.CompilerParams(dimension_semantics=("arbitrary",)),
        cost_estimate=pl.CostEstimate(
            flops=8 * rows * depth * width,
            transcendentals=2 * rows * width,
            bytes_accessed=8 * depth * width + 2 * rows * depth,
        ),
        name="hidden_units",
    )(*xs, *doubled)


def in_blocks(near, far, shift):
    ordered = (near[0], near[1], far[...], near[2])
    return jnp.concatenate([ordered[(i - shift) % NY] for i in range(NY)], axis=0)


def down_kernel(n0, f0, n1, f1, n2a, n2b, f2, n3, f3, *rest):
    weights = rest[:8]
    state_ref, out_ref = rest[8:10]
    width, depth = weights[0].shape
    rows = out_ref.shape[0]
    group = rows // NY
    pairs = ((n0, f0), (n1, f1), ((n2a[0], n2a[1], n2b[0]), f2), (n3, f3))
    total = None
    for m, pair in enumerate(pairs):
        act = in_blocks(*pair, m)
        for c in range(2):
            term = contract(act[:, c * width : (c + 1) * width], weights[2 * m + c][...], 1, 0)
            total = term if total is None else total + term
    new = lax.broadcasted_iota(jnp.int32, (rows, rows), 0)
    old = lax.broadcasted_iota(jnp.int32, (rows, rows), 1)
    want = (new // CAP % NY) * group + (new // (CAP * NY)) * CAP + new % CAP
    order = jnp.where(old == want, 1.0, 0.0).astype(BF16)
    out_ref[:, 0:depth] = contract(order, total.astype(BF16), 1, 0).astype(BF16)
    out_ref[:, depth:] = state_ref[...]


def expert_down(hs, weights, states, tiles=2):
    rows, units = hs[1].shape
    group = rows // tiles
    out_rows = NY * rows
    columns = weights[0].shape[1] + states.shape[1]

    def spec(h):
        if h.ndim == 2:
            return pl.BlockSpec((group, units), lambda n: (n, 0))
        return pl.BlockSpec((h.shape[0], group, units), lambda n: (0, n, 0))

    return pl.pallas_call(
        down_kernel,
        grid=(tiles,),
        in_specs=[spec(h) for h in hs]
        + [pl.BlockSpec(w.shape, lambda n: (0, 0)) for w in weights]
        + [pl.BlockSpec((out_rows // tiles, states.shape[1]), lambda n: (n, 0))],
        out_specs=pl.BlockSpec((out_rows // tiles, columns), lambda n: (n, 0)),
        out_shape=jax.ShapeDtypeStruct((out_rows, columns), BF16),
        compiler_params=pltpu.CompilerParams(dimension_semantics=("arbitrary",)),
        cost_estimate=pl.CostEstimate(
            flops=2 * out_rows * columns * sum(w.shape[0] for w in weights),
            transcendentals=0,
            bytes_accessed=8 * 10**6,
        ),
        name="expert_down",
    )(*hs, *weights, states)


def combine_kernel(idx_ref, back_ref, slot_ref, weight_ref, o0, o1, o2, o3, *, part):
    y = idx_ref[0] // 2
    core = idx_ref[0] % 2
    firsts = [(((y + i) % NY) * 2 + core) * part for i in range(NY)]
    own = own_columns(slot_ref[...], firsts, part)
    block = lax.broadcasted_iota(jnp.int32, own.shape, 1) // part
    spot = (own // CAP) * (CAP * NY) + block * CAP + own % CAP
    place = lax.broadcasted_iota(jnp.int32, (back_ref.shape[0], NY * part), 0)
    weight = jnp.concatenate(
        [weight_ref[pl.ds(pl.multiple_of(first, part), part), :] for first in firsts], axis=0
    )
    back = back_ref[...]
    mixed = None
    for j in range(2):
        chosen = jnp.where(place == spot[j : j + 1], 1.0, 0.0).astype(BF16)
        term = contract(chosen, back, 0, 0) * weight[:, j : j + 1]
        mixed = term if mixed is None else mixed + term
    for i, out in enumerate((o0, o1, o2, o3)):
        out[...] = mixed[i * part : (i + 1) * part].astype(out.dtype)


def combine(index, back, slots, weight, part, width):
    total = weight.shape[0]
    return pl.pallas_call(
        functools.partial(combine_kernel, part=part),
        grid_spec=pltpu.PrefetchScalarGridSpec(
            num_scalar_prefetch=1,
            grid=(1,),
            in_specs=[
                pl.BlockSpec((back.shape[0], width), lambda n, idx: (0, 0)),
                pl.BlockSpec((2, total), lambda n, idx: (0, 0)),
                pl.BlockSpec((total, 2), lambda n, idx: (0, 0)),
            ],
            out_specs=[pl.BlockSpec((part, width), lambda n, idx: (0, 0)) for _ in range(NY)],
        ),
        out_shape=[jax.ShapeDtypeStruct((part, width), BF16) for _ in range(NY)],
        name="combine",
    )(index, back, slots, weight)


def finish_kernel(idx_ref, p0, p1, p2, p3, gain_ref, out_ref):
    y = idx_ref[0] // 2
    width = p0.shape[1]
    pieces = [p[...].astype(F32) for p in (p0, p1, p2, p3)]
    square = sum(jnp.sum(p * p, axis=-1, keepdims=True) for p in pieces)
    scale = lax.rsqrt(square / (width * NY) + 1e-06)
    for i, piece in enumerate(pieces):
        columns = pl.ds(pl.multiple_of(((y + i) % NY) * width, width), width)
        out_ref[:, columns] = (piece * scale * gain_ref[:, columns]).astype(BF16)


def finish(index, pieces, gain):
    part, width = pieces[0].shape
    full = width * NY
    return pl.pallas_call(
        finish_kernel,
        grid_spec=pltpu.PrefetchScalarGridSpec(
            num_scalar_prefetch=1,
            grid=(1,),
            in_specs=[pl.BlockSpec((part, width), lambda n, idx: (0, 0)) for _ in pieces]
            + [pl.BlockSpec((1, full), lambda n, idx: (0, 0))],
            out_specs=pl.BlockSpec((part, full), lambda n, idx: (0, 0)),
        ),
        out_shape=jax.ShapeDtypeStruct((part, full), BF16),
        name="finish",
    )(index, *pieces, gain.reshape(1, full))


def from_right(x):
    return lax.ppermute(x, "y", ring(NY, -1))


def from_left(x):
    return lax.ppermute(x, "y", ring(NY, 1))


def on_device(
    queries,
    key_vectors,
    value_vectors,
    decay_logit,
    head_gain,
    routed_rows,
    pre_gain,
    expert_pick,
    route_weight,
    gate_weight,
    up_weight,
    down_weight,
    post_gain,
):
    y = lax.axis_index("y")
    core = lax.axis_index("c")
    experts = lax.axis_size(EP)
    part = routed_rows.shape[0] // (NY * 2)
    width = routed_rows.shape[1]
    index = (y * 2 + core).astype(jnp.int32).reshape(1)
    swap = [(0, 1), (1, 0)]

    gate, up, down = gate_weight[0], up_weight[0], down_weight[0]
    outgoing, slots = dispatch(index, routed_rows, pre_gain, expert_pick, part, experts)
    arrived = exchange(outgoing.reshape(experts, 2 * CAP, width // 2))

    weights = (gate, up, lax.ppermute(gate, "c", swap), lax.ppermute(up, "c", swap))
    cut = width // NY
    slices = [
        lax.dynamic_slice_in_dim(down, lax.rem(y + i, NY) * cut, cut, axis=1) for i in range(NY)
    ]
    mine = [slices[0]] + [lax.ppermute(slices[-m % NY], "y", ring(NY, -m)) for m in range(1, NY)]
    local_out, query_carry, local_state = attn_local(
        queries, key_vectors, value_vectors, decay_logit
    )
    mine, _ = lax.optimization_barrier((mine, local_state))
    arrived, local_state = lax.optimization_barrier((arrived, local_state))
    downs = []
    for piece in mine:
        downs += [piece, lax.ppermute(piece, "c", swap)]

    half = experts // 2
    top = arrived[:half].reshape(-1, width // 2)
    bottom = arrived[half:].reshape(-1, width // 2)
    right_top, right_bottom = from_right(top), from_right(bottom)
    left_top, left_bottom = from_left(top), from_left(bottom)
    far_top, far_bottom = from_left(left_top), from_right(right_bottom)

    chunk_states = exchange(local_state)
    before = prefix(chunk_states)
    sides, before = lax.optimization_barrier(
        ((right_top, right_bottom, left_top, left_bottom), before)
    )
    near = hidden_units([top, bottom, *sides], weights).reshape(3, -1, 2 * gate.shape[1])
    far = hidden_units([far_top, far_bottom], weights)
    near_left, near_right = from_left(near), from_right(near)
    far_left, far_right = from_left(far), from_right(far)
    far_far = lax.ppermute(far, "y", ring(NY, 2))
    near_left, near_right, far = lax.optimization_barrier((near_left, near_right, far))
    near_far = (from_left(near_left[:2]), from_right(near_right[2:]))
    back = expert_down(
        (near, far, near_right, far_right, *near_far, far_far, near_left, far_left),
        downs,
        before.reshape(-1, DK),
    )
    returned = exchange(back.reshape(experts, NY * CAP, cut + DK)).reshape(-1, cut + DK)

    pieces = combine(index, returned, slots, route_weight, part, cut)
    gathered = [pieces[0]] + [
        lax.ppermute(pieces[-m % NY], "y", ring(NY, -m)) for m in range(1, NY)
    ]
    routed_out = finish(index, gathered, post_gain)
    mixed_heads = attn_out(local_out, query_carry, returned, head_gain, cut // DK)
    return (mixed_heads, routed_out)


def solution(mesh):
    ep, tp = mesh.shape["ep"], mesh.shape["tp"]
    torus = Mesh(mesh.devices.reshape(ep // 4, 4, NY, tp // NY), ("z", "x", "y", "c"))
    tpa = ("y", "c")
    placed = (
        P(EP, tpa),
        P(EP, tpa),
        P(EP, tpa),
        P(EP, tpa),
        P(),
        P(EP, None),
        P(),
        P(EP, None),
        P(EP, None),
        P(EP, None, tpa),
        P(EP, None, tpa),
        P(EP, tpa, None),
        P(),
    )
    return jax.shard_map(
        on_device,
        mesh=torus,
        in_specs=placed,
        out_specs=(P(EP, tpa), P(("z", "x", "y", "c"), None)),
        check_vma=False,
    )
```

```python
import functools

import jax
import jax.numpy as jnp
from jax import lax
from jax.experimental import pallas as pl
from jax.experimental.pallas import tpu as pltpu
from jax.sharding import Mesh
from jax.sharding import PartitionSpec as P


DK = 128
DV = 256
BLK = 64
VROWS = 16
CAP = 4
NY = 4
EP = ("z", "x")
F32 = jnp.float32
BF16 = jnp.bfloat16


def ring(size, step):
    return [(i, (i + step) % size) for i in range(size)]


def contract(a, b, dim_a, dim_b):
    return lax.dot_general(
        a, b, (((dim_a,), (dim_b,)), ((), ())), preferred_element_type=F32
    )


def attn_local_kernel(q_ref, k_ref, v_ref, g_ref, o_ref, qc_ref, st_ref, state, decay):
    step = pl.program_id(0)
    heads = state.shape[0]

    @pl.when(step == 0)
    def _():
        state[...] = jnp.zeros_like(state)
        decay[...] = jnp.zeros_like(decay)

    row = lax.broadcasted_iota(jnp.int32, (BLK, BLK), 0)
    col = lax.broadcasted_iota(jnp.int32, (BLK, BLK), 1)
    causal = row >= col
    before = decay[0:1, :]
    old = [state[h] for h in range(heads)]
    for b in range(q_ref.shape[0] // BLK):
        rows = slice(b * BLK, (b + 1) * BLK)
        logit = g_ref[rows, :]
        rate = (jnp.minimum(logit, 0.0) - jnp.log1p(jnp.exp(-jnp.abs(logit)))) * (1.0 / 16.0)
        cumulative = jnp.dot(
            causal.astype(F32), rate, precision=lax.Precision.HIGHEST, preferred_element_type=F32
        )
        ending = cumulative[BLK - 1 : BLK, :]
        q = q_ref[rows, :].astype(F32)
        k = k_ref[rows, :].astype(F32)
        query_decay = (q * jnp.exp(cumulative)).astype(BF16)
        key_decay = (k * jnp.exp(-cumulative)).astype(BF16)
        key_to_end = (k * jnp.exp(ending - cumulative)).astype(BF16)
        qc_ref[rows, :] = (q * jnp.exp(cumulative + before)).astype(BF16)
        before = before + ending
        step_decay = jnp.exp(ending)
        for h in range(heads):
            ks = slice(h * DK, (h + 1) * DK)
            vs = slice(h * DV, (h + 1) * DV)
            v = v_ref[rows, vs]
            scores = contract(query_decay[:, ks], key_decay[:, ks], 1, 1)
            weights = jnp.where(causal, scores, 0.0).astype(BF16)
            inside = contract(weights, v, 1, 0)
            o_ref[rows, vs] = inside + contract(query_decay[:, ks], old[h].astype(BF16), 1, 1)
            old[h] = old[h] * step_decay[:, ks] + contract(v, key_to_end[:, ks], 0, 0)
    decay[...] = jnp.broadcast_to(before, decay.shape)
    for h in range(heads):
        state[h] = old[h]

    @pl.when(step == pl.num_programs(0) - 1)
    def _():
        for h in range(heads):
            total = jnp.exp(decay[0:1, h * DK : (h + 1) * DK])
            chunks = DV // VROWS
            own = slice(h * chunks, (h + 1) * chunks)
            st_ref[own, 0:VROWS, :] = state[h].astype(BF16).reshape(chunks, VROWS, DK)
            st_ref[own, VROWS:, :] = jnp.broadcast_to(total, (chunks, 8, DK)).astype(BF16)


def attn_local(q, k, v, g):
    rows, keys = q.shape
    values = v.shape[1]
    heads = keys // DK
    tile = 4 * BLK
    return pl.pallas_call(
        attn_local_kernel,
        grid=(rows // tile,),
        in_specs=[
            pl.BlockSpec((tile, keys), lambda n: (n, 0)),
            pl.BlockSpec((tile, keys), lambda n: (n, 0)),
            pl.BlockSpec((tile, values), lambda n: (n, 0)),
            pl.BlockSpec((tile, keys), lambda n: (n, 0)),
        ],
        out_specs=[
            pl.BlockSpec((tile, values), lambda n: (n, 0)),
            pl.BlockSpec((tile, keys), lambda n: (n, 0)),
            pl.BlockSpec((heads * DV // VROWS, VROWS + 8, DK), lambda n: (0, 0, 0)),
        ],
        out_shape=[
            jax.ShapeDtypeStruct((rows, values), F32),
            jax.ShapeDtypeStruct((rows, keys), BF16),
            jax.ShapeDtypeStruct((heads * DV // VROWS, VROWS + 8, DK), BF16),
        ],
        scratch_shapes=[
            pltpu.VMEM((heads, DV, DK), F32),
            pltpu.VMEM((8, keys), F32),
        ],
        compiler_params=pltpu.CompilerParams(dimension_semantics=("arbitrary",)),
        cost_estimate=pl.CostEstimate(
            flops=8 * 10**9, transcendentals=10**6, bytes_accessed=6 * 10**6
        ),
        name="attn_local",
    )(q, k, v, g)


def attn_out_kernel(o_ref, qc_ref, in_ref, gain_ref, out_ref):
    gain = gain_ref[...]
    for h in range(in_ref.shape[0] // DV):
        vs = slice(h * DV, (h + 1) * DV)
        carried = contract(qc_ref[:, h * DK : (h + 1) * DK], in_ref[h * DV : (h + 1) * DV, :], 1, 1)
        total = o_ref[:, vs] + carried
        mean = jnp.mean(total * total, axis=-1, keepdims=True)
        out_ref[:, vs] = (total * lax.rsqrt(mean + 1e-06) * gain).astype(BF16)


def attn_out(o, qc, returned, gain, column):
    rows, values = o.shape
    tile = 256
    return pl.pallas_call(
        attn_out_kernel,
        grid=(rows // tile,),
        in_specs=[
            pl.BlockSpec((tile, values), lambda n: (n, 0)),
            pl.BlockSpec((tile, qc.shape[1]), lambda n: (n, 0)),
            pl.BlockSpec((returned.shape[0], DK), lambda n: (0, column)),
            pl.BlockSpec((1, DV), lambda n: (0, 0)),
        ],
        out_specs=pl.BlockSpec((tile, values), lambda n: (n, 0)),
        out_shape=jax.ShapeDtypeStruct((rows, values), BF16),
        compiler_params=pltpu.CompilerParams(dimension_semantics=("arbitrary",)),
        cost_estimate=pl.CostEstimate(
            flops=3 * 10**9, transcendentals=2048, bytes_accessed=4 * 10**6
        ),
        name="attn_out",
    )(o, qc, returned, gain.reshape(1, DV))


def prefix_kernel(in_ref, out_ref):
    carry = jnp.zeros((VROWS, DK), F32)
    for s in range(in_ref.shape[0]):
        out_ref[s] = carry.astype(BF16)
        decay = in_ref[s, VROWS:, :].astype(F32)[0:1, :]
        carry = carry * decay + in_ref[s, 0:VROWS, :].astype(F32)


def exchange(x):
    return lax.all_to_all(x, EP, split_axis=0, concat_axis=0, tiled=True)


def prefix(arrived):
    return pl.pallas_call(
        prefix_kernel,
        out_shape=jax.ShapeDtypeStruct((arrived.shape[0], VROWS, DK), BF16),
        name="prefix",
    )(arrived)


def own_columns(slots, first_rows, part):
    rows = slots.shape[1]
    wide = jnp.concatenate([slots] * 4, axis=0).astype(F32).astype(BF16)
    count = part * len(first_rows)
    row = lax.broadcasted_iota(jnp.int32, (rows, count), 0)
    col = lax.broadcasted_iota(jnp.int32, (rows, count), 1)
    source = col % part
    for i, first in enumerate(first_rows):
        source += jnp.where(col // part == i, first, 0)
    pick = jnp.where(row == source, 1.0, 0.0).astype(BF16)
    return contract(wide, pick, 1, 0)[0:2].astype(jnp.int32)


def dispatch_kernel(
    idx_ref, rows_ref, gain_ref, pick_ref, first_ref, second_ref, slot_ref, *, part, experts
):
    total = pick_ref.shape[1]
    pick = pick_ref[...]
    first = pick[0:1]
    second = pick[1:2]
    expert = lax.broadcasted_iota(jnp.int32, (experts, total), 0)
    hit0 = first == expert
    hit1 = second == expert
    named = jnp.where(hit0 | hit1, 1.0, 0.0).astype(BF16)
    row = lax.broadcasted_iota(jnp.int32, (total, total), 0)
    col = lax.broadcasted_iota(jnp.int32, (total, total), 1)
    earlier = (row < col) & (col // part == row // part)
    before = contract(named, jnp.where(earlier, 1.0, 0.0).astype(BF16), 1, 0)
    rank0 = jnp.sum(jnp.where(hit0, before, 0.0), axis=0, keepdims=True)
    rank1 = jnp.sum(jnp.where(hit1, before, 0.0), axis=0, keepdims=True)
    slots = pick * CAP + jnp.concatenate([rank0, rank1], axis=0).astype(jnp.int32)
    slot_ref[...] = slots
    values = rows_ref[...].astype(F32)
    mean = jnp.mean(values * values, axis=-1, keepdims=True)
    normed = (values * lax.rsqrt(mean + 1e-06) * gain_ref[...]).astype(BF16)
    own = own_columns(slots, [idx_ref[0] * part], part)
    place = lax.broadcasted_iota(jnp.int32, (first_ref.shape[0], part), 0)
    target = (place // (2 * CAP)) * CAP + place % CAP
    chosen = (own[0:1] == target) | (own[1:2] == target)
    quarter = first_ref.shape[1]
    masks = [
        jnp.where(chosen & (place // CAP % 2 == h), 1.0, 0.0).astype(BF16) for h in range(2)
    ]
    for i, out_ref in enumerate((first_ref, second_ref)):
        start = 2 * i * quarter
        piece = contract(masks[0], normed[:, start : start + quarter], 1, 0) + contract(
            masks[1], normed[:, start + quarter : start + 2 * quarter], 1, 0
        )
        out_ref[...] = piece.astype(BF16)


def dispatch(index, rows, gain, pick, part, experts):
    total, width = rows.shape
    return pl.pallas_call(
        functools.partial(dispatch_kernel, part=part, experts=experts),
        grid_spec=pltpu.PrefetchScalarGridSpec(
            num_scalar_prefetch=1,
            grid=(1,),
            in_specs=[
                pl.BlockSpec((part, width), lambda n, idx: (idx[0], 0)),
                pl.BlockSpec((1, width), lambda n, idx: (0, 0)),
                pl.BlockSpec((2, total), lambda n, idx: (0, 0)),
            ],
            out_specs=[
                pl.BlockSpec((experts * CAP * 2, width // 4), lambda n, idx: (0, 0)),
                pl.BlockSpec((experts * CAP * 2, width // 4), lambda n, idx: (0, 0)),
                pl.BlockSpec((2, total), lambda n, idx: (0, 0)),
            ],
        ),
        out_shape=[
            jax.ShapeDtypeStruct((experts * CAP * 2, width // 4), BF16),
            jax.ShapeDtypeStruct((experts * CAP * 2, width // 4), BF16),
            jax.ShapeDtypeStruct((2, total), jnp.int32),
        ],
        name="dispatch",
    )(index, rows, gain.reshape(1, width), pick.T)


def two_quarters(xs):
    rows = xs[0].shape[0]
    new = lax.broadcasted_iota(jnp.int32, (rows // 2, rows), 0)
    old = lax.broadcasted_iota(jnp.int32, (rows // 2, rows), 1)
    spread = (new // CAP) * (2 * CAP) + new % CAP
    out = []
    for h in range(2):
        order = jnp.where(old == spread + h * CAP, 1.0, 0.0).astype(BF16)
        out.append(
            jnp.concatenate([contract(order, r[...], 1, 0).astype(BF16) for r in xs], axis=0)
        )
    return out


def add_products(acc, xs, weights):
    x = two_quarters(xs)
    width = weights[0].shape[1]
    for j in range(4):
        acc[:, j * width : (j + 1) * width] += contract(x[0], weights[2 * j][...], 1, 0) + contract(
            x[1], weights[2 * j + 1][...], 1, 0
        )


def first_half_kernel(*refs, parts):
    acc = refs[parts + 8]

    @pl.when(pl.program_id(0) == 0)
    def _():
        acc[...] = jnp.zeros_like(acc)

    add_products(acc, refs[:parts], refs[parts : parts + 8])


def hidden_kernel(*refs, parts):
    start_ref, out_ref, acc = refs[parts + 8 : parts + 11]
    step = pl.program_id(0)

    @pl.when(step == 0)
    def _():
        acc[...] = start_ref[...]

    add_products(acc, refs[:parts], refs[parts : parts + 8])
    width = out_ref.shape[1] // 2

    @pl.when(step == pl.num_programs(0) - 1)
    def _():
        for j in range(2):
            gate = acc[:, 2 * j * width : (2 * j + 1) * width]
            up = acc[:, (2 * j + 1) * width : (2 * j + 2) * width]
            value = gate / (1.0 + jnp.exp(-gate)) * up
            out_ref[:, j * width : (j + 1) * width] = value.astype(BF16)


def half_specs(xs, weights, half, ktile):
    steps = xs[0].shape[1] // ktile
    specs = [pl.BlockSpec((x.shape[0], ktile), lambda n: (0, n)) for x in xs]
    doubled = []
    for w in weights:
        for quarter in (2 * half, 2 * half + 1):
            doubled.append(w)
            specs.append(
                pl.BlockSpec(
                    (ktile, w.shape[1]), lambda n, quarter=quarter: (n + quarter * steps, 0)
                )
            )
    return steps, specs, doubled


def half_cost(rows, weights, width):
    return pl.CostEstimate(
        flops=4 * rows * weights[0].shape[0] * width,
        transcendentals=rows * width,
        bytes_accessed=4 * weights[0].shape[0] * weights[0].shape[1] + 6 * rows * width,
    )


def first_half(xs, weights, ktile=256):
    rows = sum(x.shape[0] for x in xs) // 2
    width = 4 * weights[0].shape[1]
    steps, specs, doubled = half_specs(xs, weights, 0, ktile)
    return pl.pallas_call(
        functools.partial(first_half_kernel, parts=len(xs)),
        grid=(steps,),
        in_specs=specs,
        out_specs=pl.BlockSpec((rows, width), lambda n: (0, 0)),
        out_shape=jax.ShapeDtypeStruct((rows, width), F32),
        compiler_params=pltpu.CompilerParams(dimension_semantics=("arbitrary",)),
        cost_estimate=half_cost(rows, weights, width),
        name="first_half",
    )(*xs, *doubled)


def hidden_units(xs, weights, start, block, ktile=256):
    rows = sum(x.shape[0] for x in xs) // 2
    width = 4 * weights[0].shape[1]
    steps, specs, doubled = half_specs(xs, weights, 1, ktile)
    return pl.pallas_call(
        functools.partial(hidden_kernel, parts=len(xs)),
        grid=(steps,),
        in_specs=specs + [pl.BlockSpec((rows, width), lambda n: (block, 0))],
        out_specs=pl.BlockSpec((rows, width // 2), lambda n: (0, 0)),
        out_shape=jax.ShapeDtypeStruct((rows, width // 2), BF16),
        scratch_shapes=[pltpu.VMEM((rows, width), F32)],
        compiler_params=pltpu.CompilerParams(dimension_semantics=("arbitrary",)),
        cost_estimate=half_cost(rows, weights, width),
        name="hidden_units",
    )(*xs, *doubled, start)


def in_blocks(near, far, shift):
    ordered = (near[0], near[1], far[...], near[2])
    return jnp.concatenate([ordered[(i - shift) % NY] for i in range(NY)], axis=0)


def down_kernel(n0, f0, n1, f1, n2a, n2b, f2, n3, f3, *rest):
    weights = rest[:8]
    state_ref, out_ref = rest[8:10]
    width, depth = weights[0].shape
    rows = out_ref.shape[0]
    group = rows // NY
    pairs = ((n0, f0), (n1, f1), ((n2a[0], n2a[1], n2b[0]), f2), (n3, f3))
    total = None
    for m, pair in enumerate(pairs):
        act = in_blocks(*pair, m)
        for c in range(2):
            term = contract(act[:, c * width : (c + 1) * width], weights[2 * m + c][...], 1, 0)
            total = term if total is None else total + term
    new = lax.broadcasted_iota(jnp.int32, (rows, rows), 0)
    old = lax.broadcasted_iota(jnp.int32, (rows, rows), 1)
    want = (new // CAP % NY) * group + (new // (CAP * NY)) * CAP + new % CAP
    order = jnp.where(old == want, 1.0, 0.0).astype(BF16)
    out_ref[:, 0:depth] = contract(order, total.astype(BF16), 1, 0).astype(BF16)
    out_ref[:, depth:] = state_ref[...]


def expert_down(hs, weights, states, tiles=2):
    rows, units = hs[1].shape
    group = rows // tiles
    out_rows = NY * rows
    columns = weights[0].shape[1] + states.shape[1]

    def spec(h):
        if h.ndim == 2:
            return pl.BlockSpec((group, units), lambda n: (n, 0))
        return pl.BlockSpec((h.shape[0], group, units), lambda n: (0, n, 0))

    return pl.pallas_call(
        down_kernel,
        grid=(tiles,),
        in_specs=[spec(h) for h in hs]
        + [pl.BlockSpec(w.shape, lambda n: (0, 0)) for w in weights]
        + [pl.BlockSpec((out_rows // tiles, states.shape[1]), lambda n: (n, 0))],
        out_specs=pl.BlockSpec((out_rows // tiles, columns), lambda n: (n, 0)),
        out_shape=jax.ShapeDtypeStruct((out_rows, columns), BF16),
        compiler_params=pltpu.CompilerParams(dimension_semantics=("arbitrary",)),
        cost_estimate=pl.CostEstimate(
            flops=2 * out_rows * columns * sum(w.shape[0] for w in weights),
            transcendentals=0,
            bytes_accessed=8 * 10**6,
        ),
        name="expert_down",
    )(*hs, *weights, states)


def combine_kernel(idx_ref, back_ref, slot_ref, weight_ref, o0, o1, o2, o3, *, part):
    y = idx_ref[0] // 2
    core = idx_ref[0] % 2
    firsts = [(((y + i) % NY) * 2 + core) * part for i in range(NY)]
    own = own_columns(slot_ref[...], firsts, part)
    block = lax.broadcasted_iota(jnp.int32, own.shape, 1) // part
    spot = (own // CAP) * (CAP * NY) + block * CAP + own % CAP
    place = lax.broadcasted_iota(jnp.int32, (back_ref.shape[0], NY * part), 0)
    weight = jnp.concatenate(
        [weight_ref[pl.ds(pl.multiple_of(first, part), part), :] for first in firsts], axis=0
    )
    back = back_ref[...]
    mixed = None
    for j in range(2):
        chosen = jnp.where(place == spot[j : j + 1], 1.0, 0.0).astype(BF16)
        term = contract(chosen, back, 0, 0) * weight[:, j : j + 1]
        mixed = term if mixed is None else mixed + term
    for i, out in enumerate((o0, o1, o2, o3)):
        out[...] = mixed[i * part : (i + 1) * part].astype(out.dtype)


def combine(index, back, slots, weight, part, width):
    total = weight.shape[0]
    return pl.pallas_call(
        functools.partial(combine_kernel, part=part),
        grid_spec=pltpu.PrefetchScalarGridSpec(
            num_scalar_prefetch=1,
            grid=(1,),
            in_specs=[
                pl.BlockSpec((back.shape[0], width), lambda n, idx: (0, 0)),
                pl.BlockSpec((2, total), lambda n, idx: (0, 0)),
                pl.BlockSpec((total, 2), lambda n, idx: (0, 0)),
            ],
            out_specs=[pl.BlockSpec((part, width), lambda n, idx: (0, 0)) for _ in range(NY)],
        ),
        out_shape=[jax.ShapeDtypeStruct((part, width), BF16) for _ in range(NY)],
        name="combine",
    )(index, back, slots, weight)


def finish_kernel(idx_ref, p0, p1, p2, p3, gain_ref, out_ref):
    y = idx_ref[0] // 2
    width = p0.shape[1]
    pieces = [p[...].astype(F32) for p in (p0, p1, p2, p3)]
    square = sum(jnp.sum(p * p, axis=-1, keepdims=True) for p in pieces)
    scale = lax.rsqrt(square / (width * NY) + 1e-06)
    for i, piece in enumerate(pieces):
        columns = pl.ds(pl.multiple_of(((y + i) % NY) * width, width), width)
        out_ref[:, columns] = (piece * scale * gain_ref[:, columns]).astype(BF16)


def finish(index, pieces, gain):
    part, width = pieces[0].shape
    full = width * NY
    return pl.pallas_call(
        finish_kernel,
        grid_spec=pltpu.PrefetchScalarGridSpec(
            num_scalar_prefetch=1,
            grid=(1,),
            in_specs=[pl.BlockSpec((part, width), lambda n, idx: (0, 0)) for _ in pieces]
            + [pl.BlockSpec((1, full), lambda n, idx: (0, 0))],
            out_specs=pl.BlockSpec((part, full), lambda n, idx: (0, 0)),
        ),
        out_shape=jax.ShapeDtypeStruct((part, full), BF16),
        name="finish",
    )(index, *pieces, gain.reshape(1, full))


def from_right(x):
    return lax.ppermute(x, "y", ring(NY, -1))


def from_left(x):
    return lax.ppermute(x, "y", ring(NY, 1))


def on_device(
    queries,
    key_vectors,
    value_vectors,
    decay_logit,
    head_gain,
    routed_rows,
    pre_gain,
    expert_pick,
    route_weight,
    gate_weight,
    up_weight,
    down_weight,
    post_gain,
):
    y = lax.axis_index("y")
    core = lax.axis_index("c")
    experts = lax.axis_size(EP)
    part = routed_rows.shape[0] // (NY * 2)
    width = routed_rows.shape[1]
    index = (y * 2 + core).astype(jnp.int32).reshape(1)
    swap = [(0, 1), (1, 0)]

    gate, up, down = gate_weight[0], up_weight[0], down_weight[0]
    out_a, out_b, slots = dispatch(index, routed_rows, pre_gain, expert_pick, part, experts)
    rows_a = exchange(out_a.reshape(experts, 2 * CAP, width // 4)).reshape(out_a.shape)
    rows_b = exchange(out_b.reshape(experts, 2 * CAP, width // 4)).reshape(out_b.shape)
    right_a, left_a = from_right(rows_a), from_left(rows_a)

    weights = (gate, up, lax.ppermute(gate, "c", swap), lax.ppermute(up, "c", swap))
    cut = width // NY
    slices = [
        lax.dynamic_slice_in_dim(down, lax.rem(y + i, NY) * cut, cut, axis=1) for i in range(NY)
    ]
    mine = [slices[0]] + [lax.ppermute(slices[-m % NY], "y", ring(NY, -m)) for m in range(1, NY)]
    local_out, query_carry, local_state = attn_local(
        queries, key_vectors, value_vectors, decay_logit
    )
    mine, _ = lax.optimization_barrier((mine, local_state))
    rows_b, local_state = lax.optimization_barrier((rows_b, local_state))
    downs = []
    for piece in mine:
        downs += [piece, lax.ppermute(piece, "c", swap)]

    far_a = from_left(left_a)
    right_b, left_b = from_right(rows_b), from_left(rows_b)
    far_b = from_right(right_b)

    chunk_states = exchange(local_state)
    before = prefix(chunk_states)
    right_b, left_b, before = lax.optimization_barrier((right_b, left_b, before))
    summed = first_half([rows_a, right_a, left_a, far_a], weights)
    near = hidden_units([rows_b, right_b, left_b], weights, summed, 0)
    near = near.reshape(3, -1, 2 * gate.shape[1])
    far = hidden_units([far_b], weights, summed, 3)
    near_left, near_right = from_left(near), from_right(near)
    far_left, far_right = from_left(far), from_right(far)
    far_far = lax.ppermute(far, "y", ring(NY, 2))
    near_left, near_right, far = lax.optimization_barrier((near_left, near_right, far))
    near_far = (from_left(near_left[:2]), from_right(near_right[2:]))
    back = expert_down(
        (near, far, near_right, far_right, *near_far, far_far, near_left, far_left),
        downs,
        before.reshape(-1, DK),
    )
    returned = exchange(back.reshape(experts, NY * CAP, cut + DK)).reshape(-1, cut + DK)

    pieces = combine(index, returned, slots, route_weight, part, cut)
    gathered = [pieces[0]] + [
        lax.ppermute(pieces[-m % NY], "y", ring(NY, -m)) for m in range(1, NY)
    ]
    routed_out = finish(index, gathered, post_gain)
    mixed_heads = attn_out(local_out, query_carry, returned, head_gain, cut // DK)
    return (mixed_heads, routed_out)


def solution(mesh):
    ep, tp = mesh.shape["ep"], mesh.shape["tp"]
    torus = Mesh(mesh.devices.reshape(ep // 4, 4, NY, tp // NY), ("z", "x", "y", "c"))
    tpa = ("y", "c")
    placed = (
        P(EP, tpa),
        P(EP, tpa),
        P(EP, tpa),
        P(EP, tpa),
        P(),
        P(EP, None),
        P(),
        P(EP, None),
        P(EP, None),
        P(EP, None, tpa),
        P(EP, None, tpa),
        P(EP, tpa, None),
        P(),
    )
    return jax.shard_map(
        on_device,
        mesh=torus,
        in_specs=placed,
        out_specs=(P(EP, tpa), P(("z", "x", "y", "c"), None)),
        check_vma=False,
    )
```

```python
import functools

import jax
import jax.numpy as jnp
from jax import lax
from jax.experimental import pallas as pl
from jax.experimental.pallas import tpu as pltpu
from jax.sharding import Mesh
from jax.sharding import PartitionSpec as P


DK = 128
DV = 256
BLK = 64
VROWS = 16
CAP = 4
NY = 4
EP = ("z", "x")
F32 = jnp.float32
BF16 = jnp.bfloat16


def ring(size, step):
    return [(i, (i + step) % size) for i in range(size)]


def contract(a, b, dim_a, dim_b):
    return lax.dot_general(
        a, b, (((dim_a,), (dim_b,)), ((), ())), preferred_element_type=F32
    )


def attn_local_kernel(q_ref, k_ref, v_ref, g_ref, o_ref, qc_ref, st_ref, state, decay):
    step = pl.program_id(0)
    heads = state.shape[0]

    @pl.when(step == 0)
    def _():
        state[...] = jnp.zeros_like(state)
        decay[...] = jnp.zeros_like(decay)

    row = lax.broadcasted_iota(jnp.int32, (BLK, BLK), 0)
    col = lax.broadcasted_iota(jnp.int32, (BLK, BLK), 1)
    causal = row >= col
    before = decay[0:1, :]
    old = [state[h] for h in range(heads)]
    for b in range(q_ref.shape[0] // BLK):
        rows = slice(b * BLK, (b + 1) * BLK)
        logit = g_ref[rows, :]
        rate = (jnp.minimum(logit, 0.0) - jnp.log1p(jnp.exp(-jnp.abs(logit)))) * (1.0 / 16.0)
        cumulative = jnp.dot(
            causal.astype(F32), rate, precision=lax.Precision.HIGHEST, preferred_element_type=F32
        )
        ending = cumulative[BLK - 1 : BLK, :]
        q = q_ref[rows, :].astype(F32)
        k = k_ref[rows, :].astype(F32)
        query_decay = (q * jnp.exp(cumulative)).astype(BF16)
        key_decay = (k * jnp.exp(-cumulative)).astype(BF16)
        key_to_end = (k * jnp.exp(ending - cumulative)).astype(BF16)
        qc_ref[rows, :] = (q * jnp.exp(cumulative + before)).astype(BF16)
        before = before + ending
        step_decay = jnp.exp(ending)
        for h in range(heads):
            ks = slice(h * DK, (h + 1) * DK)
            vs = slice(h * DV, (h + 1) * DV)
            v = v_ref[rows, vs]
            scores = contract(query_decay[:, ks], key_decay[:, ks], 1, 1)
            weights = jnp.where(causal, scores, 0.0).astype(BF16)
            inside = contract(weights, v, 1, 0)
            o_ref[rows, vs] = inside + contract(query_decay[:, ks], old[h].astype(BF16), 1, 1)
            old[h] = old[h] * step_decay[:, ks] + contract(v, key_to_end[:, ks], 0, 0)
    decay[...] = jnp.broadcast_to(before, decay.shape)
    for h in range(heads):
        state[h] = old[h]

    @pl.when(step == pl.num_programs(0) - 1)
    def _():
        for h in range(heads):
            total = jnp.exp(decay[0:1, h * DK : (h + 1) * DK])
            chunks = DV // VROWS
            own = slice(h * chunks, (h + 1) * chunks)
            st_ref[own, 0:VROWS, :] = state[h].astype(BF16).reshape(chunks, VROWS, DK)
            st_ref[own, VROWS:, :] = jnp.broadcast_to(total, (chunks, 8, DK)).astype(BF16)


def attn_local(q, k, v, g):
    rows, keys = q.shape
    values = v.shape[1]
    heads = keys // DK
    tile = 4 * BLK
    return pl.pallas_call(
        attn_local_kernel,
        grid=(rows // tile,),
        in_specs=[
            pl.BlockSpec((tile, keys), lambda n: (n, 0)),
            pl.BlockSpec((tile, keys), lambda n: (n, 0)),
            pl.BlockSpec((tile, values), lambda n: (n, 0)),
            pl.BlockSpec((tile, keys), lambda n: (n, 0)),
        ],
        out_specs=[
            pl.BlockSpec((tile, values), lambda n: (n, 0)),
            pl.BlockSpec((tile, keys), lambda n: (n, 0)),
            pl.BlockSpec((heads * DV // VROWS, VROWS + 8, DK), lambda n: (0, 0, 0)),
        ],
        out_shape=[
            jax.ShapeDtypeStruct((rows, values), F32),
            jax.ShapeDtypeStruct((rows, keys), BF16),
            jax.ShapeDtypeStruct((heads * DV // VROWS, VROWS + 8, DK), BF16),
        ],
        scratch_shapes=[
            pltpu.VMEM((heads, DV, DK), F32),
            pltpu.VMEM((8, keys), F32),
        ],
        compiler_params=pltpu.CompilerParams(dimension_semantics=("arbitrary",)),
        cost_estimate=pl.CostEstimate(
            flops=8 * 10**9, transcendentals=10**6, bytes_accessed=6 * 10**6
        ),
        name="attn_local",
    )(q, k, v, g)


def attn_out_kernel(o_ref, qc_ref, in_ref, gain_ref, out_ref):
    gain = gain_ref[...]
    for h in range(in_ref.shape[0] // DV):
        vs = slice(h * DV, (h + 1) * DV)
        carried = contract(qc_ref[:, h * DK : (h + 1) * DK], in_ref[h * DV : (h + 1) * DV, :], 1, 1)
        total = o_ref[:, vs] + carried
        mean = jnp.mean(total * total, axis=-1, keepdims=True)
        out_ref[:, vs] = (total * lax.rsqrt(mean + 1e-06) * gain).astype(BF16)


def attn_out(o, qc, returned, gain, column):
    rows, values = o.shape
    tile = 256
    return pl.pallas_call(
        attn_out_kernel,
        grid=(rows // tile,),
        in_specs=[
            pl.BlockSpec((tile, values), lambda n: (n, 0)),
            pl.BlockSpec((tile, qc.shape[1]), lambda n: (n, 0)),
            pl.BlockSpec((returned.shape[0], DK), lambda n: (0, column)),
            pl.BlockSpec((1, DV), lambda n: (0, 0)),
        ],
        out_specs=pl.BlockSpec((tile, values), lambda n: (n, 0)),
        out_shape=jax.ShapeDtypeStruct((rows, values), BF16),
        compiler_params=pltpu.CompilerParams(dimension_semantics=("arbitrary",)),
        cost_estimate=pl.CostEstimate(
            flops=3 * 10**9, transcendentals=2048, bytes_accessed=4 * 10**6
        ),
        name="attn_out",
    )(o, qc, returned, gain.reshape(1, DV))


def prefix_kernel(in_ref, out_ref):
    carry = jnp.zeros((VROWS, DK), F32)
    for s in range(in_ref.shape[0]):
        out_ref[s] = carry.astype(BF16)
        decay = in_ref[s, VROWS:, :].astype(F32)[0:1, :]
        carry = carry * decay + in_ref[s, 0:VROWS, :].astype(F32)


def exchange(x):
    return lax.all_to_all(x, EP, split_axis=0, concat_axis=0, tiled=True)


def prefix(arrived):
    return pl.pallas_call(
        prefix_kernel,
        out_shape=jax.ShapeDtypeStruct((arrived.shape[0], VROWS, DK), BF16),
        name="prefix",
    )(arrived)


def own_columns(slots, first_rows, part):
    rows = slots.shape[1]
    wide = jnp.concatenate([slots] * 4, axis=0).astype(F32).astype(BF16)
    count = part * len(first_rows)
    row = lax.broadcasted_iota(jnp.int32, (rows, count), 0)
    col = lax.broadcasted_iota(jnp.int32, (rows, count), 1)
    source = col % part
    for i, first in enumerate(first_rows):
        source += jnp.where(col // part == i, first, 0)
    pick = jnp.where(row == source, 1.0, 0.0).astype(BF16)
    return contract(wide, pick, 1, 0)[0:2].astype(jnp.int32)


def dispatch_kernel(idx_ref, rows_ref, gain_ref, pick_ref, out_ref, slot_ref, *, part, experts):
    total = pick_ref.shape[1]
    pick = pick_ref[...]
    first = pick[0:1]
    second = pick[1:2]
    expert = lax.broadcasted_iota(jnp.int32, (experts, total), 0)
    hit0 = first == expert
    hit1 = second == expert
    named = jnp.where(hit0 | hit1, 1.0, 0.0).astype(BF16)
    row = lax.broadcasted_iota(jnp.int32, (total, total), 0)
    col = lax.broadcasted_iota(jnp.int32, (total, total), 1)
    earlier = (row < col) & (col // part == row // part)
    before = contract(named, jnp.where(earlier, 1.0, 0.0).astype(BF16), 1, 0)
    rank0 = jnp.sum(jnp.where(hit0, before, 0.0), axis=0, keepdims=True)
    rank1 = jnp.sum(jnp.where(hit1, before, 0.0), axis=0, keepdims=True)
    slots = pick * CAP + jnp.concatenate([rank0, rank1], axis=0).astype(jnp.int32)
    slot_ref[...] = slots
    values = rows_ref[...].astype(F32)
    mean = jnp.mean(values * values, axis=-1, keepdims=True)
    normed = (values * lax.rsqrt(mean + 1e-06) * gain_ref[...]).astype(BF16)
    own = own_columns(slots, [idx_ref[0] * part], part)
    place = lax.broadcasted_iota(jnp.int32, (out_ref.shape[0], part), 0)
    target = (place // (2 * CAP)) * CAP + place % CAP
    chosen = (own[0:1] == target) | (own[1:2] == target)
    half = out_ref.shape[1]
    total_out = None
    for h in range(2):
        mine = chosen & (place // CAP % 2 == h)
        piece = contract(
            jnp.where(mine, 1.0, 0.0).astype(BF16), normed[:, h * half : (h + 1) * half], 1, 0
        )
        total_out = piece if total_out is None else total_out + piece
    out_ref[...] = total_out.astype(BF16)


def dispatch(index, rows, gain, pick, part, experts):
    total, width = rows.shape
    return pl.pallas_call(
        functools.partial(dispatch_kernel, part=part, experts=experts),
        grid_spec=pltpu.PrefetchScalarGridSpec(
            num_scalar_prefetch=1,
            grid=(1,),
            in_specs=[
                pl.BlockSpec((part, width), lambda n, idx: (idx[0], 0)),
                pl.BlockSpec((1, width), lambda n, idx: (0, 0)),
                pl.BlockSpec((2, total), lambda n, idx: (0, 0)),
            ],
            out_specs=[
                pl.BlockSpec((experts * CAP * 2, width // 2), lambda n, idx: (0, 0)),
                pl.BlockSpec((2, total), lambda n, idx: (0, 0)),
            ],
        ),
        out_shape=[
            jax.ShapeDtypeStruct((experts * CAP * 2, width // 2), BF16),
            jax.ShapeDtypeStruct((2, total), jnp.int32),
        ],
        name="dispatch",
    )(index, rows, gain.reshape(1, width), pick.T)


def hidden_kernel(*refs, parts, ktile):
    xs = refs[:parts]
    weights = refs[parts : parts + 4]
    out_ref, xbuf, wbuf, acc, sems = refs[parts + 4 :]
    rows, depth = xs[0].shape
    width = weights[0].shape[1]
    copies = []
    for t in range(depth // ktile):
        group = [
            pltpu.make_async_copy(
                x.at[:, pl.ds(t * ktile, ktile)], xbuf.at[t, i], sems.at[t, i]
            )
            for i, x in enumerate(xs)
        ]
        for j in range(8):
            start = (j % 2) * depth + t * ktile
            group.append(
                pltpu.make_async_copy(
                    weights[j // 2].at[pl.ds(start, ktile), :],
                    wbuf.at[t, j],
                    sems.at[t, parts + j],
                )
            )
        for copy in group:
            copy.start()
        copies.append(group)
    new = lax.broadcasted_iota(jnp.int32, (rows // 2, rows), 0)
    old = lax.broadcasted_iota(jnp.int32, (rows // 2, rows), 1)
    spread = (new // CAP) * (2 * CAP) + new % CAP
    orders = [jnp.where(old == spread + h * CAP, 1.0, 0.0).astype(BF16) for h in range(2)]
    for t, group in enumerate(copies):
        for copy in group:
            copy.wait()
        x = [
            jnp.concatenate(
                [contract(order, xbuf[t, i], 1, 0).astype(BF16) for i in range(parts)], axis=0
            )
            for order in orders
        ]
        for j in range(4):
            term = contract(x[0], wbuf[t, 2 * j], 1, 0) + contract(x[1], wbuf[t, 2 * j + 1], 1, 0)
            columns = slice(j * width, (j + 1) * width)
            acc[:, columns] = term if t == 0 else acc[:, columns] + term
    for j in range(2):
        gate = acc[:, 2 * j * width : (2 * j + 1) * width]
        up = acc[:, (2 * j + 1) * width : (2 * j + 2) * width]
        value = gate / (1.0 + jnp.exp(-gate)) * up
        out_ref[:, j * width : (j + 1) * width] = value.astype(BF16)


def hidden_units(xs, weights, ktile=512):
    parts = len(xs)
    in_rows, half = xs[0].shape
    rows = parts * in_rows // 2
    depth, width = weights[0].shape
    steps = half // ktile
    return pl.pallas_call(
        functools.partial(hidden_kernel, parts=parts, ktile=ktile),
        in_specs=[pl.BlockSpec(memory_space=pl.ANY)] * (parts + 4),
        out_shape=jax.ShapeDtypeStruct((rows, 2 * width), BF16),
        scratch_shapes=[
            pltpu.VMEM((steps, parts, in_rows, ktile), BF16),
            pltpu.VMEM((steps, 8, ktile, width), BF16),
            pltpu.VMEM((rows, 4 * width), F32),
            pltpu.SemaphoreType.DMA((steps, parts + 8)),
        ],
        cost_estimate=pl.CostEstimate(
            flops=8 * rows * depth * width,
            transcendentals=2 * rows * width,
            bytes_accessed=8 * depth * width + 2 * rows * depth,
        ),
        name="hidden_units",
    )(*xs, *weights)


def down_kernel(n0, f0, n1, f1, n2a, n2b, f2, n3, f3, *rest):
    weights = rest[:8]
    state_ref, out_ref, abuf, wbuf, acc, sems = rest[8:]
    rows, _ = f0.shape
    width, depth = weights[0].shape
    copies = []
    pairs = (
        (n0.at[0], n0.at[1], f0, n0.at[2]),
        (n1.at[0], n1.at[1], f1, n1.at[2]),
        (n2a.at[0], n2a.at[1], f2, n2b.at[0]),
        (n3.at[0], n3.at[1], f3, n3.at[2]),
    )
    for m, ordered in enumerate(pairs):
        group = [
            pltpu.make_async_copy(
                ordered[(i - m) % NY], abuf.at[m, pl.ds(i * rows, rows), :], sems.at[m, i]
            )
            for i in range(NY)
        ]
        for c in range(2):
            group.append(
                pltpu.make_async_copy(
                    weights[2 * m + c], wbuf.at[2 * m + c], sems.at[m, NY + c]
                )
            )
        for copy in group:
            copy.start()
        copies.append(group)
    for m, group in enumerate(copies):
        for copy in group:
            copy.wait()
        term = contract(abuf[m, :, 0:width], wbuf[2 * m], 1, 0) + contract(
            abuf[m, :, width : 2 * width], wbuf[2 * m + 1], 1, 0
        )
        acc[...] = term if m == 0 else acc[...] + term
    group = 32
    tile = NY * group
    new = lax.broadcasted_iota(jnp.int32, (tile, tile), 0)
    old = lax.broadcasted_iota(jnp.int32, (tile, tile), 1)
    want = (new // CAP % NY) * group + (new // (CAP * NY)) * CAP + new % CAP
    order = jnp.where(old == want, 1.0, 0.0).astype(BF16)
    for t in range(rows // group):
        mine = jnp.concatenate(
            [acc[pl.ds(i * rows + t * group, group), :] for i in range(NY)], axis=0
        )
        out_ref[pl.ds(t * tile, tile), 0:depth] = contract(
            order, mine.astype(BF16), 1, 0
        ).astype(BF16)
    out_ref[:, depth:] = state_ref[...]


def expert_down(hs, weights, states):
    rows, units = hs[1].shape
    width, depth = weights[0].shape
    out_rows = NY * rows
    columns = depth + states.shape[1]
    return pl.pallas_call(
        down_kernel,
        in_specs=[pl.BlockSpec(memory_space=pl.ANY)] * (len(hs) + len(weights))
        + [pl.BlockSpec(memory_space=pltpu.VMEM)],
        out_shape=jax.ShapeDtypeStruct((out_rows, columns), BF16),
        scratch_shapes=[
            pltpu.VMEM((NY, out_rows, units), BF16),
            pltpu.VMEM((len(weights), width, depth), BF16),
            pltpu.VMEM((out_rows, depth), F32),
            pltpu.SemaphoreType.DMA((NY, NY + 2)),
        ],
        cost_estimate=pl.CostEstimate(
            flops=2 * out_rows * units * NY * depth,
            transcendentals=0,
            bytes_accessed=8 * 10**6,
        ),
        name="expert_down",
    )(*hs, *weights, states)


def combine_kernel(idx_ref, back_ref, slot_ref, weight_ref, o0, o1, o2, o3, *, part):
    y = idx_ref[0] // 2
    core = idx_ref[0] % 2
    firsts = [(((y + i) % NY) * 2 + core) * part for i in range(NY)]
    own = own_columns(slot_ref[...], firsts, part)
    block = lax.broadcasted_iota(jnp.int32, own.shape, 1) // part
    spot = (own // CAP) * (CAP * NY) + block * CAP + own % CAP
    place = lax.broadcasted_iota(jnp.int32, (back_ref.shape[0], NY * part), 0)
    weight = jnp.concatenate(
        [weight_ref[pl.ds(pl.multiple_of(first, part), part), :] for first in firsts], axis=0
    )
    back = back_ref[...]
    mixed = None
    for j in range(2):
        chosen = jnp.where(place == spot[j : j + 1], 1.0, 0.0).astype(BF16)
        term = contract(chosen, back, 0, 0) * weight[:, j : j + 1]
        mixed = term if mixed is None else mixed + term
    for i, out in enumerate((o0, o1, o2, o3)):
        out[...] = mixed[i * part : (i + 1) * part].astype(out.dtype)


def combine(index, back, slots, weight, part, width):
    total = weight.shape[0]
    return pl.pallas_call(
        functools.partial(combine_kernel, part=part),
        grid_spec=pltpu.PrefetchScalarGridSpec(
            num_scalar_prefetch=1,
            grid=(1,),
            in_specs=[
                pl.BlockSpec((back.shape[0], width), lambda n, idx: (0, 0)),
                pl.BlockSpec((2, total), lambda n, idx: (0, 0)),
                pl.BlockSpec((total, 2), lambda n, idx: (0, 0)),
            ],
            out_specs=[pl.BlockSpec((part, width), lambda n, idx: (0, 0)) for _ in range(NY)],
        ),
        out_shape=[jax.ShapeDtypeStruct((part, width), BF16) for _ in range(NY)],
        name="combine",
    )(index, back, slots, weight)


def finish_kernel(idx_ref, p0, p1, p2, p3, gain_ref, out_ref):
    y = idx_ref[0] // 2
    width = p0.shape[1]
    pieces = [p[...].astype(F32) for p in (p0, p1, p2, p3)]
    square = sum(jnp.sum(p * p, axis=-1, keepdims=True) for p in pieces)
    scale = lax.rsqrt(square / (width * NY) + 1e-06)
    for i, piece in enumerate(pieces):
        columns = pl.ds(pl.multiple_of(((y + i) % NY) * width, width), width)
        out_ref[:, columns] = (piece * scale * gain_ref[:, columns]).astype(BF16)


def finish(index, pieces, gain):
    part, width = pieces[0].shape
    full = width * NY
    return pl.pallas_call(
        finish_kernel,
        grid_spec=pltpu.PrefetchScalarGridSpec(
            num_scalar_prefetch=1,
            grid=(1,),
            in_specs=[pl.BlockSpec((part, width), lambda n, idx: (0, 0)) for _ in pieces]
            + [pl.BlockSpec((1, full), lambda n, idx: (0, 0))],
            out_specs=pl.BlockSpec((part, full), lambda n, idx: (0, 0)),
        ),
        out_shape=jax.ShapeDtypeStruct((part, full), BF16),
        name="finish",
    )(index, *pieces, gain.reshape(1, full))


def from_right(x):
    return lax.ppermute(x, "y", ring(NY, -1))


def from_left(x):
    return lax.ppermute(x, "y", ring(NY, 1))


def on_device(
    queries,
    key_vectors,
    value_vectors,
    decay_logit,
    head_gain,
    routed_rows,
    pre_gain,
    expert_pick,
    route_weight,
    gate_weight,
    up_weight,
    down_weight,
    post_gain,
):
    y = lax.axis_index("y")
    core = lax.axis_index("c")
    experts = lax.axis_size(EP)
    part = routed_rows.shape[0] // (NY * 2)
    width = routed_rows.shape[1]
    index = (y * 2 + core).astype(jnp.int32).reshape(1)
    swap = [(0, 1), (1, 0)]

    gate, up, down = gate_weight[0], up_weight[0], down_weight[0]
    outgoing, slots = dispatch(index, routed_rows, pre_gain, expert_pick, part, experts)
    arrived = exchange(outgoing.reshape(experts, 2 * CAP, width // 2))

    weights = (gate, up, lax.ppermute(gate, "c", swap), lax.ppermute(up, "c", swap))
    cut = width // NY
    slices = [
        lax.dynamic_slice_in_dim(down, lax.rem(y + i, NY) * cut, cut, axis=1) for i in range(NY)
    ]
    mine = [slices[0]] + [lax.ppermute(slices[-m % NY], "y", ring(NY, -m)) for m in range(1, NY)]
    local_out, query_carry, local_state = attn_local(
        queries, key_vectors, value_vectors, decay_logit
    )
    mine, _ = lax.optimization_barrier((mine, local_state))
    arrived, local_state = lax.optimization_barrier((arrived, local_state))
    downs = []
    for piece in mine:
        downs += [piece, lax.ppermute(piece, "c", swap)]

    half = experts // 2
    top = arrived[:half].reshape(-1, width // 2)
    bottom = arrived[half:].reshape(-1, width // 2)
    right_top, right_bottom = from_right(top), from_right(bottom)
    left_top, left_bottom = from_left(top), from_left(bottom)
    far_top, far_bottom = from_left(left_top), from_right(right_bottom)

    chunk_states = exchange(local_state)
    before = prefix(chunk_states)
    sides, before = lax.optimization_barrier(
        ((right_top, right_bottom, left_top, left_bottom), before)
    )
    near = hidden_units([top, bottom, *sides], weights).reshape(3, -1, 2 * gate.shape[1])
    far = hidden_units([far_top, far_bottom], weights)
    near_left, near_right = from_left(near), from_right(near)
    far_left, far_right = from_left(far), from_right(far)
    far_far = lax.ppermute(far, "y", ring(NY, 2))
    near_left, near_right, far = lax.optimization_barrier((near_left, near_right, far))
    near_far = (from_left(near_left[:2]), from_right(near_right[2:]))
    back = expert_down(
        (near, far, near_right, far_right, *near_far, far_far, near_left, far_left),
        downs,
        before.reshape(-1, DK),
    )
    returned = exchange(back.reshape(experts, NY * CAP, cut + DK)).reshape(-1, cut + DK)

    pieces = combine(index, returned, slots, route_weight, part, cut)
    gathered = [pieces[0]] + [
        lax.ppermute(pieces[-m % NY], "y", ring(NY, -m)) for m in range(1, NY)
    ]
    routed_out = finish(index, gathered, post_gain)
    mixed_heads = attn_out(local_out, query_carry, returned, head_gain, cut // DK)
    return (mixed_heads, routed_out)


def solution(mesh):
    ep, tp = mesh.shape["ep"], mesh.shape["tp"]
    torus = Mesh(mesh.devices.reshape(ep // 4, 4, NY, tp // NY), ("z", "x", "y", "c"))
    tpa = ("y", "c")
    placed = (
        P(EP, tpa),
        P(EP, tpa),
        P(EP, tpa),
        P(EP, tpa),
        P(),
        P(EP, None),
        P(),
        P(EP, None),
        P(EP, None),
        P(EP, None, tpa),
        P(EP, None, tpa),
        P(EP, tpa, None),
        P(),
    )
    return jax.shard_map(
        on_device,
        mesh=torus,
        in_specs=placed,
        out_specs=(P(EP, tpa), P(("z", "x", "y", "c"), None)),
        check_vma=False,
    )
```
